32 devices in a mesh: sp: 16 (over z, y, x), tp: 2 (over core).
Axes of the slice: x: 2, y: 2, z: 4, core: 2. Of those that a mesh axis runs over, the one named last changes fastest.
Arguments:
- mid_rows: bfloat16 [4096, 2048], P(('sp', 'tp')), may hold values from -6 to 6
- cotangent: bfloat16 [4096, 2048], P(('sp', 'tp')), may hold values from -6 to 6
- routes: int32 [4096, 2], P(('sp', 'tp')), may hold values from 0 to 15, all different within a row; in each aligned block of 128 rows (0 to 127, 128 to 255, ...) at most 32 rows name the same one
- route_weight: float32 [4096, 2], P(('sp', 'tp')), may hold values from 0.3 to 2
- filtered: bfloat16 [4096, 2048], P('sp', 'tp'), may hold values from -30 to 30
- conv_taps: float32 [31, 2048], P(None, 'tp'), may hold values from -1 to 1
- norm_gain: float32 [2048], P('tp'), may hold values from 0.1 to 1.9
- out_weight: bfloat16 [2048, 2048], P('tp'), may hold values from -0.125 to 0.125
- gate_weight: bfloat16 [16, 2048, 1024], P('sp', None, 'tp'), may hold values from -0.125 to 0.125
- up_weight: bfloat16 [16, 2048, 1024], P('sp', None, 'tp'), may hold values from -0.125 to 0.125
- down_weight: bfloat16 [16, 1024, 2048], P('sp', 'tp'), may hold values from -0.1875 to 0.1875
Outputs:
- gate_grad: float32 [16, 2048, 1024], P('sp', None, 'tp')
- up_grad: float32 [16, 2048, 1024], P('sp', None, 'tp')
- down_grad: float32 [16, 1024, 2048], P('sp', 'tp')
- proj_grad: float32 [2048, 2048], P('sp', 'tp')
- input_grad: bfloat16 [4096, 2048], P('sp', 'tp')
The draws below stay inside these ranges and needn't reach their ends.
Inputs may be any that keep to these rules, and one draw needn't show every extreme that they name: `routes`: each row names 2 different experts. In each aligned block of 128 rows no expert is named by more than 32 rows.
All inputs are finite; a program needn't handle non-finite values.
Results may differ from the reference program's by a relative error of at most 0.0075.
Values may be sent and summed in bfloat16 or wider, within the bound.
A program may use at most 128 MiB of HBM per device.

```python
import math
import jax
import jax.numpy as jnp
import numpy as np
from jax import lax

D = 2048
FFE = 1024
TAPS = 31
TOPK = 2
EXPERTS = 16
TOKENS = 4096
ROWS_DEV = 128
CAP = 32
N_SP = 16
N_TP = 2


def draw_filtered(key, part):
    base_key, chan_key, row_key = jax.random.split(key, 3)
    channel = jnp.arange(D)
    block_factor = jnp.where(channel >= D // 2, 3.0, 1.0)
    spread = jnp.exp(jax.random.uniform(chan_key, (D,), jnp.float32, -0.7, 0.7))
    values = jnp.clip(jax.random.normal(base_key, (TOKENS, D), jnp.float32), -4.0, 4.0)
    return (values * block_factor * spread).astype(jnp.bfloat16)


def raised(values, own_key, source, target, shards_of, factor):
    def block_of(dim):
        return (jnp.arange(values.shape[dim]) // (values.shape[dim] // shards_of)).reshape((-1,) + (1,) * (values.ndim - 1 - dim))

    one_side = jax.random.permutation(own_key, shards_of)[block_of(target)]
    second = (block_of(target) + shards_of // 2) % shards_of
    return jnp.where((block_of(source) == one_side) | (block_of(source) == second), factor * values, values)


def block_levels(own_key, extent, cuts, smallest, top_value):
    gain, own = 1.0, jax.random.fold_in(own_key, 6)
    for axis_at, blocks in cuts:
        steps = jnp.exp(jax.random.uniform(jax.random.fold_in(own, axis_at), (blocks,), jnp.float32, smallest / len(cuts), top_value / len(cuts)))
        gain = gain * jnp.repeat(steps, extent[axis_at] // blocks).reshape([-1 if axis == axis_at else 1 for axis in range(len(extent))])
    return gain


def deal_out(stream_key, own, number, rows, count, top, limit, lean):
    sequence = jax.random.permutation(stream_key, count)
    heavy_load, common = portions_of(count, rows * top, limit, lean, True), portions_of(count, rows * top, limit, lean, False)
    places = jnp.arange(count)

    def named(lengths, offset_by):
        used = int((lengths > 0).sum())
        fixed = max(1, used // 4)
        moved = fixed + (places - fixed + offset_by * (used - fixed)) % max(1, count - fixed)
        return jnp.zeros((count,), jnp.int32).at[sequence[jnp.where(places < fixed, places, moved)]].set(jnp.asarray(lengths, jnp.int32))

    lengths = jnp.where(number % 4 == 0, named(heavy_load, number // 4), named(common, number - number // 4 - 1))
    mixed = jax.random.permutation(jax.random.fold_in(own, 3), count)
    source_of, taker = mixed[0:count // 2 * 2:2], mixed[1:count // 2 * 2:2]
    slack = jnp.minimum(lengths[source_of] - 1, limit - lengths[taker]) // 2
    slack = jnp.where((source_of == sequence[0]) | (taker == sequence[0]) | (lengths[taker] == 0), 0, jnp.maximum(slack, 0))
    moved = jax.random.randint(jax.random.fold_in(own, 4), (count // 2,), 0, 1 << 20) % (slack + 1)
    lengths = lengths.at[source_of].add(-moved).at[taker].add(moved)
    labels = jnp.searchsorted(jnp.cumsum(lengths), jnp.arange(rows * top), side="right").astype(jnp.int32)
    grid = labels.reshape(top, rows).T
    grid = grid[jax.random.permutation(jax.random.fold_in(own, 1), rows)]
    offset_by = jax.random.randint(jax.random.fold_in(own, 2), (rows, 1), 0, top)
    return jnp.take_along_axis(grid, (jnp.arange(top)[None, :] + offset_by) % top, axis=1)


def portions_of(number_of, total, bound, skew, full):
    weights = [(1 << 20) // math.isqrt(rank ** skew) + 1 for rank in range(1, number_of + 1)]
    largest = bound if full else min(bound, max(-(-total // number_of), total * weights[0] // sum(weights)))
    least = 1 if total - largest >= number_of - 1 else 0
    holding, rest = [largest] + [least] * (number_of - 1), total - largest - least * (number_of - 1)
    while rest > 0:
        candidates = [i for i in range(1, number_of) if holding[i] < largest] or [i for i in range(1, number_of) if holding[i] < bound]
        pool, budget = sum([weights[i] for i in candidates]), rest
        for i in candidates:
            addition = min(bound - holding[i], max(1, budget * weights[i] // pool), rest)
            holding[i] = holding[i] + addition
            rest = rest - addition
    return np.array(holding)


def gaussian(rng, shape, scale, limit, cuts=(), kind=jnp.bfloat16):
    level = block_levels(rng, shape, cuts, -0.22, 0.18) if cuts else 1.0
    values = jax.random.normal(rng, shape, jnp.float32) * scale * level
    return jnp.minimum(jnp.maximum(values, -limit), limit).astype(kind)


def bell_draw_with(key, dims, deviation, bound, cuts, heavy, kind=jnp.bfloat16):
    values = deviation * jax.random.normal(key, dims, jnp.float32)
    if cuts:
        values = values * block_levels(key, dims, cuts, -0.22, 0.18)
    return jnp.clip(raised(values, jax.random.fold_in(key, 3), *heavy), -bound, bound).astype(kind)


def setup_inputs(seed: int = 0) -> dict:
    keys = jax.random.split(jax.random.key(seed), 12)
    mid_rows = gaussian(keys[0], (TOKENS, D), 1.0, 6.0, ((0, 32),))
    cotangent = bell_draw_with(keys[1], (TOKENS, D), 1.0, 6.0, ((0, 32),), (0, 1, 32, 2.75))
    routes_keys = jax.random.split(jax.random.fold_in(keys[2], 1), TOKENS // ROWS_DEV)
    routes_turns = jax.random.permutation(jax.random.fold_in(keys[2], 3), TOKENS // ROWS_DEV)
    routes = jax.vmap(lambda own, number: deal_out(jax.random.fold_in(keys[2], 2), own, number, ROWS_DEV, EXPERTS, TOPK, CAP, 2))(routes_keys, routes_turns).reshape((TOKENS, TOPK))
    route_weight = jnp.clip(jnp.exp(math.log(2.0) - 1.89712 * jax.random.uniform(keys[3], (TOKENS, TOPK), jnp.float32) ** block_levels(keys[3], (TOKENS, TOPK), ((0, 32),), -0.2, 0.2)), 0.3, 2.0)
    filtered = draw_filtered(jax.random.fold_in(keys[11], 71), 0)
    conv_taps = gaussian(keys[5], (TAPS, D), TAPS ** -0.5, 1.0, ((1, 2),), jnp.float32)
    norm_gain = jnp.clip(1.0 + 0.18 * jax.random.normal(keys[6], (D,), jnp.float32), 0.1, 1.9)
    out_weight = gaussian(keys[7], (D, D), D ** -0.5, 0.125, ((0, 2),))
    gate_weight = gaussian(keys[8], (EXPERTS, D, FFE), D ** -0.5, 0.125, ((0, 16), (2, 2)))
    up_weight = gaussian(keys[9], (EXPERTS, D, FFE), D ** -0.5, 0.125, ((0, 16), (2, 2)))
    down_weight = gaussian(keys[10], (EXPERTS, FFE, D), FFE ** -0.5, 0.1875, ((0, 16), (1, 2)))
    return dict(mid_rows=mid_rows, cotangent=cotangent, routes=routes, route_weight=route_weight, filtered=filtered, conv_taps=conv_taps, norm_gain=norm_gain, out_weight=out_weight, gate_weight=gate_weight, up_weight=up_weight, down_weight=down_weight)


NORM_EPS = 1e-05

def silu_grad(pre_act):
    logistic = jax.nn.sigmoid(pre_act)
    return logistic * (1.0 + pre_act * (1.0 - logistic))

def reference(mid_rows, cotangent, routes, route_weight, filtered, conv_taps, norm_gain, out_weight, gate_weight, up_weight, down_weight):
    total_routes = TOKENS * TOPK
    flattened = routes.reshape(total_routes)
    weight_flat = jnp.concatenate([route_weight.reshape(total_routes), jnp.zeros((1,), jnp.float32)])
    route_ids = jnp.arange(total_routes, dtype=jnp.int32)
    slot_total = N_SP * N_TP * CAP
    half_width = FFE // N_TP

    def expert_step(collected, expert):
        chosen = flattened == expert
        positions = jnp.cumsum(chosen.astype(jnp.int32)) - 1
        target = jnp.where(chosen, positions, slot_total).astype(jnp.int32)
        slot_owner = jnp.full((slot_total + 1,), total_routes, jnp.int32).at[target].set(route_ids)[:slot_total]
        token_of = (slot_owner // TOPK).astype(jnp.int32)
        inputs = jnp.take(mid_rows, token_of, axis=0, mode='fill', fill_value=0)
        cot_rows = jnp.take(cotangent, token_of, axis=0, mode='fill', fill_value=0).astype(jnp.float32)
        route_scale = weight_flat[slot_owner]
        routed = (route_scale[:, None] * cot_rows).astype(jnp.bfloat16)
        gate_mat = gate_weight[expert]
        up_mat = up_weight[expert]
        down_mat = down_weight[expert]
        pre_gate = jnp.dot(inputs, gate_mat, preferred_element_type=jnp.float32)
        pre_up = jnp.dot(inputs, up_mat, preferred_element_type=jnp.float32)
        gate_act = jax.nn.silu(pre_gate)
        hidden = (gate_act * pre_up).astype(jnp.bfloat16)
        down_part = jnp.dot(hidden.T, routed, preferred_element_type=jnp.float32)
        hidden_grad = jnp.dot(routed, down_mat.T, preferred_element_type=jnp.float32)
        gate_pre = (hidden_grad * pre_up * silu_grad(pre_gate)).astype(jnp.bfloat16)
        up_pre = (hidden_grad * gate_act).astype(jnp.bfloat16)
        gate_part = jnp.dot(inputs.T, gate_pre, preferred_element_type=jnp.float32)
        up_part = jnp.dot(inputs.T, up_pre, preferred_element_type=jnp.float32)
        summed = jnp.zeros((slot_total, D), jnp.float32)
        for band_index in range(N_TP):
            band_start = band_index * half_width
            band_stop = band_start + half_width
            band_term = jnp.dot(gate_pre[:, band_start:band_stop], gate_mat[:, band_start:band_stop].T, preferred_element_type=jnp.float32)
            band_term = band_term + jnp.dot(up_pre[:, band_start:band_stop], up_mat[:, band_start:band_stop].T, preferred_element_type=jnp.float32)
            summed = summed + lax.optimization_barrier(band_term.astype(jnp.bfloat16)).astype(jnp.float32)
        route_grad = summed.astype(jnp.bfloat16)
        collected = collected.at[slot_owner].set(route_grad)
        return (collected, (gate_part, up_part, down_part))
    start_rows = jnp.zeros((total_routes + 1, D), jnp.bfloat16)
    collected, (gate_grad, up_grad, down_grad) = lax.scan(expert_step, start_rows, jnp.arange(EXPERTS, dtype=jnp.int32))
    route_sum = lax.optimization_barrier(jnp.sum(collected[:total_routes].astype(jnp.float32).reshape(TOKENS, TOPK, D), axis=1))
    mid_grad = (cotangent.astype(jnp.float32) + route_sum).astype(jnp.bfloat16)
    values = filtered.astype(jnp.float32)
    average = lax.optimization_barrier(jnp.mean(values, axis=1, keepdims=True))
    variance = lax.optimization_barrier(jnp.mean(values * values, axis=1, keepdims=True)) - average * average
    inv_scale = lax.rsqrt(variance + NORM_EPS)
    normed = (values - average) * inv_scale
    scaled = normed * norm_gain
    activated = jax.nn.silu(scaled).astype(jnp.bfloat16)
    proj_grad = jnp.dot(mid_grad.T, activated, preferred_element_type=jnp.float32)
    act_grad = jnp.dot(mid_grad, out_weight.T, preferred_element_type=jnp.float32)
    scaled_grad = act_grad * silu_grad(scaled) * norm_gain
    grad_mean = lax.optimization_barrier(jnp.mean(scaled_grad, axis=1, keepdims=True))
    grad_corr = lax.optimization_barrier(jnp.mean(scaled_grad * normed, axis=1, keepdims=True))
    conv_grad = (inv_scale * (scaled_grad - grad_mean - normed * grad_corr)).astype(jnp.bfloat16)
    halo_width = TAPS // 2
    padded = jnp.pad(conv_grad, ((halo_width, halo_width), (0, 0))).astype(jnp.float32)
    accumulated = jnp.zeros((TOKENS, D), jnp.float32)
    for offset in range(TAPS):
        lead = 2 * halo_width - offset
        accumulated = accumulated + conv_taps[offset] * padded[lead:lead + TOKENS]
    input_grad = accumulated.astype(jnp.bfloat16)
    return (gate_grad, up_grad, down_grad, proj_grad, input_grad)
```

```python
import functools

import jax
import jax.numpy as jnp
from jax import lax
from jax.experimental import pallas as pl
from jax.experimental.pallas import tpu as pltpu
from jax.sharding import PartitionSpec as P

MESH = pl.DeviceIdType.MESH
NORM_EPS = 1e-05


def extended(block, sides, width):
    for axis, dim in sides:
        count = lax.axis_size(axis)
        forward = [(i, i + 1) for i in range(count - 1)]
        backward = [(target, source) for source, target in forward]
        low = lax.ppermute(
            lax.slice_in_dim(block, block.shape[dim] - width, None, axis=dim), axis, forward
        )
        high = lax.ppermute(lax.slice_in_dim(block, 0, width, axis=dim), axis, backward)
        block = jnp.concatenate([low, block, high], axis=dim)
    return block


def silu_grad(pre_act):
    logistic = jax.nn.sigmoid(pre_act)
    return logistic * (1.0 + pre_act * (1.0 - logistic))


def slot_targets(routes, experts, capacity):
    token_count, per_token = routes.shape
    flattened = routes.reshape(token_count * per_token)
    one_hot = flattened[:, None] == jnp.arange(experts, dtype=jnp.int32)[None, :]
    route_ids = jnp.arange(token_count * per_token, dtype=jnp.int32)
    before = (route_ids[None, :] < route_ids[:, None]).astype(jnp.bfloat16)
    earlier = jnp.dot(before, one_hot.astype(jnp.bfloat16), preferred_element_type=jnp.float32)
    positions = jnp.sum(jnp.where(one_hot, earlier, 0.0), axis=1).astype(jnp.int32)
    return (flattened * capacity + positions).reshape(token_count, per_token)


def halving_orders(count):
    bits = count.bit_length() - 1
    turned = min(bits, 3)
    return [
        [(start + step) % turned for step in range(turned)] + list(range(turned, bits))
        for start in range(turned)
    ]


def column_groups(columns, groups):
    lanes = 128
    tiles = columns // lanes
    sizes = [tiles // groups + (1 if g < tiles % groups else 0) for g in range(groups)]
    starts = [sum(sizes[:g]) * lanes for g in range(groups)]
    return [(start, size * lanes) for start, size in zip(starts, sizes) if size]


def picked(block, place, dim):
    return lax.dynamic_index_in_dim(block, place, dim, keepdims=False)


def reduced_products(rows, columns, axis):
    count = lax.axis_size(axis)
    tokens, width = rows.shape
    bits = count.bit_length() - 1
    own = lax.axis_index(axis)
    product = transposed_product(rows, columns).astype(jnp.bfloat16)
    cut = product.reshape((2,) * bits + (width // count, columns.shape[1]))
    orders = halving_orders(count)
    groups = column_groups(columns.shape[1], len(orders))
    orders = orders[: len(groups)]
    totals = [lax.slice_in_dim(cut, start, start + size, axis=bits + 1) for start, size in groups]
    left = [list(range(bits - 1, -1, -1)) for _ in groups]
    for step in range(bits):
        outgoing, kept = [], []
        for total, order, dims in zip(totals, orders, left):
            mine = (own >> order[step]) & 1
            dim = dims.index(order[step])
            dims.pop(dim)
            outgoing.append(picked(total, 1 - mine, dim).astype(jnp.bfloat16))
            kept.append(picked(total, mine, dim).astype(jnp.float32))
        if step == 0:
            outgoing, rows = lax.optimization_barrier((outgoing, rows))
        arrived = [
            lax.ppermute(block, axis, [(i, i ^ (1 << order[step])) for i in range(count)])
            for block, order in zip(outgoing, orders)
        ]
        arrived = lax.optimization_barrier(arrived)
        totals = [own_part + got.astype(jnp.float32) for own_part, got in zip(kept, arrived)]
    return jnp.concatenate(totals, axis=1), rows


def row_product(rows, matrix, dim=0):
    return lax.dot_general(
        rows, matrix, (((1,), (dim,)), ((), ())), preferred_element_type=jnp.float32
    )


def transposed_product(left, right):
    return lax.dot_general(
        left, right, (((0,), (0,)), ((), ())), preferred_element_type=jnp.float32
    )


def line_extent(count):
    bits = count.bit_length() - 1
    return 1 << -(-bits // 3)


def chunk_orders(extent):
    orders = []
    for own in range(extent):
        toward = [i for i in range(own + 1, extent)] if 2 * own < extent - 1 else [i for i in range(own - 1, -1, -1)]
        back = [i for i in range(extent) if i != own and i not in toward]
        back.sort(key=lambda i: abs(i - own))
        if own in (0, extent - 1):
            order = toward
        else:
            order = toward[:1] + back + toward[1:]
        orders.append([own] + order)
    return orders


def relay_orders(extent):
    return [
        sorted(
            (i for i in range(extent) if i != own),
            key=lambda i: (own if i > own else extent - 1 - own, abs(i - own)),
        )
        for own in range(extent)
    ]


def looked_up(table, row, column):
    value = jnp.int32(0)
    for i, entries in enumerate(table):
        for k, entry in enumerate(entries):
            value = value + jnp.where((row == i) & (column == k), entry, 0)
    return value


def routed_kernel(
    extent,
    plane,
    capacity,
    mid_hbm,
    cot_hbm,
    meta,
    gate_hbm,
    up_hbm,
    down_hbm,
    tokens_out,
    inputs_out,
    routed_out,
    hidden_out,
    gate_pre_out,
    up_pre_out,
    tok,
    metas,
    picks,
    rows,
    gate,
    up,
    down,
    pre_gate,
    pre_up,
    hidden,
    gate_pre,
    up_pre,
    part_own,
    part_sent,
    part_got,
    ret_sent,
    ret_got,
    line_sent,
    line_got,
    total,
    tokens,
    load_sem,
    meta_sems,
    tok_send,
    tok_recv,
    row_send,
    row_recv,
    swap_send,
    swap_recv,
    part_sems,
    ret_send,
    ret_recv,
    line_send,
    line_recv,
    out_sems,
    token_sems,
):
    sp, tp = lax.axis_index("sp"), lax.axis_index("tp")
    z, p = sp // plane, sp % plane
    slots = plane * capacity
    token_count, width = tok.shape[2], tok.shape[3]
    other = 1 - tp
    step = min(512, width)
    columns = width // step
    orders, relays = chunk_orders(extent), relay_orders(extent)
    load_from = [mid_hbm, cot_hbm]

    def remote(src, dst, send, recv, to_sp, to_tp):
        return pltpu.make_async_remote_copy(
            src_ref=src,
            dst_ref=dst,
            send_sem=send,
            recv_sem=recv,
            device_id=(to_sp, to_tp),
            device_id_type=MESH,
        )

    loads = [
        pltpu.make_async_copy(mid_hbm, tok.at[0, z], load_sem.at[0]),
        pltpu.make_async_copy(cot_hbm, tok.at[1, z], load_sem.at[1]),
        pltpu.make_async_copy(gate_hbm, gate, load_sem.at[2]),
        pltpu.make_async_copy(up_hbm, up, load_sem.at[3]),
        pltpu.make_async_copy(down_hbm, down, load_sem.at[4]),
    ]
    for load in loads:
        load.start()
    metas[z] = meta[...]

    barrier = pltpu.get_barrier_semaphore()

    def greet(to_sp, to_tp):
        pl.semaphore_signal(barrier, inc=1, device_id=(to_sp, to_tp), device_id_type=MESH)

    def line_peer(i):
        return lax.rem(z + i, extent)

    def plane_peer(i):
        return lax.rem(p + i, plane)

    for i in range(1, extent):
        greet(line_peer(i) * plane + p, tp)

    @pl.loop(1, plane)
    def _(i):
        greet(z * plane + plane_peer(i), tp)

    greet(sp, other)
    pl.semaphore_wait(barrier, extent - 1 + plane - 1 + 1)

    def meta_copy(to_z, from_z):
        return remote(
            meta, metas.at[from_z], meta_sems.at[0, to_z], meta_sems.at[1, from_z], to_z * plane + p, tp
        )

    def tok_copy(t, origin, up_way):
        to_z = z + 1 if up_way else z - 1
        return remote(
            tok.at[t, origin],
            tok.at[t, origin],
            tok_send.at[t, origin, int(up_way)],
            tok_recv.at[t, origin],
            to_z * plane + p,
            tp,
        )

    def forwards(origin, up_way):
        if up_way:
            return (origin <= z) & (z < extent - 1)
        return (origin >= z) & (z > 0)

    def row_copy(t, origin, q):
        return remote(
            picks.at[t, origin, q],
            rows.at[t, origin, 0, p],
            row_send.at[t, origin, q],
            row_recv.at[t, origin, p],
            z * plane + q,
            tp,
        )

    def row_arrival(t, origin, q):
        return remote(
            picks.at[t, origin, q],
            rows.at[t, origin, 0, q],
            row_send.at[t, origin, q],
            row_recv.at[t, origin, q],
            z * plane + q,
            tp,
        )

    def swap_copy(t, origin):
        return remote(
            rows.at[t, origin, 0],
            rows.at[t, origin, 1],
            swap_send.at[t, origin],
            swap_recv.at[t, origin],
            sp,
            other,
        )

    def part_copy(origin):
        return remote(
            part_sent.at[origin],
            part_got.at[origin],
            part_sems.at[0, origin],
            part_sems.at[1, origin],
            sp,
            other,
        )

    def ret_copy(origin, q):
        return remote(
            ret_sent.at[origin, q],
            ret_got.at[origin, p],
            ret_send.at[origin, q],
            ret_recv.at[origin, p],
            z * plane + q,
            tp,
        )

    def ret_arrival(origin, q):
        return remote(
            ret_sent.at[origin, q],
            ret_got.at[origin, q],
            ret_send.at[origin, q],
            ret_recv.at[origin, q],
            z * plane + q,
            tp,
        )

    def band(j):
        return pl.ds(j * step, step)

    def line_copy(home, j):
        to_z = jnp.where(home > z, z + 1, z - 1)
        slot = jnp.where((home < z) & (to_z == home), extent, home)
        return remote(
            line_sent.at[home, :, band(j)],
            line_got.at[slot, :, band(j)],
            line_send.at[home, j],
            line_recv.at[slot, j],
            to_z * plane + p,
            tp,
        )

    def line_arrival(slot, j):
        return remote(
            line_sent.at[0, :, band(j)],
            line_got.at[slot, :, band(j)],
            line_send.at[0, j],
            line_recv.at[slot, j],
            z * plane + p,
            other,
        )

    def has_inflow(home):
        return ((home > z) & (z > 0)) | ((home < z) & (z < extent - 1))

    def hits(origin):
        slot = lax.broadcasted_iota(jnp.int32, (slots, token_count), 0) + z * slots
        slot = slot.astype(jnp.float32)
        return [slot == metas[origin, pl.ds(k, 1), :] for k in range(TOPK_ROWS)]

    def chooser(origin):
        first, second = hits(origin)
        return jnp.where(first | second, 1.0, 0.0).astype(jnp.bfloat16)

    def scale_of(origin):
        first, second = hits(origin)
        weighted = jnp.where(first, metas[origin, pl.ds(TOPK_ROWS, 1), :], 0.0) + jnp.where(
            second, metas[origin, pl.ds(TOPK_ROWS + 1, 1), :], 0.0
        )
        return jnp.sum(weighted, axis=1, keepdims=True)

    def arrive(t, k):
        origin = looked_up(orders, z, k)

        @pl.when(k > 0)
        def _():
            tok_copy(t, origin, True).wait_recv()
            if t == 0:
                meta_copy(origin, origin).wait_recv()

        for up_way in (False, True):

            @pl.when(forwards(origin, up_way))
            def _():
                tok_copy(t, origin, up_way).start()

        select = chooser(origin)
        if t == 1:
            scale = scale_of(origin)
        for j in range(columns):
            picked = jnp.dot(
                select, tok[t, origin, :, band(j)], preferred_element_type=jnp.float32
            )
            if t == 1:
                picked = scale * picked
            picks[t, origin, :, :, band(j)] = picked.astype(jnp.bfloat16).reshape(
                plane, capacity, step
            )

        @pl.loop(1, plane)
        def _(i):
            row_copy(t, origin, plane_peer(i)).start()

        rows[t, origin, 0, p] = picks[t, origin, p]

    def swap(t, k):
        origin = looked_up(orders, z, k)

        @pl.loop(1, plane)
        def _(i):
            row_arrival(t, origin, plane_peer(i)).wait_recv()

        swap_copy(t, origin).start()

    def expert_rows(t, origin):
        return rows[t, origin].reshape(2 * slots, width)

    half = gate.shape[1]
    tile = min(256, half)

    def first_products(k):
        origin = looked_up(orders, z, k)

        @pl.when(k == 0)
        def _():
            loads[2].wait()
            loads[3].wait()

        swap_copy(0, origin).wait_recv()

        @pl.loop(0, half // tile)
        def _(n):
            cut = pl.ds(pl.multiple_of(n * tile, tile), tile)
            block = expert_rows(0, origin)
            pre_gate[:, cut] = jnp.dot(block, gate[:, cut], preferred_element_type=jnp.float32)
            pre_up[:, cut] = jnp.dot(block, up[:, cut], preferred_element_type=jnp.float32)

    def products(k):
        origin = looked_up(orders, z, k)

        @pl.when(k == 0)
        def _():
            loads[4].wait()

        swap_copy(1, origin).wait_recv()

        @pl.loop(0, half // tile)
        def _(n):
            cut = pl.ds(pl.multiple_of(n * tile, tile), tile)
            hidden_grad = lax.dot_general(
                expert_rows(1, origin),
                down[cut, :],
                (((1,), (1,)), ((), ())),
                preferred_element_type=jnp.float32,
            )
            g, u = pre_gate[:, cut], pre_up[:, cut]
            logistic = jax.nn.sigmoid(g)
            gate_act = g * logistic
            hidden[origin, :, cut] = (gate_act * u).astype(jnp.bfloat16)
            gate_pre[origin, :, cut] = (
                hidden_grad * u * (logistic * (1.0 + g * (1.0 - logistic)))
            ).astype(jnp.bfloat16)
            up_pre[origin, :, cut] = (hidden_grad * gate_act).astype(jnp.bfloat16)

        wide = min(256, width)

        @pl.loop(0, width // wide)
        def _(n):
            cut = pl.ds(pl.multiple_of(n * wide, wide), wide)
            part = lax.dot_general(
                gate_pre[origin],
                gate[cut, :],
                (((1,), (1,)), ((), ())),
                preferred_element_type=jnp.float32,
            ) + lax.dot_general(
                up_pre[origin],
                up[cut, :],
                (((1,), (1,)), ((), ())),
                preferred_element_type=jnp.float32,
            )
            part = part.astype(jnp.bfloat16).reshape(2, plane, capacity, wide)
            part_own[:, :, cut] = part[0]
            part_sent[origin, :, :, cut] = part[1]

        part_copy(origin).start()
        for out in results(origin):
            out.start()

    def results(origin):
        pairs = [
            (rows.at[0, origin], inputs_out.at[origin]),
            (rows.at[1, origin], routed_out.at[origin]),
            (hidden.at[origin], hidden_out.at[origin]),
            (gate_pre.at[origin], gate_pre_out.at[origin]),
            (up_pre.at[origin], up_pre_out.at[origin]),
        ]
        return [
            pltpu.make_async_copy(src, dst, out_sems.at[i, origin])
            for i, (src, dst) in enumerate(pairs)
        ]

    def send_back(k):
        origin = looked_up(orders, z, k)
        part_copy(origin).wait_recv()
        for j in range(columns):
            both = part_own[:, :, band(j)].astype(jnp.float32) + part_got[
                origin, :, :, band(j)
            ].astype(jnp.float32)
            ret_sent[origin, :, :, band(j)] = both.astype(jnp.bfloat16)

        @pl.loop(1, plane)
        def _(i):
            ret_copy(origin, plane_peer(i)).start()

        ret_got[origin, p] = ret_sent[origin, p]

    def combine(k):
        origin = looked_up(orders, z, k)

        @pl.loop(1, plane)
        def _(i):
            ret_arrival(origin, plane_peer(i)).wait_recv()

        select = chooser(origin)
        for j in range(columns):
            back = ret_got[origin, :, :, band(j)].reshape(slots, step)
            added = lax.dot_general(
                select, back, (((0,), (0,)), ((), ())), preferred_element_type=jnp.float32
            )

            @pl.when(origin == z)
            def _():
                total[:, band(j)] = added

            @pl.when(origin != z)
            def _():
                line_sent[origin, :, band(j)] = added.astype(jnp.bfloat16)

            @pl.when((origin != z) & jnp.logical_not(has_inflow(origin)))
            def _():
                line_copy(origin, j).start()

    for load in loads[:2]:
        load.wait()
    for i in range(1, extent):
        meta_copy(line_peer(i), z).start()

    arrive(0, 0)

    @pl.loop(0, extent)
    def _(k):
        arrive(1, k)
        swap(0, k)
        first_products(k)

        @pl.when(k > 0)
        def _():
            combine(k - 1)

        swap(1, k)

        @pl.when(k < extent - 1)
        def _():
            arrive(0, k + 1)

        products(k)
        send_back(k)

    combine(extent - 1)

    @pl.loop(0, extent - 1)
    def _(k):
        home = looked_up(relays, z, k)

        @pl.when(has_inflow(home))
        def _():
            for j in range(columns):
                line_arrival(home, j).wait_recv()
                line_sent[home, :, band(j)] = (
                    line_sent[home, :, band(j)].astype(jnp.float32)
                    + line_got[home, :, band(j)].astype(jnp.float32)
                ).astype(jnp.bfloat16)
                line_copy(home, j).start()

    for j in range(columns):
        for slot, there in ((z, z > 0), (extent, z < extent - 1)):

            @pl.when(there)
            def _():
                line_arrival(slot, j).wait_recv()
                total[:, band(j)] = total[:, band(j)] + line_got[slot, :, band(j)].astype(
                    jnp.float32
                )

        tokens[tp, :, band(j)] = (
            tok[1, z, :, band(j)].astype(jnp.float32) + total[:, band(j)]
        ).astype(jnp.bfloat16)
    token_swap = remote(
        tokens.at[tp], tokens.at[tp], token_sems.at[0], token_sems.at[1], sp, other
    )
    token_swap.start()

    for i in range(1, extent):
        meta_copy(line_peer(i), z).wait_send()

    @pl.loop(0, extent)
    def _(origin):
        for t in range(2):
            for up_way in (False, True):

                @pl.when(forwards(origin, up_way))
                def _():
                    tok_copy(t, origin, up_way).wait_send()

            @pl.loop(1, plane)
            def _(i):
                row_copy(t, origin, plane_peer(i)).wait_send()

            swap_copy(t, origin).wait_send()
        part_copy(origin).wait_send()

        @pl.loop(1, plane)
        def _(i):
            ret_copy(origin, plane_peer(i)).wait_send()

        @pl.when(origin != z)
        def _():
            for j in range(columns):
                line_copy(origin, j).wait_send()

        for out in results(origin):
            out.wait()

    token_swap.wait()
    last = pltpu.make_async_copy(tokens, tokens_out, load_sem.at[0])
    last.start()
    last.wait()


TOPK_ROWS = 2


def routed_backward(mid_rows, cotangent, meta, gate_mat, up_mat, down_mat, capacity):
    sp_count = lax.axis_size("sp")
    extent = line_extent(sp_count)
    plane = sp_count // extent
    token_count, width = mid_rows.shape
    half = gate_mat.shape[1]
    slots = plane * capacity
    kind = jnp.bfloat16
    any_space = pl.BlockSpec(memory_space=pl.ANY)
    dma = pltpu.SemaphoreType.DMA
    columns = width // min(512, width)
    rows_shape = (extent, 2, plane, capacity, width)
    small_shape = (extent, 2 * slots, half)
    out = pl.pallas_call(
        functools.partial(routed_kernel, extent, plane, capacity),
        out_shape=[
            jax.ShapeDtypeStruct((2, token_count, width), kind),
            jax.ShapeDtypeStruct(rows_shape, kind),
            jax.ShapeDtypeStruct(rows_shape, kind),
            jax.ShapeDtypeStruct(small_shape, kind),
            jax.ShapeDtypeStruct(small_shape, kind),
            jax.ShapeDtypeStruct(small_shape, kind),
        ],
        in_specs=[any_space, any_space, pl.BlockSpec(memory_space=pltpu.VMEM)] + [any_space] * 3,
        out_specs=[any_space] * 6,
        scratch_shapes=[
            pltpu.VMEM((2, extent, token_count, width), kind),
            pltpu.VMEM((extent,) + meta.shape, jnp.float32),
            pltpu.VMEM((2, extent, plane, capacity, width), kind),
            pltpu.VMEM((2,) + rows_shape, kind),
            pltpu.VMEM(gate_mat.shape, kind),
            pltpu.VMEM(up_mat.shape, kind),
            pltpu.VMEM(down_mat.shape, kind),
            pltpu.VMEM((2 * slots, half), jnp.float32),
            pltpu.VMEM((2 * slots, half), jnp.float32),
            pltpu.VMEM(small_shape, kind),
            pltpu.VMEM(small_shape, kind),
            pltpu.VMEM(small_shape, kind),
            pltpu.VMEM((plane, capacity, width), kind),
            pltpu.VMEM((extent, plane, capacity, width), kind),
            pltpu.VMEM((extent, plane, capacity, width), kind),
            pltpu.VMEM((extent, plane, capacity, width), kind),
            pltpu.VMEM((extent, plane, capacity, width), kind),
            pltpu.VMEM((extent, token_count, width), kind),
            pltpu.VMEM((extent + 1, token_count, width), kind),
            pltpu.VMEM((token_count, width), jnp.float32),
            pltpu.VMEM((2, token_count, width), kind),
            dma((5,)),
            dma((2, extent)),
            dma((2, extent, 2)),
            dma((2, extent)),
            dma((2, extent, plane)),
            dma((2, extent, plane)),
            dma((2, extent)),
            dma((2, extent)),
            dma((2, extent)),
            dma((extent, plane)),
            dma((extent, plane)),
            dma((extent, columns)),
            dma((extent + 1, columns)),
            dma((5, extent)),
            dma((2,)),
        ],
        compiler_params=pltpu.CompilerParams(
            collective_id=0, has_side_effects=True, vmem_limit_bytes=62 * 1024 * 1024
        ),
    )(mid_rows, cotangent, meta, gate_mat, up_mat, down_mat)
    tokens, inputs, routed, hidden, gate_pre, up_pre = out
    every = 2 * slots * extent
    return (
        tokens.reshape(2 * token_count, width),
        inputs.reshape(every, width),
        routed.reshape(every, width),
        hidden.reshape(every, half),
        gate_pre.reshape(every, half),
        up_pre.reshape(every, half),
    )


def per_device(
    mid_rows,
    cotangent,
    routes,
    route_weight,
    filtered,
    conv_taps,
    norm_gain,
    out_weight,
    gate_weight,
    up_weight,
    down_weight,
):
    sp_count = lax.axis_size("sp")
    token_count, model_width = mid_rows.shape
    per_token = routes.shape[1]
    local_experts = gate_weight.shape[0]
    experts = local_experts * sp_count
    capacity = 2 * token_count * per_token // sp_count
    values = filtered.astype(jnp.float32)
    channel_sum, squares = lax.psum(
        (jnp.sum(values, axis=1), jnp.sum(values * values, axis=1)), "tp"
    )
    target = slot_targets(routes, experts, capacity).astype(jnp.float32)
    meta = jnp.concatenate([target.T, route_weight.T], axis=0)
    meta = jnp.pad(meta, ((0, 8 - meta.shape[0]), (0, 0)))
    grad_tokens, inputs, routed, hidden, gate_pre, up_pre = routed_backward(
        mid_rows, cotangent, meta, gate_weight[0], up_weight[0], down_weight[0], capacity
    )
    gate_grad = transposed_product(inputs, gate_pre)[None]
    up_grad = transposed_product(inputs, up_pre)[None]
    down_grad = transposed_product(hidden, routed)[None]
    average = channel_sum / model_width
    variance = squares / model_width - average * average
    inv_scale = lax.rsqrt(variance + NORM_EPS)[:, None]
    normed = (values - average[:, None]) * inv_scale
    scaled = normed * norm_gain
    activated = jax.nn.silu(scaled).astype(jnp.bfloat16)
    proj_grad, grad_tokens = reduced_products(grad_tokens, activated, "sp")
    act_grad = lax.dot_general(
        grad_tokens, out_weight, (((1,), (1,)), ((), ())), preferred_element_type=jnp.float32
    )
    scaled_grad = act_grad * silu_grad(scaled) * norm_gain
    grad_total, corr_total = lax.psum(
        (jnp.sum(scaled_grad, axis=1), jnp.sum(scaled_grad * normed, axis=1)), "tp"
    )
    grad_mean = (grad_total / model_width)[:, None]
    grad_corr = (corr_total / model_width)[:, None]
    conv_grad = (inv_scale * (scaled_grad - grad_mean - normed * grad_corr)).astype(jnp.bfloat16)
    halo_width = conv_taps.shape[0] // 2
    padded = extended(conv_grad, (("sp", 0),), halo_width)
    seq_rows = conv_grad.shape[0]
    accumulated = jnp.zeros(conv_grad.shape, jnp.float32)
    for offset in range(conv_taps.shape[0]):
        lead = 2 * halo_width - offset
        accumulated = accumulated + conv_taps[offset] * padded[lead : lead + seq_rows]
    input_grad = accumulated.astype(jnp.bfloat16)
    return (gate_grad, up_grad, down_grad, proj_grad, input_grad)


def solution(mesh):
    in_specs = (
        P(("sp", "tp"), None),
        P(("sp", "tp"), None),
        P(("sp", "tp"), None),
        P(("sp", "tp"), None),
        P("sp", "tp"),
        P(None, "tp"),
        P("tp"),
        P("tp", None),
        P("sp", None, "tp"),
        P("sp", None, "tp"),
        P("sp", "tp", None),
    )
    out_specs = (
        P("sp", None, "tp"),
        P("sp", None, "tp"),
        P("sp", "tp", None),
        P("sp", "tp"),
        P("sp", "tp"),
    )
    return jax.shard_map(
        per_device, mesh=mesh, in_specs=in_specs, out_specs=out_specs, check_vma=False
    )
```

```python
import functools
import math

import jax
import jax.numpy as jnp
from jax import lax
from jax.experimental import pallas as pl
from jax.experimental.pallas import tpu as pltpu
from jax.sharding import PartitionSpec as P

MESH = pl.DeviceIdType.MESH
NORM_EPS = 1e-05
SPARE = 4 << 20


def slot_targets(routes, experts, capacity):
    token_count, per_token = routes.shape
    flattened = routes.reshape(token_count * per_token)
    one_hot = flattened[:, None] == jnp.arange(experts, dtype=jnp.int32)[None, :]
    route_ids = jnp.arange(token_count * per_token, dtype=jnp.int32)
    before = (route_ids[None, :] < route_ids[:, None]).astype(jnp.bfloat16)
    earlier = jnp.dot(before, one_hot.astype(jnp.bfloat16), preferred_element_type=jnp.float32)
    positions = jnp.sum(jnp.where(one_hot, earlier, 0.0), axis=1).astype(jnp.int32)
    return (flattened * capacity + positions).reshape(token_count, per_token)


def transposed_product(left, right):
    return lax.dot_general(
        left, right, (((0,), (0,)), ((), ())), preferred_element_type=jnp.float32
    )


def line_extent(count):
    bits = count.bit_length() - 1
    return 1 << -(-bits // 3)


def chunk_orders(extent):
    orders = []
    for own in range(extent):
        toward = [i for i in range(own + 1, extent)] if 2 * own < extent - 1 else [i for i in range(own - 1, -1, -1)]
        back = [i for i in range(extent) if i != own and i not in toward]
        back.sort(key=lambda i: abs(i - own))
        if own in (0, extent - 1):
            order = toward
        else:
            order = toward[:1] + back + toward[1:]
        orders.append([own] + order)
    return orders


def relay_orders(extent):
    return [
        sorted(
            (i for i in range(extent) if i != own),
            key=lambda i: (own if i > own else extent - 1 - own, abs(i - own)),
        )
        for own in range(extent)
    ]


def sum_orders(extent):
    return [
        sorted((i for i in range(extent) if i != own), key=lambda i: -abs(i - own)) + [own]
        for own in range(extent)
    ]


def sum_relays(extent):
    return [
        sorted(
            (i for i in range(extent) if i != own),
            key=lambda i: (own if i > own else extent - 1 - own, -abs(i - own)),
        )
        for own in range(extent)
    ]


def looked_up(table, row, column):
    value = jnp.int32(0)
    for i, entries in enumerate(table):
        for k, entry in enumerate(entries):
            value = value + jnp.where((row == i) & (column == k), entry, 0)
    return value


def routed_kernel(
    extent,
    plane,
    capacity,
    mid_hbm,
    cot_hbm,
    meta,
    gate_hbm,
    up_hbm,
    down_hbm,
    filtered_hbm,
    out_weight_hbm,
    taps,
    gain,
    proj_out,
    input_out,
    inputs_out,
    routed_out,
    hidden_out,
    gate_pre_out,
    up_pre_out,
    tok,
    metas,
    picks,
    rows,
    gate,
    up,
    down,
    pre_gate,
    pre_up,
    hidden,
    gate_pre,
    up_pre,
    part_sent,
    part_got,
    ret_sent,
    ret_got,
    line_sent,
    line_got,
    total,
    tokens,
    load_sem,
    meta_sems,
    tok_send,
    tok_recv,
    row_send,
    row_recv,
    swap_send,
    swap_recv,
    part_sems,
    ret_send,
    ret_recv,
    line_send,
    line_recv,
    out_sems,
    token_sems,
    values,
    out_weight,
    stats,
    normed,
    inverse,
    active,
    blocks,
    sums_sent,
    sums_got,
    sums_own,
    padded,
    spread,
    stat_sems,
    active_send,
    active_recv,
    block_send,
    block_recv,
    sums_send,
    sums_recv,
    halo_sems,
):
    sp, tp = lax.axis_index("sp"), lax.axis_index("tp")
    z, p = sp // plane, sp % plane
    slots = plane * capacity
    token_count, width = tok.shape[2], tok.shape[3]
    other = 1 - tp
    step = width // extent
    columns = extent
    orders, relays = chunk_orders(extent), relay_orders(extent)

    def remote(src, dst, send, recv, to_sp, to_tp):
        return pltpu.make_async_remote_copy(
            src_ref=src,
            dst_ref=dst,
            send_sem=send,
            recv_sem=recv,
            device_id=(to_sp, to_tp),
            device_id_type=MESH,
        )

    loads = [
        pltpu.make_async_copy(mid_hbm, tok.at[0, z], load_sem.at[0]),
        pltpu.make_async_copy(cot_hbm, tok.at[1, z], load_sem.at[1]),
        pltpu.make_async_copy(gate_hbm, gate, load_sem.at[2]),
        pltpu.make_async_copy(up_hbm, up, load_sem.at[3]),
        pltpu.make_async_copy(down_hbm, down, load_sem.at[4]),
        pltpu.make_async_copy(filtered_hbm, values, load_sem.at[5]),
        pltpu.make_async_copy(out_weight_hbm, out_weight, load_sem.at[6]),
    ]
    for load in loads:
        load.start()
    metas[z] = meta[...]

    barrier = pltpu.get_barrier_semaphore()

    def greet(to_sp, to_tp):
        pl.semaphore_signal(barrier, inc=1, device_id=(to_sp, to_tp), device_id_type=MESH)

    def line_peer(i):
        return lax.rem(z + i, extent)

    def plane_peer(i):
        return lax.rem(p + i, plane)

    for i in range(1, extent):
        greet(line_peer(i) * plane + p, tp)

    @pl.loop(1, plane)
    def _(i):
        greet(z * plane + plane_peer(i), tp)
        greet(z * plane + plane_peer(i), other)

    greet(sp, other)
    last_sp = extent * plane - 1

    @pl.when(sp > 0)
    def _():
        greet(sp - 1, tp)

    @pl.when(sp < last_sp)
    def _():
        greet(sp + 1, tp)

    ends = jnp.where(sp > 0, 1, 0) + jnp.where(sp < last_sp, 1, 0)
    pl.semaphore_wait(barrier, extent - 1 + 2 * (plane - 1) + 1 + ends)

    def meta_copy(to_z, from_z):
        return remote(
            meta, metas.at[from_z], meta_sems.at[0, to_z], meta_sems.at[1, from_z], to_z * plane + p, tp
        )

    def tok_copy(t, origin, up_way):
        to_z = z + 1 if up_way else z - 1
        return remote(
            tok.at[t, origin],
            tok.at[t, origin],
            tok_send.at[t, origin, int(up_way)],
            tok_recv.at[t, origin],
            to_z * plane + p,
            tp,
        )

    def forwards(origin, up_way):
        if up_way:
            return (origin <= z) & (z < extent - 1)
        return (origin >= z) & (z > 0)

    def row_copy(t, origin, q):
        return remote(
            picks.at[t, origin, q],
            rows.at[t, origin, 0, p],
            row_send.at[t, origin, q],
            row_recv.at[t, origin, p],
            z * plane + q,
            tp,
        )

    def row_arrival(t, origin, q):
        return remote(
            picks.at[t, origin, q],
            rows.at[t, origin, 0, q],
            row_send.at[t, origin, q],
            row_recv.at[t, origin, q],
            z * plane + q,
            tp,
        )

    def swap_copy(t, origin):
        return remote(
            rows.at[t, origin, 0],
            rows.at[t, origin, 1],
            swap_send.at[t, origin],
            swap_recv.at[t, origin],
            sp,
            other,
        )

    def part_copy(origin):
        return remote(
            part_sent.at[origin],
            part_got.at[origin],
            part_sems.at[0, origin],
            part_sems.at[1, origin],
            sp,
            other,
        )

    def ret_copy(origin, q):
        return remote(
            ret_sent.at[origin, q],
            ret_got.at[origin, p],
            ret_send.at[origin, q],
            ret_recv.at[origin, p],
            z * plane + q,
            tp,
        )

    def ret_arrival(origin, q):
        return remote(
            ret_sent.at[origin, q],
            ret_got.at[origin, q],
            ret_send.at[origin, q],
            ret_recv.at[origin, q],
            z * plane + q,
            tp,
        )

    def band(j):
        return pl.ds(j * step, step)

    def line_copy(home, j):
        to_z = jnp.where(home > z, z + 1, z - 1)
        slot = jnp.where((home < z) & (to_z == home), extent, home)
        return remote(
            line_sent.at[home, :, band(j)],
            line_got.at[slot, :, band(j)],
            line_send.at[home, j],
            line_recv.at[slot, j],
            to_z * plane + p,
            tp,
        )

    def line_arrival(slot, j):
        return remote(
            line_sent.at[0, :, band(j)],
            line_got.at[slot, :, band(j)],
            line_send.at[0, j],
            line_recv.at[slot, j],
            z * plane + p,
            other,
        )

    def has_inflow(home):
        return ((home > z) & (z > 0)) | ((home < z) & (z < extent - 1))

    def hits(origin):
        slot = lax.broadcasted_iota(jnp.int32, (slots, token_count), 0) + z * slots
        slot = slot.astype(jnp.float32)
        return [slot == metas[origin, pl.ds(k, 1), :] for k in range(TOPK_ROWS)]

    def chooser(origin):
        first, second = hits(origin)
        return jnp.where(first | second, 1.0, 0.0).astype(jnp.bfloat16)

    def scale_of(origin):
        first, second = hits(origin)
        weighted = jnp.where(first, metas[origin, pl.ds(TOPK_ROWS, 1), :], 0.0) + jnp.where(
            second, metas[origin, pl.ds(TOPK_ROWS + 1, 1), :], 0.0
        )
        return jnp.sum(weighted, axis=1, keepdims=True)

    def arrive(t, k):
        origin = looked_up(orders, z, k)

        @pl.when(k > 0)
        def _():
            tok_copy(t, origin, True).wait_recv()
            if t == 0:
                meta_copy(origin, origin).wait_recv()

        for up_way in (False, True):

            @pl.when(forwards(origin, up_way))
            def _():
                tok_copy(t, origin, up_way).start()

        select = chooser(origin)
        if t == 1:
            scale = scale_of(origin)
        for j in range(columns):
            picked = jnp.dot(
                select, tok[t, origin, :, band(j)], preferred_element_type=jnp.float32
            )
            if t == 1:
                picked = scale * picked
            picks[t, origin, :, :, band(j)] = picked.astype(jnp.bfloat16).reshape(
                plane, capacity, step
            )

        @pl.loop(1, plane)
        def _(i):
            row_copy(t, origin, plane_peer(i)).start()

        rows[t, origin, 0, p] = picks[t, origin, p]

    def swap(t, k):
        origin = looked_up(orders, z, k)

        @pl.loop(1, plane)
        def _(i):
            row_arrival(t, origin, plane_peer(i)).wait_recv()

        swap_copy(t, origin).start()

    def expert_rows(t, origin):
        return rows[t, origin].reshape(2 * slots, width)

    half = gate.shape[1]
    tile = min(256, half)

    def first_products(k):
        origin = looked_up(orders, z, k)

        @pl.when(k == 0)
        def _():
            loads[2].wait()
            loads[3].wait()

        swap_copy(0, origin).wait_recv()

        @pl.loop(0, half // tile)
        def _(n):
            cut = pl.ds(pl.multiple_of(n * tile, tile), tile)
            block = expert_rows(0, origin)
            pre_gate[:, cut] = jnp.dot(block, gate[:, cut], preferred_element_type=jnp.float32)
            pre_up[:, cut] = jnp.dot(block, up[:, cut], preferred_element_type=jnp.float32)

    def products(k):
        origin = looked_up(orders, z, k)

        @pl.when(k == 0)
        def _():
            loads[4].wait()

        swap_copy(1, origin).wait_recv()

        @pl.loop(0, half // tile)
        def _(n):
            cut = pl.ds(pl.multiple_of(n * tile, tile), tile)
            hidden_grad = lax.dot_general(
                expert_rows(1, origin),
                down[cut, :],
                (((1,), (1,)), ((), ())),
                preferred_element_type=jnp.float32,
            )
            g, u = pre_gate[:, cut], pre_up[:, cut]
            logistic = jax.nn.sigmoid(g)
            gate_act = g * logistic
            hidden[origin, :, cut] = (gate_act * u).astype(jnp.bfloat16)
            gate_pre[origin, :, cut] = (
                hidden_grad * u * (logistic * (1.0 + g * (1.0 - logistic)))
            ).astype(jnp.bfloat16)
            up_pre[origin, :, cut] = (hidden_grad * gate_act).astype(jnp.bfloat16)

        wide = min(256, width)

        @pl.loop(0, width // wide)
        def _(n):
            cut = pl.ds(pl.multiple_of(n * wide, wide), wide)
            part = lax.dot_general(
                gate_pre[origin],
                gate[cut, :],
                (((1,), (1,)), ((), ())),
                preferred_element_type=jnp.float32,
            ) + lax.dot_general(
                up_pre[origin],
                up[cut, :],
                (((1,), (1,)), ((), ())),
                preferred_element_type=jnp.float32,
            )
            part = part.astype(jnp.bfloat16).reshape(2, plane, capacity, wide)
            ret_sent[origin, :, :, cut] = part[0]
            part_sent[origin, :, :, cut] = part[1]

        part_copy(origin).start()
        for out in results(origin):
            out.start()

    def results(origin):
        pairs = [
            (rows.at[0, origin], inputs_out.at[origin]),
            (rows.at[1, origin], routed_out.at[origin]),
            (hidden.at[origin], hidden_out.at[origin]),
            (gate_pre.at[origin], gate_pre_out.at[origin]),
            (up_pre.at[origin], up_pre_out.at[origin]),
        ]
        return [
            pltpu.make_async_copy(src, dst, out_sems.at[i, origin])
            for i, (src, dst) in enumerate(pairs)
        ]

    def send_back(k):
        origin = looked_up(orders, z, k)
        part_copy(origin).wait_recv()
        for j in range(columns):
            both = ret_sent[origin, :, :, band(j)].astype(jnp.float32) + part_got[
                origin, :, :, band(j)
            ].astype(jnp.float32)
            ret_sent[origin, :, :, band(j)] = both.astype(jnp.bfloat16)

        @pl.loop(1, plane)
        def _(i):
            ret_copy(origin, plane_peer(i)).start()

        ret_got[origin, p] = ret_sent[origin, p]

    def combine(k):
        origin = looked_up(orders, z, k)

        @pl.loop(1, plane)
        def _(i):
            ret_arrival(origin, plane_peer(i)).wait_recv()

        select = chooser(origin)
        for j in range(columns):
            back = ret_got[origin, :, :, band(j)].reshape(slots, step)
            added = lax.dot_general(
                select, back, (((0,), (0,)), ((), ())), preferred_element_type=jnp.float32
            )

            @pl.when(origin == z)
            def _():
                total[:, band(j)] = added

            @pl.when(origin != z)
            def _():
                line_sent[origin, :, band(j)] = added.astype(jnp.bfloat16)

            @pl.when((origin != z) & jnp.logical_not(has_inflow(origin)))
            def _():
                line_copy(origin, j).start()

    for load in loads[:2]:
        load.wait()
    for i in range(1, extent):
        meta_copy(line_peer(i), z).start()

    local = values.shape[1]
    strip = min(256, local)
    strips = local // strip
    row_count = values.shape[0]

    def strip_at(n):
        return pl.ds(pl.multiple_of(n * strip, strip), strip)

    def stat_copy(i):
        return remote(
            stats.at[i, 0], stats.at[i, 1], stat_sems.at[0, i], stat_sems.at[1, i], sp, other
        )

    def paired(i, first, second):
        lane = lax.broadcasted_iota(jnp.int32, (row_count, stats.shape[3]), 1)
        stats[i, 0] = jnp.where(lane == 0, first, second)
        stat_copy(i).start()

    def both_sums(i):
        stat_copy(i).wait_recv()
        merged = (stats[i, 0] + stats[i, 1]) / width
        return merged[:, 0:1], merged[:, 1:2]

    def active_copy(q):
        return remote(
            active.at[p], active.at[p], active_send.at[q], active_recv.at[p], z * plane + q, tp
        )

    def active_arrival(q):
        return remote(
            active.at[q], active.at[q], active_send.at[q], active_recv.at[q], z * plane + q, tp
        )

    def prepare():
        loads[5].wait()
        sums = jnp.zeros((row_count, 1), jnp.float32)
        squares = jnp.zeros((row_count, 1), jnp.float32)
        for n in range(strips):
            block = values[:, n * strip : (n + 1) * strip].astype(jnp.float32)
            sums = sums + jnp.sum(block, axis=1, keepdims=True)
            squares = squares + jnp.sum(block * block, axis=1, keepdims=True)
        paired(0, sums, squares)
        average, second = both_sums(0)
        scale = lax.rsqrt(second - average * average + NORM_EPS)
        inverse[...] = jnp.broadcast_to(scale, inverse.shape)
        for n in range(strips):
            cut = slice(n * strip, (n + 1) * strip)
            flat = (values[:, cut].astype(jnp.float32) - average) * scale
            normed[:, cut] = flat
            scaled = flat * gain[:, cut]
            active[p, :, cut] = (scaled * jax.nn.sigmoid(scaled)).astype(jnp.bfloat16)

        @pl.loop(1, plane)
        def _(i):
            active_copy(plane_peer(i)).start()

    arrive(0, 0)
    prepare()

    @pl.loop(0, extent)
    def _(k):
        arrive(1, k)
        swap(0, k)
        first_products(k)

        @pl.when(k > 0)
        def _():
            combine(k - 1)

        swap(1, k)

        @pl.when(k < extent - 1)
        def _():
            arrive(0, k + 1)

        products(k)
        send_back(k)

    combine(extent - 1)

    @pl.loop(0, extent - 1)
    def _(k):
        home = looked_up(relays, z, k)

        @pl.when(has_inflow(home))
        def _():
            for j in range(columns):
                line_arrival(home, j).wait_recv()
                line_sent[home, :, band(j)] = (
                    line_sent[home, :, band(j)].astype(jnp.float32)
                    + line_got[home, :, band(j)].astype(jnp.float32)
                ).astype(jnp.bfloat16)
                line_copy(home, j).start()

    own_block = width // (extent * plane)
    lanes = blocks.shape[4]

    def block_at(j, q):
        start = (j * plane + q) * own_block
        return pl.ds(pl.multiple_of(start // lanes * lanes, lanes), lanes)

    def token_copy(j):
        return remote(
            tokens.at[tp, :, band(j)],
            tokens.at[tp, :, band(j)],
            token_sems.at[0, j],
            token_sems.at[1, j],
            sp,
            other,
        )

    def token_arrival(j):
        return remote(
            tokens.at[other, :, band(j)],
            tokens.at[other, :, band(j)],
            token_sems.at[0, j],
            token_sems.at[1, j],
            sp,
            other,
        )

    def block_copy(j, q, to_tp):
        return remote(
            tokens.at[tp, :, block_at(j, q)],
            blocks.at[j, p, tp],
            block_send.at[j, q, to_tp],
            block_recv.at[j, p, tp],
            z * plane + q,
            to_tp,
        )

    def block_arrival(j, q, from_tp):
        return remote(
            tokens.at[tp, :, block_at(j, q)],
            blocks.at[j, q, from_tp],
            block_send.at[j, q, from_tp],
            block_recv.at[j, q, from_tp],
            z * plane + q,
            from_tp,
        )

    for j in range(columns):
        for slot, there in ((z, z > 0), (extent, z < extent - 1)):

            @pl.when(there)
            def _():
                line_arrival(slot, j).wait_recv()
                total[:, band(j)] = total[:, band(j)] + line_got[slot, :, band(j)].astype(
                    jnp.float32
                )

        tokens[tp, :, band(j)] = (
            tok[1, z, :, band(j)].astype(jnp.float32) + total[:, band(j)]
        ).astype(jnp.bfloat16)

        @pl.loop(1, plane)
        def _(i):
            for to_tp in range(2):
                block_copy(j, plane_peer(i), to_tp).start()

        token_copy(j).start()

    pieces = 2
    piece = local // pieces

    def piece_at(h):
        return pl.ds(h * piece, piece)

    def sums_copy(j, h):
        to_z = jnp.where(j > z, z + 1, z - 1)
        slot = jnp.where((j < z) & (to_z == j), extent, j)
        return remote(
            sums_sent.at[j, :, piece_at(h)],
            sums_got.at[slot, :, piece_at(h)],
            sums_send.at[j, h],
            sums_recv.at[slot, h],
            to_z * plane + p,
            tp,
        )

    def sums_arrival(slot, h):
        return remote(
            sums_sent.at[0, :, piece_at(h)],
            sums_got.at[slot, :, piece_at(h)],
            sums_send.at[0, h],
            sums_recv.at[slot, h],
            sp,
            other,
        )

    @pl.loop(1, plane)
    def _(i):
        active_arrival(plane_peer(i)).wait_recv()

    @pl.loop(0, extent)
    def _(k):
        j = looked_up(sum_orders(extent), z, k)

        @pl.loop(1, plane)
        def _(i):
            for from_tp in range(2):
                block_arrival(j, plane_peer(i), from_tp).wait_recv()

        token_arrival(j).wait_recv()
        for half_at in range(2):
            blocks[j, p, half_at] = tokens[half_at, :, block_at(j, p)]
        for n in range(strips):
            cut = slice(n * strip, (n + 1) * strip)
            spread[:lanes, cut] = lax.dot_general(
                blocks[j].reshape(plane * row_count, lanes),
                active[:, :, cut].reshape(plane * row_count, strip),
                (((0,), (0,)), ((), ())),
                preferred_element_type=jnp.float32,
            )
        start = lax.rem((j * plane + p) * own_block, lanes)
        mine = spread[pl.ds(pl.multiple_of(start, own_block), own_block), :]

        @pl.when(j == z)
        def _():
            sums_own[...] = mine

        @pl.when(j != z)
        def _():
            sums_sent[j] = mine.astype(jnp.bfloat16)

        @pl.when((j != z) & jnp.logical_not(has_inflow(j)))
        def _():
            for h in range(pieces):
                sums_copy(j, h).start()

    def relay(k):
        j = looked_up(sum_relays(extent), z, k)

        @pl.when(has_inflow(j))
        def _():
            for h in range(pieces):
                sums_arrival(j, h).wait_recv()
                sums_sent[j, :, piece_at(h)] = (
                    sums_sent[j, :, piece_at(h)].astype(jnp.float32)
                    + sums_got[j, :, piece_at(h)].astype(jnp.float32)
                ).astype(jnp.bfloat16)
                sums_copy(j, h).start()

    loads[6].wait()
    grad_sum = jnp.zeros((row_count, 1), jnp.float32)
    grad_corr = jnp.zeros((row_count, 1), jnp.float32)
    for n in range(strips):
        cut = slice(n * strip, (n + 1) * strip)
        act_grad = lax.dot_general(
            tokens[...].reshape(row_count, width),
            out_weight[cut, :],
            (((1,), (1,)), ((), ())),
            preferred_element_type=jnp.float32,
        )
        flat = normed[:, cut]
        weight = gain[:, cut]
        scaled = flat * weight
        logistic = jax.nn.sigmoid(scaled)
        slope = act_grad * (logistic * (1.0 + scaled * (1.0 - logistic))) * weight
        spread[:row_count, cut] = slope
        grad_sum = grad_sum + jnp.sum(slope, axis=1, keepdims=True)
        grad_corr = grad_corr + jnp.sum(slope * flat, axis=1, keepdims=True)
    paired(1, grad_sum, grad_corr)
    near_relays = max(0, extent - 1 - 1)
    for k in range(near_relays):
        relay(k)
    mean, corr = both_sums(1)
    edge = (padded.shape[0] - row_count) // 2
    scale = inverse[:, 0:1]
    for n in range(strips):
        cut = slice(n * strip, (n + 1) * strip)
        padded[edge : edge + row_count, cut] = (
            scale * (spread[:row_count, cut] - mean - normed[:, cut] * corr)
        ).astype(jnp.bfloat16)

    def halo_copy(up_way):
        if up_way:
            src, dst, to = row_count, 0, sp + 1
        else:
            src, dst, to = edge, edge + row_count, sp - 1
        return remote(
            padded.at[pl.ds(src, edge), :],
            padded.at[pl.ds(dst, edge), :],
            halo_sems.at[0, int(up_way)],
            halo_sems.at[1, int(up_way)],
            to,
            tp,
        )

    inside = {True: sp < last_sp, False: sp > 0}
    for up_way in (True, False):

        @pl.when(inside[up_way])
        def _():
            halo_copy(up_way).start()

    for k in range(near_relays, extent - 1):
        relay(k)

    for up_way in (True, False):
        at = 0 if up_way else edge + row_count

        @pl.when(inside[not up_way])
        def _():
            halo_copy(up_way).wait_recv()

        @pl.when(jnp.logical_not(inside[not up_way]))
        def _():
            padded[at : at + edge, :] = jnp.zeros((edge, local), jnp.bfloat16)

    tap_count = taps.shape[0]
    reach = tap_count // 2
    narrow = min(128, local)
    spread[...] = padded[...].astype(jnp.float32)
    depth = (edge + reach) // 8 * 8 + row_count

    @pl.loop(0, local // narrow)
    def _(n):
        cut = pl.ds(pl.multiple_of(n * narrow, narrow), narrow)
        acc = jnp.zeros((row_count, narrow), jnp.float32)
        for s in range(8):
            picks_at = [o for o in range(tap_count) if (edge + reach - o) % 8 == s]
            if not picks_at:
                continue
            shifted = spread[s : s + depth, cut]
            for o in picks_at:
                m = (edge + reach - o) // 8 * 8
                acc = acc + taps[o : o + 1, cut] * shifted[m : m + row_count]
        values[:, cut] = acc.astype(jnp.bfloat16)

    finish = pltpu.make_async_copy(values, input_out, load_sem.at[0])
    finish.start()
    for h in range(pieces):
        for slot, there in ((z, z > 0), (extent, z < extent - 1)):

            @pl.when(there)
            def _():
                sums_arrival(slot, h).wait_recv()
                sums_own[:, piece_at(h)] = sums_own[:, piece_at(h)] + sums_got[
                    slot, :, piece_at(h)
                ].astype(jnp.float32)

    store = pltpu.make_async_copy(sums_own, proj_out, load_sem.at[1])
    store.start()
    for i in range(2):
        stat_copy(i).wait_send()
    for up_way in (True, False):

        @pl.when(inside[up_way])
        def _():
            halo_copy(up_way).wait_send()

    @pl.loop(1, plane)
    def _(i):
        active_copy(plane_peer(i)).wait_send()

    for j in range(columns):
        token_copy(j).wait_send()

        @pl.loop(1, plane)
        def _(i):
            for to_tp in range(2):
                block_copy(j, plane_peer(i), to_tp).wait_send()

        @pl.when(z != j)
        def _():
            for h in range(pieces):
                sums_copy(j, h).wait_send()

    for i in range(1, extent):
        meta_copy(line_peer(i), z).wait_send()

    @pl.loop(0, extent)
    def _(origin):
        for t in range(2):
            for up_way in (False, True):

                @pl.when(forwards(origin, up_way))
                def _():
                    tok_copy(t, origin, up_way).wait_send()

            @pl.loop(1, plane)
            def _(i):
                row_copy(t, origin, plane_peer(i)).wait_send()

            swap_copy(t, origin).wait_send()
        part_copy(origin).wait_send()

        @pl.loop(1, plane)
        def _(i):
            ret_copy(origin, plane_peer(i)).wait_send()

        @pl.when(origin != z)
        def _():
            for j in range(columns):
                line_copy(origin, j).wait_send()

        for out in results(origin):
            out.wait()

    finish.wait()
    store.wait()


TOPK_ROWS = 2


def routed_backward(
    mid_rows,
    cotangent,
    meta,
    gate_mat,
    up_mat,
    down_mat,
    filtered,
    out_weight,
    taps,
    gain,
    capacity,
):
    sp_count = lax.axis_size("sp")
    extent = line_extent(sp_count)
    plane = sp_count // extent
    token_count, width = mid_rows.shape
    half = gate_mat.shape[1]
    slots = plane * capacity
    kind = jnp.bfloat16
    any_space = pl.BlockSpec(memory_space=pl.ANY)
    vmem = pl.BlockSpec(memory_space=pltpu.VMEM)
    dma = pltpu.SemaphoreType.DMA
    columns = extent
    row_count, local = filtered.shape
    own_block = width // sp_count
    lanes = min(max(own_block, 128), width // extent)
    edge = -(-(taps.shape[0] // 2) // 16) * 16
    rows_shape = (extent, 2, plane, capacity, width)
    small_shape = (extent, 2 * slots, half)
    scratch = [
        pltpu.VMEM((2, extent, token_count, width), kind),
        pltpu.VMEM((extent,) + meta.shape, jnp.float32),
        pltpu.VMEM((2, extent, plane, capacity, width), kind),
        pltpu.VMEM((2,) + rows_shape, kind),
        pltpu.VMEM(gate_mat.shape, kind),
        pltpu.VMEM(up_mat.shape, kind),
        pltpu.VMEM(down_mat.shape, kind),
        pltpu.VMEM((2 * slots, half), jnp.float32),
        pltpu.VMEM((2 * slots, half), jnp.float32),
        pltpu.VMEM(small_shape, kind),
        pltpu.VMEM(small_shape, kind),
        pltpu.VMEM(small_shape, kind),
        pltpu.VMEM((extent, plane, capacity, width), kind),
        pltpu.VMEM((extent, plane, capacity, width), kind),
        pltpu.VMEM((extent, plane, capacity, width), kind),
        pltpu.VMEM((extent, plane, capacity, width), kind),
        pltpu.VMEM((extent, token_count, width), kind),
        pltpu.VMEM((extent + 1, token_count, width), kind),
        pltpu.VMEM((token_count, width), jnp.float32),
        pltpu.VMEM((2, token_count, width), kind),
        dma((7,)),
        dma((2, extent)),
        dma((2, extent, 2)),
        dma((2, extent)),
        dma((2, extent, plane)),
        dma((2, extent, plane)),
        dma((2, extent)),
        dma((2, extent)),
        dma((2, extent)),
        dma((extent, plane)),
        dma((extent, plane)),
        dma((extent, columns)),
        dma((extent + 1, columns)),
        dma((5, extent)),
        dma((2, columns)),
        pltpu.VMEM((row_count, local), kind),
        pltpu.VMEM(out_weight.shape, kind),
        pltpu.VMEM((2, 2, row_count, 128), jnp.float32),
        pltpu.VMEM((row_count, local), jnp.float32),
        pltpu.VMEM((row_count, 128), jnp.float32),
        pltpu.VMEM((plane, row_count, local), kind),
        pltpu.VMEM((extent, plane, 2, token_count, lanes), kind),
        pltpu.VMEM((extent, own_block, local), kind),
        pltpu.VMEM((extent + 1, own_block, local), kind),
        pltpu.VMEM((own_block, local), jnp.float32),
        pltpu.VMEM((row_count + 2 * edge, local), kind),
        pltpu.VMEM((row_count + 2 * edge, local), jnp.float32),
        dma((2, 2)),
        dma((plane,)),
        dma((plane,)),
        dma((extent, plane, 2)),
        dma((extent, plane, 2)),
        dma((extent, 2)),
        dma((extent + 1, 2)),
        dma((2, 2)),
    ]
    held = sum(
        math.prod(s.shape) * jnp.dtype(s.dtype).itemsize
        for s in scratch
        if s.memory_space == pltpu.VMEM
    )
    out = pl.pallas_call(
        functools.partial(routed_kernel, extent, plane, capacity),
        out_shape=[
            jax.ShapeDtypeStruct((own_block, local), jnp.float32),
            jax.ShapeDtypeStruct((row_count, local), kind),
            jax.ShapeDtypeStruct(rows_shape, kind),
            jax.ShapeDtypeStruct(rows_shape, kind),
            jax.ShapeDtypeStruct(small_shape, kind),
            jax.ShapeDtypeStruct(small_shape, kind),
            jax.ShapeDtypeStruct(small_shape, kind),
        ],
        in_specs=[any_space] * 2 + [vmem] + [any_space] * 5 + [vmem] * 2,
        out_specs=[any_space] * 7,
        scratch_shapes=scratch,
        compiler_params=pltpu.CompilerParams(
            collective_id=0, has_side_effects=True, vmem_limit_bytes=min(held + SPARE, 67_043_328)
        ),
    )(
        mid_rows, cotangent, meta, gate_mat, up_mat, down_mat, filtered, out_weight, taps, gain
    )
    proj_grad, input_grad, inputs, routed, hidden, gate_pre, up_pre = out
    every = 2 * slots * extent
    return (
        proj_grad,
        input_grad,
        inputs.reshape(every, width),
        routed.reshape(every, width),
        hidden.reshape(every, half),
        gate_pre.reshape(every, half),
        up_pre.reshape(every, half),
    )


def per_device(
    mid_rows,
    cotangent,
    routes,
    route_weight,
    filtered,
    conv_taps,
    norm_gain,
    out_weight,
    gate_weight,
    up_weight,
    down_weight,
):
    sp_count = lax.axis_size("sp")
    token_count, model_width = mid_rows.shape
    per_token = routes.shape[1]
    local_experts = gate_weight.shape[0]
    experts = local_experts * sp_count
    capacity = 2 * token_count * per_token // sp_count
    target = slot_targets(routes, experts, capacity).astype(jnp.float32)
    meta = jnp.concatenate([target.T, route_weight.T], axis=0)
    meta = jnp.pad(meta, ((0, 8 - meta.shape[0]), (0, 0)))
    proj_grad, input_grad, inputs, routed, hidden, gate_pre, up_pre = routed_backward(
        mid_rows,
        cotangent,
        meta,
        gate_weight[0],
        up_weight[0],
        down_weight[0],
        filtered,
        out_weight,
        conv_taps,
        norm_gain[None],
        capacity,
    )
    gate_grad = transposed_product(inputs, gate_pre)[None]
    up_grad = transposed_product(inputs, up_pre)[None]
    down_grad = transposed_product(hidden, routed)[None]
    return (gate_grad, up_grad, down_grad, proj_grad, input_grad)


def solution(mesh):
    in_specs = (
        P(("sp", "tp"), None),
        P(("sp", "tp"), None),
        P(("sp", "tp"), None),
        P(("sp", "tp"), None),
        P("sp", "tp"),
        P(None, "tp"),
        P("tp"),
        P("tp", None),
        P("sp", None, "tp"),
        P("sp", None, "tp"),
        P("sp", "tp", None),
    )
    out_specs = (
        P("sp", None, "tp"),
        P("sp", None, "tp"),
        P("sp", "tp", None),
        P("sp", "tp"),
        P("sp", "tp"),
    )
    return jax.shard_map(
        per_device, mesh=mesh, in_specs=in_specs, out_specs=out_specs, check_vma=False
    )
```

```python
import functools
import math

import jax
import jax.numpy as jnp
from jax import lax
from jax.experimental import pallas as pl
from jax.experimental.pallas import tpu as pltpu
from jax.sharding import PartitionSpec as P

MESH = pl.DeviceIdType.MESH
NORM_EPS = 1e-05
SPARE = 4 << 20


def slot_targets(routes, experts, capacity):
    token_count, per_token = routes.shape
    flattened = routes.reshape(token_count * per_token)
    one_hot = flattened[:, None] == jnp.arange(experts, dtype=jnp.int32)[None, :]
    route_ids = jnp.arange(token_count * per_token, dtype=jnp.int32)
    before = (route_ids[None, :] < route_ids[:, None]).astype(jnp.bfloat16)
    earlier = jnp.dot(before, one_hot.astype(jnp.bfloat16), preferred_element_type=jnp.float32)
    positions = jnp.sum(jnp.where(one_hot, earlier, 0.0), axis=1).astype(jnp.int32)
    return (flattened * capacity + positions).reshape(token_count, per_token)


def transposed_product(left, right):
    return lax.dot_general(
        left, right, (((0,), (0,)), ((), ())), preferred_element_type=jnp.float32
    )


def line_extent(count):
    bits = count.bit_length() - 1
    return 1 << -(-bits // 3)


def chunk_orders(extent):
    orders = []
    for own in range(extent):
        toward = [i for i in range(own + 1, extent)] if 2 * own < extent - 1 else [i for i in range(own - 1, -1, -1)]
        back = [i for i in range(extent) if i != own and i not in toward]
        back.sort(key=lambda i: abs(i - own))
        if own in (0, extent - 1):
            order = toward[1:] + toward[:1]
        else:
            order = toward[:1] + back + toward[1:]
        orders.append([own] + order)
    return orders


def relay_orders(extent):
    return [
        sorted(
            (i for i in range(extent) if i != own),
            key=lambda i: (own if i > own else extent - 1 - own, abs(i - own)),
        )
        for own in range(extent)
    ]


def sum_orders(extent):
    return [
        sorted((i for i in range(extent) if i != own), key=lambda i: -abs(i - own)) + [own]
        for own in range(extent)
    ]


def sum_relays(extent):
    return [
        sorted(
            (i for i in range(extent) if i != own),
            key=lambda i: (own if i > own else extent - 1 - own, -abs(i - own)),
        )
        for own in range(extent)
    ]


def looked_up(table, row, column):
    value = jnp.int32(0)
    for i, entries in enumerate(table):
        for k, entry in enumerate(entries):
            value = value + jnp.where((row == i) & (column == k), entry, 0)
    return value


def routed_kernel(
    extent,
    plane,
    capacity,
    mid_hbm,
    cot_hbm,
    meta,
    gate_hbm,
    up_hbm,
    down_hbm,
    filtered_hbm,
    out_weight_hbm,
    taps,
    gain,
    proj_out,
    input_out,
    inputs_out,
    routed_out,
    hidden_out,
    gate_pre_out,
    up_pre_out,
    tok,
    metas,
    picks,
    rows,
    gate,
    up,
    down,
    pre_gate,
    pre_up,
    hidden,
    gate_pre,
    up_pre,
    part_sent,
    part_got,
    ret_sent,
    ret_got,
    line_sent,
    line_got,
    total,
    tokens,
    load_sem,
    meta_sems,
    tok_send,
    tok_recv,
    row_send,
    row_recv,
    swap_send,
    swap_recv,
    part_sems,
    ret_send,
    ret_recv,
    line_send,
    line_recv,
    out_sems,
    token_sems,
    values,
    out_weight,
    stats,
    normed,
    inverse,
    active,
    blocks,
    sums_sent,
    sums_got,
    sums_own,
    padded,
    spread,
    stat_sems,
    active_send,
    active_recv,
    block_send,
    block_recv,
    block_swaps,
    sums_send,
    sums_recv,
    halo_sems,
):
    sp, tp = lax.axis_index("sp"), lax.axis_index("tp")
    z, p = sp // plane, sp % plane
    slots = plane * capacity
    token_count, width = tok.shape[2], tok.shape[3]
    other = 1 - tp
    step = width // extent
    columns = extent
    orders, relays = chunk_orders(extent), relay_orders(extent)

    def remote(src, dst, send, recv, to_sp, to_tp):
        return pltpu.make_async_remote_copy(
            src_ref=src,
            dst_ref=dst,
            send_sem=send,
            recv_sem=recv,
            device_id=(to_sp, to_tp),
            device_id_type=MESH,
        )

    loads = [
        pltpu.make_async_copy(mid_hbm, tok.at[0, z], load_sem.at[0]),
        pltpu.make_async_copy(cot_hbm, tok.at[1, z], load_sem.at[1]),
        pltpu.make_async_copy(gate_hbm, gate, load_sem.at[2]),
        pltpu.make_async_copy(up_hbm, up, load_sem.at[3]),
        pltpu.make_async_copy(down_hbm, down, load_sem.at[4]),
        pltpu.make_async_copy(filtered_hbm, values, load_sem.at[5]),
        pltpu.make_async_copy(out_weight_hbm, out_weight, load_sem.at[6]),
    ]
    for load in loads:
        load.start()
    metas[z] = meta[...]

    barrier = pltpu.get_barrier_semaphore()

    def greet(to_sp, to_tp):
        pl.semaphore_signal(barrier, inc=1, device_id=(to_sp, to_tp), device_id_type=MESH)

    def line_peer(i):
        return lax.rem(z + i, extent)

    def plane_peer(i):
        return lax.rem(p + i, plane)

    for i in range(1, extent):
        greet(line_peer(i) * plane + p, tp)

    @pl.loop(1, plane)
    def _(i):
        greet(z * plane + plane_peer(i), tp)

    greet(sp, other)
    last_sp = extent * plane - 1

    @pl.when(sp > 0)
    def _():
        greet(sp - 1, tp)

    @pl.when(sp < last_sp)
    def _():
        greet(sp + 1, tp)

    ends = jnp.where(sp > 0, 1, 0) + jnp.where(sp < last_sp, 1, 0)
    pl.semaphore_wait(barrier, extent - 1 + plane - 1 + 1 + ends)

    def meta_copy(to_z, from_z):
        return remote(
            meta, metas.at[from_z], meta_sems.at[0, to_z], meta_sems.at[1, from_z], to_z * plane + p, tp
        )

    def tok_copy(t, origin, up_way):
        to_z = z + 1 if up_way else z - 1
        return remote(
            tok.at[t, origin],
            tok.at[t, origin],
            tok_send.at[t, origin, int(up_way)],
            tok_recv.at[t, origin],
            to_z * plane + p,
            tp,
        )

    def forwards(origin, up_way):
        if up_way:
            return (origin <= z) & (z < extent - 1)
        return (origin >= z) & (z > 0)

    def row_copy(t, origin, q):
        return remote(
            picks.at[t, origin, q],
            rows.at[t, origin, 0, p],
            row_send.at[t, origin, q],
            row_recv.at[t, origin, p],
            z * plane + q,
            tp,
        )

    def row_arrival(t, origin, q):
        return remote(
            picks.at[t, origin, q],
            rows.at[t, origin, 0, q],
            row_send.at[t, origin, q],
            row_recv.at[t, origin, q],
            z * plane + q,
            tp,
        )

    def swap_copy(t, origin):
        return remote(
            rows.at[t, origin, 0],
            rows.at[t, origin, 1],
            swap_send.at[t, origin],
            swap_recv.at[t, origin],
            sp,
            other,
        )

    def part_copy(origin):
        return remote(
            part_sent.at[origin],
            part_got.at[origin],
            part_sems.at[0, origin],
            part_sems.at[1, origin],
            sp,
            other,
        )

    def ret_copy(origin, q):
        return remote(
            ret_sent.at[origin, q],
            ret_got.at[origin, p],
            ret_send.at[origin, q],
            ret_recv.at[origin, p],
            z * plane + q,
            tp,
        )

    def ret_arrival(origin, q):
        return remote(
            ret_sent.at[origin, q],
            ret_got.at[origin, q],
            ret_send.at[origin, q],
            ret_recv.at[origin, q],
            z * plane + q,
            tp,
        )

    def band(j):
        return pl.ds(j * step, step)

    def line_copy(home, j):
        to_z = jnp.where(home > z, z + 1, z - 1)
        slot = jnp.where((home < z) & (to_z == home), extent, home)
        return remote(
            line_sent.at[home, :, band(j)],
            line_got.at[slot, :, band(j)],
            line_send.at[home, j],
            line_recv.at[slot, j],
            to_z * plane + p,
            tp,
        )

    def line_arrival(slot, j):
        return remote(
            line_sent.at[0, :, band(j)],
            line_got.at[slot, :, band(j)],
            line_send.at[0, j],
            line_recv.at[slot, j],
            z * plane + p,
            other,
        )

    def has_inflow(home):
        return ((home > z) & (z > 0)) | ((home < z) & (z < extent - 1))

    def hits(origin):
        slot = lax.broadcasted_iota(jnp.int32, (slots, token_count), 0) + z * slots
        slot = slot.astype(jnp.float32)
        return [slot == metas[origin, pl.ds(k, 1), :] for k in range(TOPK_ROWS)]

    def chooser(origin):
        first, second = hits(origin)
        return jnp.where(first | second, 1.0, 0.0).astype(jnp.bfloat16)

    def scale_of(origin):
        first, second = hits(origin)
        weighted = jnp.where(first, metas[origin, pl.ds(TOPK_ROWS, 1), :], 0.0) + jnp.where(
            second, metas[origin, pl.ds(TOPK_ROWS + 1, 1), :], 0.0
        )
        return jnp.sum(weighted, axis=1, keepdims=True)

    def late(up_way):
        if extent < 3:
            return False
        return (z == extent - 2) if up_way else (z == 1)

    def send_own(t, held_back):
        for up_way in (False, True):
            now = forwards(z, up_way)
            if t == 1 and extent > 2:
                now = now & (late(up_way) == held_back)
            elif held_back:
                continue

            @pl.when(now)
            def _():
                tok_copy(t, z, up_way).start()

    def forward(t, distance):
        below = lax.rem(z - distance + extent, extent)
        above = lax.rem(z + distance, extent)
        for origin, up_way, there in (
            (above, False, (z + distance < extent) & (z > 0)),
            (below, True, (z >= distance) & (z < extent - 1)),
        ):

            @pl.when(there)
            def _():
                tok_copy(t, origin, up_way).wait_recv()
                tok_copy(t, origin, up_way).start()

        if t == 1 and extent > 2:

            @pl.when(distance == extent - 2)
            def _():
                send_own(1, True)

    def arrive(t, k):
        origin = looked_up(orders, z, k)

        @pl.when((origin != z) & jnp.logical_not(has_inflow(origin)))
        def _():
            tok_copy(t, origin, True).wait_recv()

        if t == 0:

            @pl.when(origin != z)
            def _():
                meta_copy(origin, origin).wait_recv()

        select = chooser(origin)
        if t == 1:
            scale = scale_of(origin)
        for j in range(columns):
            picked = jnp.dot(
                select, tok[t, origin, :, band(j)], preferred_element_type=jnp.float32
            )
            if t == 1:
                picked = scale * picked
            picks[t, origin, :, :, band(j)] = picked.astype(jnp.bfloat16).reshape(
                plane, capacity, step
            )

        @pl.loop(1, plane)
        def _(i):
            row_copy(t, origin, plane_peer(i)).start()

        rows[t, origin, 0, p] = picks[t, origin, p]

    def swap(t, k):
        origin = looked_up(orders, z, k)

        @pl.loop(1, plane)
        def _(i):
            row_arrival(t, origin, plane_peer(i)).wait_recv()

        swap_copy(t, origin).start()

    def expert_rows(t, origin):
        return rows[t, origin].reshape(2 * slots, width)

    half = gate.shape[1]
    tile = min(256, half)

    def first_products(k):
        origin = looked_up(orders, z, k)

        @pl.when(k == 0)
        def _():
            loads[2].wait()
            loads[3].wait()

        swap_copy(0, origin).wait_recv()

        @pl.loop(0, half // tile)
        def _(n):
            cut = pl.ds(pl.multiple_of(n * tile, tile), tile)
            block = expert_rows(0, origin)
            pre_gate[:, cut] = jnp.dot(block, gate[:, cut], preferred_element_type=jnp.float32)
            pre_up[:, cut] = jnp.dot(block, up[:, cut], preferred_element_type=jnp.float32)

    def products(k):
        origin = looked_up(orders, z, k)

        @pl.when(k == 0)
        def _():
            loads[4].wait()

        swap_copy(1, origin).wait_recv()

        @pl.loop(0, half // tile)
        def _(n):
            cut = pl.ds(pl.multiple_of(n * tile, tile), tile)
            hidden_grad = lax.dot_general(
                expert_rows(1, origin),
                down[cut, :],
                (((1,), (1,)), ((), ())),
                preferred_element_type=jnp.float32,
            )
            g, u = pre_gate[:, cut], pre_up[:, cut]
            logistic = jax.nn.sigmoid(g)
            gate_act = g * logistic
            hidden[origin, :, cut] = (gate_act * u).astype(jnp.bfloat16)
            gate_pre[origin, :, cut] = (
                hidden_grad * u * (logistic * (1.0 + g * (1.0 - logistic)))
            ).astype(jnp.bfloat16)
            up_pre[origin, :, cut] = (hidden_grad * gate_act).astype(jnp.bfloat16)

        wide = min(256, width)

        @pl.loop(0, width // wide)
        def _(n):
            cut = pl.ds(pl.multiple_of(n * wide, wide), wide)
            part = lax.dot_general(
                gate_pre[origin],
                gate[cut, :],
                (((1,), (1,)), ((), ())),
                preferred_element_type=jnp.float32,
            ) + lax.dot_general(
                up_pre[origin],
                up[cut, :],
                (((1,), (1,)), ((), ())),
                preferred_element_type=jnp.float32,
            )
            part = part.astype(jnp.bfloat16).reshape(2, plane, capacity, wide)
            ret_sent[origin, :, :, cut] = part[0]
            part_sent[origin, :, :, cut] = part[1]

        part_copy(origin).start()
        for out in results(origin):
            out.start()

    def results(origin):
        pairs = [
            (rows.at[0, origin], inputs_out.at[origin]),
            (rows.at[1, origin], routed_out.at[origin]),
            (hidden.at[origin], hidden_out.at[origin]),
            (gate_pre.at[origin], gate_pre_out.at[origin]),
            (up_pre.at[origin], up_pre_out.at[origin]),
        ]
        return [
            pltpu.make_async_copy(src, dst, out_sems.at[i, origin])
            for i, (src, dst) in enumerate(pairs)
        ]

    def send_back(k):
        origin = looked_up(orders, z, k)
        part_copy(origin).wait_recv()
        for j in range(columns):
            both = ret_sent[origin, :, :, band(j)].astype(jnp.float32) + part_got[
                origin, :, :, band(j)
            ].astype(jnp.float32)
            ret_sent[origin, :, :, band(j)] = both.astype(jnp.bfloat16)

        @pl.loop(1, plane)
        def _(i):
            ret_copy(origin, plane_peer(i)).start()

        ret_got[origin, p] = ret_sent[origin, p]

    def combine(k):
        origin = looked_up(orders, z, k)

        @pl.loop(1, plane)
        def _(i):
            ret_arrival(origin, plane_peer(i)).wait_recv()

        select = chooser(origin)
        for j in range(columns):
            back = ret_got[origin, :, :, band(j)].reshape(slots, step)
            added = lax.dot_general(
                select, back, (((0,), (0,)), ((), ())), preferred_element_type=jnp.float32
            )

            @pl.when(origin == z)
            def _():
                total[:, band(j)] = added

            @pl.when(origin != z)
            def _():
                line_sent[origin, :, band(j)] = added.astype(jnp.bfloat16)

            @pl.when((origin != z) & jnp.logical_not(has_inflow(origin)))
            def _():
                line_copy(origin, j).start()

    for load in loads[:2]:
        load.wait()
    for i in range(1, extent):
        meta_copy(line_peer(i), z).start()

    local = values.shape[1]
    strip = min(256, local)
    strips = local // strip
    row_count = values.shape[0]

    def strip_at(n):
        return pl.ds(pl.multiple_of(n * strip, strip), strip)

    def stat_copy(i):
        return remote(
            stats.at[i, 0], stats.at[i, 1], stat_sems.at[0, i], stat_sems.at[1, i], sp, other
        )

    def paired(i, first, second):
        lane = lax.broadcasted_iota(jnp.int32, (row_count, stats.shape[3]), 1)
        stats[i, 0] = jnp.where(lane == 0, first, second)
        stat_copy(i).start()

    def both_sums(i):
        stat_copy(i).wait_recv()
        merged = (stats[i, 0] + stats[i, 1]) / width
        return merged[:, 0:1], merged[:, 1:2]

    share = row_count // extent

    def active_copy(q, owner, i):
        part = active.at[owner, pl.ds(i * share, share)]
        return remote(
            part, part, active_send.at[q, i], active_recv.at[owner, i], z * plane + q, tp
        )

    def prepare():
        loads[5].wait()
        sums = jnp.zeros((row_count, 1), jnp.float32)
        squares = jnp.zeros((row_count, 1), jnp.float32)
        for n in range(strips):
            block = values[:, n * strip : (n + 1) * strip].astype(jnp.float32)
            sums = sums + jnp.sum(block, axis=1, keepdims=True)
            squares = squares + jnp.sum(block * block, axis=1, keepdims=True)
        paired(0, sums, squares)
        average, second = both_sums(0)
        scale = lax.rsqrt(second - average * average + NORM_EPS)
        inverse[...] = jnp.broadcast_to(scale, inverse.shape)
        for n in range(strips):
            cut = slice(n * strip, (n + 1) * strip)
            flat = (values[:, cut].astype(jnp.float32) - average) * scale
            normed[:, cut] = flat
            scaled = flat * gain[:, cut]
            active[p, :, cut] = (scaled * jax.nn.sigmoid(scaled)).astype(jnp.bfloat16)

    def share_active(k):
        @pl.loop(1, plane)
        def _(i):
            active_copy(plane_peer(i), p, k).start()

    send_own(0, False)
    send_own(1, False)
    arrive(0, 0)
    arrive(1, 0)
    prepare()

    @pl.loop(0, extent)
    def _(k):
        @pl.when(k > 0)
        def _():
            forward(1, k)
            arrive(1, k)

        swap(0, k)
        first_products(k)
        swap(1, k)
        share_active(k)

        @pl.when(k < extent - 1)
        def _():
            forward(0, k + 1)
            arrive(0, k + 1)

        @pl.when(k > 0)
        def _():
            combine(k - 1)

        products(k)
        send_back(k)

    combine(extent - 1)

    @pl.loop(0, extent - 1)
    def _(k):
        home = looked_up(relays, z, k)

        @pl.when(has_inflow(home))
        def _():
            for j in range(columns):
                line_arrival(home, j).wait_recv()
                line_sent[home, :, band(j)] = (
                    line_sent[home, :, band(j)].astype(jnp.float32)
                    + line_got[home, :, band(j)].astype(jnp.float32)
                ).astype(jnp.bfloat16)
                line_copy(home, j).start()

    own_block = width // (extent * plane)
    lanes = blocks.shape[4]

    def block_at(j, q):
        start = (j * plane + q) * own_block
        return pl.ds(pl.multiple_of(start // lanes * lanes, lanes), lanes)

    def token_copy(j):
        return remote(
            tokens.at[tp, :, band(j)],
            tokens.at[tp, :, band(j)],
            token_sems.at[0, j],
            token_sems.at[1, j],
            sp,
            other,
        )

    def token_arrival(j):
        return remote(
            tokens.at[other, :, band(j)],
            tokens.at[other, :, band(j)],
            token_sems.at[0, j],
            token_sems.at[1, j],
            sp,
            other,
        )

    def block_copy(j, q):
        return remote(
            tokens.at[tp, :, block_at(j, q)],
            blocks.at[j, tp, p],
            block_send.at[j, q],
            block_recv.at[j, p],
            z * plane + q,
            tp,
        )

    def block_arrival(j, q):
        return remote(
            tokens.at[tp, :, block_at(j, q)],
            blocks.at[j, tp, q],
            block_send.at[j, q],
            block_recv.at[j, q],
            z * plane + q,
            tp,
        )

    def block_swap(j):
        return remote(
            blocks.at[j, tp],
            blocks.at[j, tp],
            block_swaps.at[0, j],
            block_swaps.at[1, j],
            sp,
            other,
        )

    def block_swap_arrival(j):
        return remote(
            blocks.at[j, other],
            blocks.at[j, other],
            block_swaps.at[0, j],
            block_swaps.at[1, j],
            sp,
            other,
        )

    for j in range(columns):
        for slot, there in ((z, z > 0), (extent, z < extent - 1)):

            @pl.when(there)
            def _():
                line_arrival(slot, j).wait_recv()
                total[:, band(j)] = total[:, band(j)] + line_got[slot, :, band(j)].astype(
                    jnp.float32
                )

        tokens[tp, :, band(j)] = (
            tok[1, z, :, band(j)].astype(jnp.float32) + total[:, band(j)]
        ).astype(jnp.bfloat16)

        @pl.loop(1, plane)
        def _(i):
            block_copy(j, plane_peer(i)).start()

        token_copy(j).start()

    pieces = 2
    piece = local // pieces

    def piece_at(h):
        return pl.ds(h * piece, piece)

    def sums_copy(j, h):
        to_z = jnp.where(j > z, z + 1, z - 1)
        slot = jnp.where((j < z) & (to_z == j), extent, j)
        return remote(
            sums_sent.at[j, :, piece_at(h)],
            sums_got.at[slot, :, piece_at(h)],
            sums_send.at[j, h],
            sums_recv.at[slot, h],
            to_z * plane + p,
            tp,
        )

    def sums_arrival(slot, h):
        return remote(
            sums_sent.at[0, :, piece_at(h)],
            sums_got.at[slot, :, piece_at(h)],
            sums_send.at[0, h],
            sums_recv.at[slot, h],
            sp,
            other,
        )

    loads[6].wait()
    for j in range(columns):
        token_arrival(j).wait_recv()
    grad_sum = jnp.zeros((row_count, 1), jnp.float32)
    grad_corr = jnp.zeros((row_count, 1), jnp.float32)
    for n in range(strips):
        cut = slice(n * strip, (n + 1) * strip)
        act_grad = lax.dot_general(
            tokens[...].reshape(row_count, width),
            out_weight[cut, :],
            (((1,), (1,)), ((), ())),
            preferred_element_type=jnp.float32,
        )
        flat = normed[:, cut]
        weight = gain[:, cut]
        scaled = flat * weight
        logistic = jax.nn.sigmoid(scaled)
        slope = act_grad * (logistic * (1.0 + scaled * (1.0 - logistic))) * weight
        spread[:row_count, cut] = slope
        grad_sum = grad_sum + jnp.sum(slope, axis=1, keepdims=True)
        grad_corr = grad_corr + jnp.sum(slope * flat, axis=1, keepdims=True)
    paired(1, grad_sum, grad_corr)
    mean, corr = both_sums(1)
    edge = (padded.shape[0] - row_count) // 2
    scale = inverse[:, 0:1]
    for n in range(strips):
        cut = slice(n * strip, (n + 1) * strip)
        padded[edge : edge + row_count, cut] = (
            scale * (spread[:row_count, cut] - mean - normed[:, cut] * corr)
        ).astype(jnp.bfloat16)

    def halo_copy(up_way):
        if up_way:
            src, dst, to = row_count, 0, sp + 1
        else:
            src, dst, to = edge, edge + row_count, sp - 1
        return remote(
            padded.at[pl.ds(src, edge), :],
            padded.at[pl.ds(dst, edge), :],
            halo_sems.at[0, int(up_way)],
            halo_sems.at[1, int(up_way)],
            to,
            tp,
        )

    inside = {True: sp < last_sp, False: sp > 0}
    for up_way in (True, False):

        @pl.when(inside[up_way])
        def _():
            halo_copy(up_way).start()

    @pl.loop(1, plane)
    def _(i):
        for k in range(extent):
            active_copy(plane_peer(i), plane_peer(i), k).wait_recv()

    @pl.loop(0, extent)
    def _(j):
        blocks[j, tp, p] = tokens[tp, :, block_at(j, p)]

        @pl.loop(1, plane)
        def _(i):
            block_arrival(j, plane_peer(i)).wait_recv()

        block_swap(j).start()

    @pl.loop(0, extent)
    def _(k):
        j = looked_up(sum_orders(extent), z, k)
        block_swap_arrival(j).wait_recv()
        for n in range(strips):
            cut = slice(n * strip, (n + 1) * strip)
            spread[:lanes, cut] = sum(
                lax.dot_general(
                    blocks[j, side].reshape(plane * token_count, lanes),
                    active[:, side * token_count : (side + 1) * token_count, cut].reshape(
                        plane * token_count, strip
                    ),
                    (((0,), (0,)), ((), ())),
                    preferred_element_type=jnp.float32,
                )
                for side in range(2)
            )
        start = lax.rem((j * plane + p) * own_block, lanes)
        mine = spread[pl.ds(pl.multiple_of(start, own_block), own_block), :]

        @pl.when(j == z)
        def _():
            sums_own[...] = mine

        @pl.when(j != z)
        def _():
            sums_sent[j] = mine.astype(jnp.bfloat16)

        @pl.when((j != z) & jnp.logical_not(has_inflow(j)))
        def _():
            for h in range(pieces):
                sums_copy(j, h).start()

    def relay(k):
        j = looked_up(sum_relays(extent), z, k)

        @pl.when(has_inflow(j))
        def _():
            for h in range(pieces):
                sums_arrival(j, h).wait_recv()
                sums_sent[j, :, piece_at(h)] = (
                    sums_sent[j, :, piece_at(h)].astype(jnp.float32)
                    + sums_got[j, :, piece_at(h)].astype(jnp.float32)
                ).astype(jnp.bfloat16)
                sums_copy(j, h).start()

    for up_way in (True, False):
        at = 0 if up_way else edge + row_count

        @pl.when(inside[not up_way])
        def _():
            halo_copy(up_way).wait_recv()

        @pl.when(jnp.logical_not(inside[not up_way]))
        def _():
            padded[at : at + edge, :] = jnp.zeros((edge, local), jnp.bfloat16)

    tap_count = taps.shape[0]
    reach = tap_count // 2
    narrow = min(128, local)
    spread[...] = padded[...].astype(jnp.float32)
    depth = (edge + reach) // 8 * 8 + row_count

    @pl.loop(0, local // narrow)
    def _(n):
        cut = pl.ds(pl.multiple_of(n * narrow, narrow), narrow)
        acc = jnp.zeros((row_count, narrow), jnp.float32)
        for s in range(8):
            picks_at = [o for o in range(tap_count) if (edge + reach - o) % 8 == s]
            if not picks_at:
                continue
            shifted = spread[s : s + depth, cut]
            for o in picks_at:
                m = (edge + reach - o) // 8 * 8
                acc = acc + taps[o : o + 1, cut] * shifted[m : m + row_count]
        values[:, cut] = acc.astype(jnp.bfloat16)

    finish = pltpu.make_async_copy(values, input_out, load_sem.at[0])
    finish.start()
    for k in range(extent - 1):
        relay(k)
    for h in range(pieces):
        for slot, there in ((z, z > 0), (extent, z < extent - 1)):

            @pl.when(there)
            def _():
                sums_arrival(slot, h).wait_recv()
                sums_own[:, piece_at(h)] = sums_own[:, piece_at(h)] + sums_got[
                    slot, :, piece_at(h)
                ].astype(jnp.float32)

    store = pltpu.make_async_copy(sums_own, proj_out, load_sem.at[1])
    store.start()
    for i in range(2):
        stat_copy(i).wait_send()
    for up_way in (True, False):

        @pl.when(inside[up_way])
        def _():
            halo_copy(up_way).wait_send()

    @pl.loop(1, plane)
    def _(i):
        for k in range(extent):
            active_copy(plane_peer(i), p, k).wait_send()

    for j in range(columns):
        token_copy(j).wait_send()

        @pl.loop(1, plane)
        def _(i):
            block_copy(j, plane_peer(i)).wait_send()

        block_swap(j).wait_send()

        @pl.when(z != j)
        def _():
            for h in range(pieces):
                sums_copy(j, h).wait_send()

    for i in range(1, extent):
        meta_copy(line_peer(i), z).wait_send()

    @pl.loop(0, extent)
    def _(origin):
        for t in range(2):
            for up_way in (False, True):

                @pl.when(forwards(origin, up_way))
                def _():
                    tok_copy(t, origin, up_way).wait_send()

            @pl.loop(1, plane)
            def _(i):
                row_copy(t, origin, plane_peer(i)).wait_send()

            swap_copy(t, origin).wait_send()
        part_copy(origin).wait_send()

        @pl.loop(1, plane)
        def _(i):
            ret_copy(origin, plane_peer(i)).wait_send()

        @pl.when(origin != z)
        def _():
            for j in range(columns):
                line_copy(origin, j).wait_send()

        for out in results(origin):
            out.wait()

    finish.wait()
    store.wait()


TOPK_ROWS = 2


def routed_backward(
    mid_rows,
    cotangent,
    meta,
    gate_mat,
    up_mat,
    down_mat,
    filtered,
    out_weight,
    taps,
    gain,
    capacity,
):
    sp_count = lax.axis_size("sp")
    extent = line_extent(sp_count)
    plane = sp_count // extent
    token_count, width = mid_rows.shape
    half = gate_mat.shape[1]
    slots = plane * capacity
    kind = jnp.bfloat16
    any_space = pl.BlockSpec(memory_space=pl.ANY)
    vmem = pl.BlockSpec(memory_space=pltpu.VMEM)
    dma = pltpu.SemaphoreType.DMA
    columns = extent
    row_count, local = filtered.shape
    own_block = width // sp_count
    lanes = min(max(own_block, 128), width // extent)
    edge = -(-(taps.shape[0] // 2) // 16) * 16
    rows_shape = (extent, 2, plane, capacity, width)
    small_shape = (extent, 2 * slots, half)
    scratch = [
        pltpu.VMEM((2, extent, token_count, width), kind),
        pltpu.VMEM((extent,) + meta.shape, jnp.float32),
        pltpu.VMEM((2, extent, plane, capacity, width), kind),
        pltpu.VMEM((2,) + rows_shape, kind),
        pltpu.VMEM(gate_mat.shape, kind),
        pltpu.VMEM(up_mat.shape, kind),
        pltpu.VMEM(down_mat.shape, kind),
        pltpu.VMEM((2 * slots, half), jnp.float32),
        pltpu.VMEM((2 * slots, half), jnp.float32),
        pltpu.VMEM(small_shape, kind),
        pltpu.VMEM(small_shape, kind),
        pltpu.VMEM(small_shape, kind),
        pltpu.VMEM((extent, plane, capacity, width), kind),
        pltpu.VMEM((extent, plane, capacity, width), kind),
        pltpu.VMEM((extent, plane, capacity, width), kind),
        pltpu.VMEM((extent, plane, capacity, width), kind),
        pltpu.VMEM((extent, token_count, width), kind),
        pltpu.VMEM((extent + 1, token_count, width), kind),
        pltpu.VMEM((token_count, width), jnp.float32),
        pltpu.VMEM((2, token_count, width), kind),
        dma((7,)),
        dma((2, extent)),
        dma((2, extent, 2)),
        dma((2, extent)),
        dma((2, extent, plane)),
        dma((2, extent, plane)),
        dma((2, extent)),
        dma((2, extent)),
        dma((2, extent)),
        dma((extent, plane)),
        dma((extent, plane)),
        dma((extent, columns)),
        dma((extent + 1, columns)),
        dma((5, extent)),
        dma((2, columns)),
        pltpu.VMEM((row_count, local), kind),
        pltpu.VMEM(out_weight.shape, kind),
        pltpu.VMEM((2, 2, row_count, 128), jnp.float32),
        pltpu.VMEM((row_count, local), jnp.float32),
        pltpu.VMEM((row_count, 128), jnp.float32),
        pltpu.VMEM((plane, row_count, local), kind),
        pltpu.VMEM((extent, 2, plane, token_count, lanes), kind),
        pltpu.VMEM((extent, own_block, local), kind),
        pltpu.VMEM((extent + 1, own_block, local), kind),
        pltpu.VMEM((own_block, local), jnp.float32),
        pltpu.VMEM((row_count + 2 * edge, local), kind),
        pltpu.VMEM((row_count + 2 * edge, local), jnp.float32),
        dma((2, 2)),
        dma((plane, extent)),
        dma((plane, extent)),
        dma((extent, plane)),
        dma((extent, plane)),
        dma((2, extent)),
        dma((extent, 2)),
        dma((extent + 1, 2)),
        dma((2, 2)),
    ]
    held = sum(
        math.prod(s.shape) * jnp.dtype(s.dtype).itemsize
        for s in scratch
        if s.memory_space == pltpu.VMEM
    )
    out = pl.pallas_call(
        functools.partial(routed_kernel, extent, plane, capacity),
        out_shape=[
            jax.ShapeDtypeStruct((own_block, local), jnp.float32),
            jax.ShapeDtypeStruct((row_count, local), kind),
            jax.ShapeDtypeStruct(rows_shape, kind),
            jax.ShapeDtypeStruct(rows_shape, kind),
            jax.ShapeDtypeStruct(small_shape, kind),
            jax.ShapeDtypeStruct(small_shape, kind),
            jax.ShapeDtypeStruct(small_shape, kind),
        ],
        in_specs=[any_space] * 2 + [vmem] + [any_space] * 5 + [vmem] * 2,
        out_specs=[any_space] * 7,
        scratch_shapes=scratch,
        compiler_params=pltpu.CompilerParams(
            collective_id=0, has_side_effects=True, vmem_limit_bytes=min(held + SPARE, 67_043_328)
        ),
    )(
        mid_rows, cotangent, meta, gate_mat, up_mat, down_mat, filtered, out_weight, taps, gain
    )
    proj_grad, input_grad, inputs, routed, hidden, gate_pre, up_pre = out
    every = 2 * slots * extent
    return (
        proj_grad,
        input_grad,
        inputs.reshape(every, width),
        routed.reshape(every, width),
        hidden.reshape(every, half),
        gate_pre.reshape(every, half),
        up_pre.reshape(every, half),
    )


def per_device(
    mid_rows,
    cotangent,
    routes,
    route_weight,
    filtered,
    conv_taps,
    norm_gain,
    out_weight,
    gate_weight,
    up_weight,
    down_weight,
):
    sp_count = lax.axis_size("sp")
    token_count, model_width = mid_rows.shape
    per_token = routes.shape[1]
    local_experts = gate_weight.shape[0]
    experts = local_experts * sp_count
    capacity = 2 * token_count * per_token // sp_count
    target = slot_targets(routes, experts, capacity).astype(jnp.float32)
    meta = jnp.concatenate([target.T, route_weight.T], axis=0)
    meta = jnp.pad(meta, ((0, 8 - meta.shape[0]), (0, 0)))
    proj_grad, input_grad, inputs, routed, hidden, gate_pre, up_pre = routed_backward(
        mid_rows,
        cotangent,
        meta,
        gate_weight[0],
        up_weight[0],
        down_weight[0],
        filtered,
        out_weight,
        conv_taps,
        norm_gain[None],
        capacity,
    )
    gate_grad = transposed_product(inputs, gate_pre)[None]
    up_grad = transposed_product(inputs, up_pre)[None]
    down_grad = transposed_product(hidden, routed)[None]
    return (gate_grad, up_grad, down_grad, proj_grad, input_grad)


def solution(mesh):
    in_specs = (
        P(("sp", "tp"), None),
        P(("sp", "tp"), None),
        P(("sp", "tp"), None),
        P(("sp", "tp"), None),
        P("sp", "tp"),
        P(None, "tp"),
        P("tp"),
        P("tp", None),
        P("sp", None, "tp"),
        P("sp", None, "tp"),
        P("sp", "tp", None),
    )
    out_specs = (
        P("sp", None, "tp"),
        P("sp", None, "tp"),
        P("sp", "tp", None),
        P("sp", "tp"),
        P("sp", "tp"),
    )
    return jax.shard_map(
        per_device, mesh=mesh, in_specs=in_specs, out_specs=out_specs, check_vma=False
    )
```

```python
import functools
import math

import jax
import jax.numpy as jnp
from jax import lax
from jax.experimental import pallas as pl
from jax.experimental.pallas import tpu as pltpu
from jax.sharding import PartitionSpec as P

MESH = pl.DeviceIdType.MESH
NORM_EPS = 1e-05
SPARE = 4 << 20


def slot_targets(routes, experts, capacity):
    token_count, per_token = routes.shape
    flattened = routes.reshape(token_count * per_token)
    one_hot = flattened[:, None] == jnp.arange(experts, dtype=jnp.int32)[None, :]
    route_ids = jnp.arange(token_count * per_token, dtype=jnp.int32)
    before = (route_ids[None, :] < route_ids[:, None]).astype(jnp.bfloat16)
    earlier = jnp.dot(before, one_hot.astype(jnp.bfloat16), preferred_element_type=jnp.float32)
    positions = jnp.sum(jnp.where(one_hot, earlier, 0.0), axis=1).astype(jnp.int32)
    return (flattened * capacity + positions).reshape(token_count, per_token)


def transposed_product(left, right):
    return lax.dot_general(
        left, right, (((0,), (0,)), ((), ())), preferred_element_type=jnp.float32
    )


def line_extent(count):
    bits = count.bit_length() - 1
    return 1 << -(-bits // 3)


def chunk_orders(extent):
    orders = []
    for own in range(extent):
        toward = [i for i in range(own + 1, extent)] if 2 * own < extent - 1 else [i for i in range(own - 1, -1, -1)]
        back = [i for i in range(extent) if i != own and i not in toward]
        back.sort(key=lambda i: abs(i - own))
        if own in (0, extent - 1):
            order = toward[1:] + toward[:1]
        else:
            order = toward[:1] + back + toward[1:]
        orders.append([own] + order)
    return orders


def pick_events(extent):
    table = []
    for own, order in enumerate(chunk_orders(extent)):
        rest = order[1:]
        if own in (0, extent - 1):
            near, far = rest[-1], rest[:-1]
            events = [(0, near)] + [(t, i) for i in far for t in range(2)] + [(1, near)]
        else:
            near = [i for i in rest if abs(i - own) == 1]
            far = [i for i in rest if abs(i - own) > 1]
            events = [(t, i) for t in range(2) for i in near]
            events = events + [(t, i) for i in far for t in range(2)]
        table.append(events)
    return table


def relay_orders(extent):
    return [
        sorted(
            (i for i in range(extent) if i != own),
            key=lambda i: (own if i > own else extent - 1 - own, abs(i - own)),
        )
        for own in range(extent)
    ]


def sum_orders(extent):
    return [
        sorted((i for i in range(extent) if i != own), key=lambda i: -abs(i - own)) + [own]
        for own in range(extent)
    ]


def sum_relays(extent):
    return [
        sorted(
            (i for i in range(extent) if i != own),
            key=lambda i: (own if i > own else extent - 1 - own, -abs(i - own)),
        )
        for own in range(extent)
    ]


def looked_up(table, row, column):
    value = jnp.int32(0)
    for i, entries in enumerate(table):
        for k, entry in enumerate(entries):
            value = value + jnp.where((row == i) & (column == k), entry, 0)
    return value


def routed_kernel(
    extent,
    plane,
    capacity,
    mid_hbm,
    cot_hbm,
    meta,
    gate_hbm,
    up_hbm,
    down_hbm,
    filtered_hbm,
    out_weight_hbm,
    taps,
    gain,
    proj_out,
    input_out,
    inputs_out,
    routed_out,
    hidden_out,
    gate_pre_out,
    up_pre_out,
    tok,
    metas,
    picks,
    rows,
    gate,
    up,
    down,
    pre_gate,
    pre_up,
    hidden,
    gate_pre,
    up_pre,
    part_sent,
    part_got,
    ret_sent,
    ret_got,
    line_sent,
    line_got,
    total,
    tokens,
    load_sem,
    meta_sems,
    tok_send,
    tok_recv,
    row_send,
    row_recv,
    swap_send,
    swap_recv,
    part_sems,
    ret_send,
    ret_recv,
    line_send,
    line_recv,
    out_sems,
    token_sems,
    values,
    out_weight,
    stats,
    normed,
    inverse,
    active,
    blocks,
    sums_sent,
    sums_got,
    sums_own,
    padded,
    spread,
    stat_sems,
    active_send,
    active_recv,
    block_send,
    block_recv,
    block_swaps,
    sums_send,
    sums_recv,
    halo_sems,
):
    sp, tp = lax.axis_index("sp"), lax.axis_index("tp")
    z, p = sp // plane, sp % plane
    slots = plane * capacity
    token_count, width = tok.shape[2], tok.shape[3]
    other = 1 - tp
    step = width // extent
    columns = extent
    orders, relays = chunk_orders(extent), relay_orders(extent)

    def remote(src, dst, send, recv, to_sp, to_tp):
        return pltpu.make_async_remote_copy(
            src_ref=src,
            dst_ref=dst,
            send_sem=send,
            recv_sem=recv,
            device_id=(to_sp, to_tp),
            device_id_type=MESH,
        )

    loads = [
        pltpu.make_async_copy(mid_hbm, tok.at[0, z], load_sem.at[0]),
        pltpu.make_async_copy(cot_hbm, tok.at[1, z], load_sem.at[1]),
        pltpu.make_async_copy(gate_hbm, gate, load_sem.at[2]),
        pltpu.make_async_copy(up_hbm, up, load_sem.at[3]),
        pltpu.make_async_copy(down_hbm, down, load_sem.at[4]),
        pltpu.make_async_copy(filtered_hbm, values, load_sem.at[5]),
        pltpu.make_async_copy(out_weight_hbm, out_weight, load_sem.at[6]),
    ]
    for load in loads:
        load.start()
    metas[z] = meta[...]

    barrier = pltpu.get_barrier_semaphore()

    def greet(to_sp, to_tp):
        pl.semaphore_signal(barrier, inc=1, device_id=(to_sp, to_tp), device_id_type=MESH)

    def line_peer(i):
        return lax.rem(z + i, extent)

    def plane_peer(i):
        return lax.rem(p + i, plane)

    for i in range(1, extent):
        greet(line_peer(i) * plane + p, tp)

    @pl.loop(1, plane)
    def _(i):
        greet(z * plane + plane_peer(i), tp)

    greet(sp, other)
    last_sp = extent * plane - 1

    @pl.when(sp > 0)
    def _():
        greet(sp - 1, tp)

    @pl.when(sp < last_sp)
    def _():
        greet(sp + 1, tp)

    ends = jnp.where(sp > 0, 1, 0) + jnp.where(sp < last_sp, 1, 0)
    pl.semaphore_wait(barrier, extent - 1 + plane - 1 + 1 + ends)

    def meta_copy(to_z, from_z):
        return remote(
            meta, metas.at[from_z], meta_sems.at[0, to_z], meta_sems.at[1, from_z], to_z * plane + p, tp
        )

    def tok_copy(t, origin, up_way):
        to_z = z + 1 if up_way else z - 1
        return remote(
            tok.at[t, origin],
            tok.at[t, origin],
            tok_send.at[t, origin, int(up_way)],
            tok_recv.at[t, origin],
            to_z * plane + p,
            tp,
        )

    def forwards(origin, up_way):
        if up_way:
            return (origin <= z) & (z < extent - 1)
        return (origin >= z) & (z > 0)

    def row_copy(t, origin, q):
        return remote(
            picks.at[t, origin, q],
            rows.at[t, origin, 0, p],
            row_send.at[t, origin, q],
            row_recv.at[t, origin, p],
            z * plane + q,
            tp,
        )

    def row_arrival(t, origin, q):
        return remote(
            picks.at[t, origin, q],
            rows.at[t, origin, 0, q],
            row_send.at[t, origin, q],
            row_recv.at[t, origin, q],
            z * plane + q,
            tp,
        )

    def swap_copy(t, origin):
        return remote(
            rows.at[t, origin, 0],
            rows.at[t, origin, 1],
            swap_send.at[t, origin],
            swap_recv.at[t, origin],
            sp,
            other,
        )

    def part_copy(origin):
        return remote(
            part_sent.at[origin],
            part_got.at[origin],
            part_sems.at[0, origin],
            part_sems.at[1, origin],
            sp,
            other,
        )

    def ret_copy(origin, q):
        return remote(
            ret_sent.at[origin, q],
            ret_got.at[origin, p],
            ret_send.at[origin, q],
            ret_recv.at[origin, p],
            z * plane + q,
            tp,
        )

    def ret_arrival(origin, q):
        return remote(
            ret_sent.at[origin, q],
            ret_got.at[origin, q],
            ret_send.at[origin, q],
            ret_recv.at[origin, q],
            z * plane + q,
            tp,
        )

    def band(j):
        return pl.ds(pl.multiple_of(j * step, step), step)

    def band_for(home, jj):
        return looked_up(sum_orders(extent), home, jj)

    def line_copy(home, j):
        to_z = jnp.where(home > z, z + 1, z - 1)
        slot = jnp.where((home < z) & (to_z == home), extent, home)
        return remote(
            line_sent.at[home, :, band(j)],
            line_got.at[slot, :, band(j)],
            line_send.at[home, j],
            line_recv.at[slot, j],
            to_z * plane + p,
            tp,
        )

    def line_arrival(slot, j):
        return remote(
            line_sent.at[0, :, band(j)],
            line_got.at[slot, :, band(j)],
            line_send.at[0, j],
            line_recv.at[slot, j],
            z * plane + p,
            other,
        )

    def has_inflow(home):
        return ((home > z) & (z > 0)) | ((home < z) & (z < extent - 1))

    def hits(origin):
        slot = lax.broadcasted_iota(jnp.int32, (slots, token_count), 0) + z * slots
        slot = slot.astype(jnp.float32)
        return [slot == metas[origin, pl.ds(k, 1), :] for k in range(TOPK_ROWS)]

    def chooser(origin):
        first, second = hits(origin)
        return jnp.where(first | second, 1.0, 0.0).astype(jnp.bfloat16)

    def scale_of(origin):
        first, second = hits(origin)
        weighted = jnp.where(first, metas[origin, pl.ds(TOPK_ROWS, 1), :], 0.0) + jnp.where(
            second, metas[origin, pl.ds(TOPK_ROWS + 1, 1), :], 0.0
        )
        return jnp.sum(weighted, axis=1, keepdims=True)

    def late(up_way):
        if extent < 3:
            return False
        return (z == extent - 2) if up_way else (z == 1)

    def send_own(t, held_back):
        for up_way in (False, True):
            now = forwards(z, up_way)
            if t == 1 and extent > 2:
                now = now & (late(up_way) == held_back)
            elif held_back:
                continue

            @pl.when(now)
            def _():
                tok_copy(t, z, up_way).start()

    def forward(t, distance):
        below = lax.rem(z - distance + extent, extent)
        above = lax.rem(z + distance, extent)
        for origin, up_way, there in (
            (above, False, (z + distance < extent) & (z > 0)),
            (below, True, (z >= distance) & (z < extent - 1)),
        ):

            @pl.when(there)
            def _():
                tok_copy(t, origin, up_way).wait_recv()
                tok_copy(t, origin, up_way).start()

        if t == 1 and extent > 2:

            @pl.when(distance == extent - 2)
            def _():
                send_own(1, True)

    def arrive(t, origin):
        @pl.when((origin != z) & jnp.logical_not(has_inflow(origin)))
        def _():
            tok_copy(t, origin, True).wait_recv()

        @pl.when((origin != z) & (t == 0))
        def _():
            meta_copy(origin, origin).wait_recv()

        select = chooser(origin)
        scale = jnp.where(t == 1, scale_of(origin), 1.0)
        for j in range(columns):
            picked = scale * jnp.dot(
                select, tok[t, origin, :, band(j)], preferred_element_type=jnp.float32
            )
            picks[t, origin, :, :, band(j)] = picked.astype(jnp.bfloat16).reshape(
                plane, capacity, step
            )

        @pl.loop(1, plane)
        def _(i):
            row_copy(t, origin, plane_peer(i)).start()

        rows[t, origin, 0, p] = picks[t, origin, p]

    def event(i):
        kinds = [[t for t, _ in row] for row in pick_events(extent)]
        origins = [[origin for _, origin in row] for row in pick_events(extent)]
        arrive(looked_up(kinds, z, i), looked_up(origins, z, i))

    def swap(t, k):
        origin = looked_up(orders, z, k)

        @pl.loop(1, plane)
        def _(i):
            row_arrival(t, origin, plane_peer(i)).wait_recv()

        swap_copy(t, origin).start()

    def expert_rows(t, origin):
        return rows[t, origin].reshape(2 * slots, width)

    half = gate.shape[1]
    tile = min(256, half)

    def first_products(k):
        origin = looked_up(orders, z, k)

        @pl.when(k == 0)
        def _():
            loads[2].wait()
            loads[3].wait()

        swap_copy(0, origin).wait_recv()

        @pl.loop(0, half // tile)
        def _(n):
            cut = pl.ds(pl.multiple_of(n * tile, tile), tile)
            block = expert_rows(0, origin)
            pre_gate[:, cut] = jnp.dot(block, gate[:, cut], preferred_element_type=jnp.float32)
            pre_up[:, cut] = jnp.dot(block, up[:, cut], preferred_element_type=jnp.float32)

    def products(k):
        origin = looked_up(orders, z, k)

        @pl.when(k == 0)
        def _():
            loads[4].wait()

        swap_copy(1, origin).wait_recv()

        @pl.loop(0, half // tile)
        def _(n):
            cut = pl.ds(pl.multiple_of(n * tile, tile), tile)
            hidden_grad = lax.dot_general(
                expert_rows(1, origin),
                down[cut, :],
                (((1,), (1,)), ((), ())),
                preferred_element_type=jnp.float32,
            )
            g, u = pre_gate[:, cut], pre_up[:, cut]
            logistic = jax.nn.sigmoid(g)
            gate_act = g * logistic
            hidden[origin, :, cut] = (gate_act * u).astype(jnp.bfloat16)
            gate_pre[origin, :, cut] = (
                hidden_grad * u * (logistic * (1.0 + g * (1.0 - logistic)))
            ).astype(jnp.bfloat16)
            up_pre[origin, :, cut] = (hidden_grad * gate_act).astype(jnp.bfloat16)

        wide = min(256, width)

        @pl.loop(0, width // wide)
        def _(n):
            cut = pl.ds(pl.multiple_of(n * wide, wide), wide)
            part = lax.dot_general(
                gate_pre[origin],
                gate[cut, :],
                (((1,), (1,)), ((), ())),
                preferred_element_type=jnp.float32,
            ) + lax.dot_general(
                up_pre[origin],
                up[cut, :],
                (((1,), (1,)), ((), ())),
                preferred_element_type=jnp.float32,
            )
            part = part.astype(jnp.bfloat16).reshape(2, plane, capacity, wide)
            ret_sent[origin, :, :, cut] = part[0]
            part_sent[origin, :, :, cut] = part[1]

        part_copy(origin).start()
        for out in results(origin):
            out.start()

    def results(origin):
        pairs = [
            (rows.at[0, origin], inputs_out.at[origin]),
            (rows.at[1, origin], routed_out.at[origin]),
            (hidden.at[origin], hidden_out.at[origin]),
            (gate_pre.at[origin], gate_pre_out.at[origin]),
            (up_pre.at[origin], up_pre_out.at[origin]),
        ]
        return [
            pltpu.make_async_copy(src, dst, out_sems.at[i, origin])
            for i, (src, dst) in enumerate(pairs)
        ]

    def send_back(k):
        origin = looked_up(orders, z, k)
        part_copy(origin).wait_recv()
        for j in range(columns):
            both = ret_sent[origin, :, :, band(j)].astype(jnp.float32) + part_got[
                origin, :, :, band(j)
            ].astype(jnp.float32)
            ret_sent[origin, :, :, band(j)] = both.astype(jnp.bfloat16)

        @pl.loop(1, plane)
        def _(i):
            ret_copy(origin, plane_peer(i)).start()

        ret_got[origin, p] = ret_sent[origin, p]

    def combine(k):
        origin = looked_up(orders, z, k)

        @pl.loop(1, plane)
        def _(i):
            ret_arrival(origin, plane_peer(i)).wait_recv()

        select = chooser(origin)
        for jj in range(columns):
            j = band_for(origin, jj)
            back = ret_got[origin, :, :, band(j)].reshape(slots, step)
            added = lax.dot_general(
                select, back, (((0,), (0,)), ((), ())), preferred_element_type=jnp.float32
            )

            @pl.when(origin == z)
            def _():
                total[:, band(j)] = added

            @pl.when(origin != z)
            def _():
                line_sent[origin, :, band(j)] = added.astype(jnp.bfloat16)

            @pl.when((origin != z) & jnp.logical_not(has_inflow(origin)))
            def _():
                line_copy(origin, j).start()

    def line_relay(k):
        home = looked_up(relays, z, k)

        @pl.when(has_inflow(home))
        def _():
            for jj in range(columns):
                j = band_for(home, jj)
                line_arrival(home, j).wait_recv()
                line_sent[home, :, band(j)] = (
                    line_sent[home, :, band(j)].astype(jnp.float32)
                    + line_got[home, :, band(j)].astype(jnp.float32)
                ).astype(jnp.bfloat16)
                line_copy(home, j).start()

    for load in loads[:2]:
        load.wait()
    for i in range(1, extent):
        meta_copy(line_peer(i), z).start()

    local = values.shape[1]
    strip = min(256, local)
    strips = local // strip
    row_count = values.shape[0]

    def strip_at(n):
        return pl.ds(pl.multiple_of(n * strip, strip), strip)

    def stat_copy(i):
        return remote(
            stats.at[i, 0], stats.at[i, 1], stat_sems.at[0, i], stat_sems.at[1, i], sp, other
        )

    def paired(i, first, second):
        lane = lax.broadcasted_iota(jnp.int32, (row_count, stats.shape[3]), 1)
        stats[i, 0] = jnp.where(lane == 0, first, second)
        stat_copy(i).start()

    def both_sums(i):
        stat_copy(i).wait_recv()
        merged = (stats[i, 0] + stats[i, 1]) / width
        return merged[:, 0:1], merged[:, 1:2]

    share = row_count // extent

    def active_copy(q, owner, i):
        part = active.at[owner, pl.ds(i * share, share)]
        return remote(
            part, part, active_send.at[q, i], active_recv.at[owner, i], z * plane + q, tp
        )

    def prepare():
        loads[5].wait()
        sums = jnp.zeros((row_count, 1), jnp.float32)
        squares = jnp.zeros((row_count, 1), jnp.float32)
        for n in range(strips):
            block = values[:, n * strip : (n + 1) * strip].astype(jnp.float32)
            sums = sums + jnp.sum(block, axis=1, keepdims=True)
            squares = squares + jnp.sum(block * block, axis=1, keepdims=True)
        paired(0, sums, squares)
        average, second = both_sums(0)
        scale = lax.rsqrt(second - average * average + NORM_EPS)
        inverse[...] = jnp.broadcast_to(scale, inverse.shape)
        for n in range(strips):
            cut = slice(n * strip, (n + 1) * strip)
            flat = (values[:, cut].astype(jnp.float32) - average) * scale
            normed[:, cut] = flat
            scaled = flat * gain[:, cut]
            active[p, :, cut] = (scaled * jax.nn.sigmoid(scaled)).astype(jnp.bfloat16)

    def share_active(k):
        @pl.loop(1, plane)
        def _(i):
            active_copy(plane_peer(i), p, k).start()

    send_own(0, False)
    send_own(1, False)
    arrive(0, z)
    arrive(1, z)
    prepare()

    @pl.loop(0, extent)
    def _(k):
        @pl.when(k > 0)
        def _():
            forward(1, k)

        swap(0, k)
        first_products(k)

        @pl.when(k == 0)
        def _():
            forward(0, 1)

        @pl.when(k < extent - 1)
        def _():
            event(2 * k)

        @pl.when((k > 0) & (k < extent - 1))
        def _():
            forward(0, k + 1)

        @pl.when((k > 0) & (k < extent - 1))
        def _():
            combine(k - 1)

        swap(1, k)
        share_active(k)
        products(k)

        @pl.when(k < extent - 1)
        def _():
            event(2 * k + 1)

        @pl.when(k == extent - 1)
        def _():
            combine(k - 1)

        send_back(k)

    line_relay(0)
    combine(extent - 1)

    @pl.loop(1, extent - 1)
    def _(k):
        line_relay(k)

    own_block = width // (extent * plane)
    lanes = blocks.shape[4]

    def block_at(j, q):
        start = (j * plane + q) * own_block
        return pl.ds(pl.multiple_of(start // lanes * lanes, lanes), lanes)

    def token_copy(j):
        return remote(
            tokens.at[tp, :, band(j)],
            tokens.at[tp, :, band(j)],
            token_sems.at[0, j],
            token_sems.at[1, j],
            sp,
            other,
        )

    def token_arrival(j):
        return remote(
            tokens.at[other, :, band(j)],
            tokens.at[other, :, band(j)],
            token_sems.at[0, j],
            token_sems.at[1, j],
            sp,
            other,
        )

    def block_copy(j, q):
        return remote(
            tokens.at[tp, :, block_at(j, q)],
            blocks.at[j, tp, p],
            block_send.at[j, q],
            block_recv.at[j, p],
            z * plane + q,
            tp,
        )

    def block_arrival(j, q):
        return remote(
            tokens.at[tp, :, block_at(j, q)],
            blocks.at[j, tp, q],
            block_send.at[j, q],
            block_recv.at[j, q],
            z * plane + q,
            tp,
        )

    def block_swap(j):
        return remote(
            blocks.at[j, tp],
            blocks.at[j, tp],
            block_swaps.at[0, j],
            block_swaps.at[1, j],
            sp,
            other,
        )

    def block_swap_arrival(j):
        return remote(
            blocks.at[j, other],
            blocks.at[j, other],
            block_swaps.at[0, j],
            block_swaps.at[1, j],
            sp,
            other,
        )

    def home_band(jj):
        j = band_for(z, jj)
        for slot, there in ((z, z > 0), (extent, z < extent - 1)):

            @pl.when(there)
            def _():
                line_arrival(slot, j).wait_recv()
                total[:, band(j)] = total[:, band(j)] + line_got[slot, :, band(j)].astype(
                    jnp.float32
                )

        tokens[tp, :, band(j)] = (
            tok[1, z, :, band(j)].astype(jnp.float32) + total[:, band(j)]
        ).astype(jnp.bfloat16)
        token_copy(j).start()

        @pl.loop(1, plane)
        def _(i):
            block_copy(j, plane_peer(i)).start()

        blocks[j, tp, p] = tokens[tp, :, block_at(j, p)]

    def swap_block(jj):
        j = band_for(z, jj)

        @pl.loop(1, plane)
        def _(i):
            block_arrival(j, plane_peer(i)).wait_recv()

        block_swap(j).start()

    pieces = 2
    piece = local // pieces

    def piece_at(h):
        return pl.ds(h * piece, piece)

    def sums_copy(j, h):
        to_z = jnp.where(j > z, z + 1, z - 1)
        slot = jnp.where((j < z) & (to_z == j), extent, j)
        return remote(
            sums_sent.at[j, :, piece_at(h)],
            sums_got.at[slot, :, piece_at(h)],
            sums_send.at[j, h],
            sums_recv.at[slot, h],
            to_z * plane + p,
            tp,
        )

    def sums_arrival(slot, h):
        return remote(
            sums_sent.at[0, :, piece_at(h)],
            sums_got.at[slot, :, piece_at(h)],
            sums_send.at[0, h],
            sums_recv.at[slot, h],
            sp,
            other,
        )

    def act_grads():
        loads[6].wait()
        for j in range(columns):
            token_arrival(j).wait_recv()
        grad_sum = jnp.zeros((row_count, 1), jnp.float32)
        grad_corr = jnp.zeros((row_count, 1), jnp.float32)
        for n in range(strips):
            cut = slice(n * strip, (n + 1) * strip)
            act_grad = lax.dot_general(
                tokens[...].reshape(row_count, width),
                out_weight[cut, :],
                (((1,), (1,)), ((), ())),
                preferred_element_type=jnp.float32,
            )
            flat = normed[:, cut]
            weight = gain[:, cut]
            scaled = flat * weight
            logistic = jax.nn.sigmoid(scaled)
            slope = act_grad * (logistic * (1.0 + scaled * (1.0 - logistic))) * weight
            spread[:row_count, cut] = slope
            grad_sum = grad_sum + jnp.sum(slope, axis=1, keepdims=True)
            grad_corr = grad_corr + jnp.sum(slope * flat, axis=1, keepdims=True)
        paired(1, grad_sum, grad_corr)

    def partial_block(jj):
        j = band_for(z, jj)
        block_swap_arrival(j).wait_recv()
        at = lax.rem((j * plane + p) * own_block, lanes)
        for n in range(strips):
            cut = slice(n * strip, (n + 1) * strip)
            mine = sum(
                lax.dot_general(
                    blocks[j, side].reshape(plane * token_count, lanes),
                    active[:, side * token_count : (side + 1) * token_count, cut].reshape(
                        plane * token_count, strip
                    ),
                    (((0,), (0,)), ((), ())),
                    preferred_element_type=jnp.float32,
                )
                for side in range(2)
            )
            if own_block != lanes:
                mine = sum(
                    jnp.where(at == start, mine[start : start + own_block], 0.0)
                    for start in range(0, lanes, own_block)
                )

            @pl.when(j == z)
            def _():
                sums_own[:, cut] = mine

            @pl.when(j != z)
            def _():
                sums_sent[j, :, cut] = mine.astype(jnp.bfloat16)

        @pl.when((j != z) & jnp.logical_not(has_inflow(j)))
        def _():
            for h in range(pieces):
                sums_copy(j, h).start()

    @pl.loop(1, plane)
    def _(i):
        for k in range(extent):
            active_copy(plane_peer(i), plane_peer(i), k).wait_recv()

    @pl.loop(0, extent + 2)
    def _(jj):
        @pl.when(jj < extent)
        def _():
            home_band(jj)

        @pl.when(jj == extent)
        def _():
            act_grads()

        @pl.when((jj > 0) & (jj <= extent))
        def _():
            swap_block(jj - 1)

        @pl.when(jj > 1)
        def _():
            partial_block(jj - 2)

    mean, corr = both_sums(1)
    edge = (padded.shape[0] - row_count) // 2
    scale = inverse[:, 0:1]
    for n in range(strips):
        cut = slice(n * strip, (n + 1) * strip)
        padded[edge : edge + row_count, cut] = (
            scale * (spread[:row_count, cut] - mean - normed[:, cut] * corr)
        ).astype(jnp.bfloat16)

    def halo_copy(up_way):
        if up_way:
            src, dst, to = row_count, 0, sp + 1
        else:
            src, dst, to = edge, edge + row_count, sp - 1
        return remote(
            padded.at[pl.ds(src, edge), :],
            padded.at[pl.ds(dst, edge), :],
            halo_sems.at[0, int(up_way)],
            halo_sems.at[1, int(up_way)],
            to,
            tp,
        )

    inside = {True: sp < last_sp, False: sp > 0}
    for up_way in (True, False):

        @pl.when(inside[up_way])
        def _():
            halo_copy(up_way).start()

    def relay(k):
        j = looked_up(sum_relays(extent), z, k)

        @pl.when(has_inflow(j))
        def _():
            for h in range(pieces):
                sums_arrival(j, h).wait_recv()
                sums_sent[j, :, piece_at(h)] = (
                    sums_sent[j, :, piece_at(h)].astype(jnp.float32)
                    + sums_got[j, :, piece_at(h)].astype(jnp.float32)
                ).astype(jnp.bfloat16)
                sums_copy(j, h).start()

    relay(0)
    for up_way in (True, False):
        at = 0 if up_way else edge + row_count

        @pl.when(inside[not up_way])
        def _():
            halo_copy(up_way).wait_recv()

        @pl.when(jnp.logical_not(inside[not up_way]))
        def _():
            padded[at : at + edge, :] = jnp.zeros((edge, local), jnp.bfloat16)

    tap_count = taps.shape[0]
    reach = tap_count // 2
    narrow = min(128, local)
    spread[...] = padded[...].astype(jnp.float32)
    depth = (edge + reach) // 8 * 8 + row_count

    @pl.loop(0, local // narrow)
    def _(n):
        cut = pl.ds(pl.multiple_of(n * narrow, narrow), narrow)
        acc = jnp.zeros((row_count, narrow), jnp.float32)
        for s in range(8):
            picks_at = [o for o in range(tap_count) if (edge + reach - o) % 8 == s]
            if not picks_at:
                continue
            shifted = spread[s : s + depth, cut]
            for o in picks_at:
                m = (edge + reach - o) // 8 * 8
                acc = acc + taps[o : o + 1, cut] * shifted[m : m + row_count]
        values[:, cut] = acc.astype(jnp.bfloat16)

    finish = pltpu.make_async_copy(values, input_out, load_sem.at[0])
    finish.start()
    for k in range(1, extent - 1):
        relay(k)
    for h in range(pieces):
        for slot, there in ((z, z > 0), (extent, z < extent - 1)):

            @pl.when(there)
            def _():
                sums_arrival(slot, h).wait_recv()
                sums_own[:, piece_at(h)] = sums_own[:, piece_at(h)] + sums_got[
                    slot, :, piece_at(h)
                ].astype(jnp.float32)

    store = pltpu.make_async_copy(sums_own, proj_out, load_sem.at[1])
    store.start()
    for i in range(2):
        stat_copy(i).wait_send()
    for up_way in (True, False):

        @pl.when(inside[up_way])
        def _():
            halo_copy(up_way).wait_send()

    @pl.loop(1, plane)
    def _(i):
        for k in range(extent):
            active_copy(plane_peer(i), p, k).wait_send()

    for j in range(columns):
        token_copy(j).wait_send()

        @pl.loop(1, plane)
        def _(i):
            block_copy(j, plane_peer(i)).wait_send()

        block_swap(j).wait_send()

        @pl.when(z != j)
        def _():
            for h in range(pieces):
                sums_copy(j, h).wait_send()

    for i in range(1, extent):
        meta_copy(line_peer(i), z).wait_send()

    @pl.loop(0, extent)
    def _(origin):
        for t in range(2):
            for up_way in (False, True):

                @pl.when(forwards(origin, up_way))
                def _():
                    tok_copy(t, origin, up_way).wait_send()

            @pl.loop(1, plane)
            def _(i):
                row_copy(t, origin, plane_peer(i)).wait_send()

            swap_copy(t, origin).wait_send()
        part_copy(origin).wait_send()

        @pl.loop(1, plane)
        def _(i):
            ret_copy(origin, plane_peer(i)).wait_send()

        @pl.when(origin != z)
        def _():
            for j in range(columns):
                line_copy(origin, j).wait_send()

        for out in results(origin):
            out.wait()

    finish.wait()
    store.wait()


TOPK_ROWS = 2


def routed_backward(
    mid_rows,
    cotangent,
    meta,
    gate_mat,
    up_mat,
    down_mat,
    filtered,
    out_weight,
    taps,
    gain,
    capacity,
):
    sp_count = lax.axis_size("sp")
    extent = line_extent(sp_count)
    plane = sp_count // extent
    token_count, width = mid_rows.shape
    half = gate_mat.shape[1]
    slots = plane * capacity
    kind = jnp.bfloat16
    any_space = pl.BlockSpec(memory_space=pl.ANY)
    vmem = pl.BlockSpec(memory_space=pltpu.VMEM)
    dma = pltpu.SemaphoreType.DMA
    columns = extent
    row_count, local = filtered.shape
    own_block = width // sp_count
    lanes = min(max(own_block, 128), width // extent)
    edge = -(-(taps.shape[0] // 2) // 16) * 16
    rows_shape = (extent, 2, plane, capacity, width)
    small_shape = (extent, 2 * slots, half)
    scratch = [
        pltpu.VMEM((2, extent, token_count, width), kind),
        pltpu.VMEM((extent,) + meta.shape, jnp.float32),
        pltpu.VMEM((2, extent, plane, capacity, width), kind),
        pltpu.VMEM((2,) + rows_shape, kind),
        pltpu.VMEM(gate_mat.shape, kind),
        pltpu.VMEM(up_mat.shape, kind),
        pltpu.VMEM(down_mat.shape, kind),
        pltpu.VMEM((2 * slots, half), jnp.float32),
        pltpu.VMEM((2 * slots, half), jnp.float32),
        pltpu.VMEM(small_shape, kind),
        pltpu.VMEM(small_shape, kind),
        pltpu.VMEM(small_shape, kind),
        pltpu.VMEM((extent, plane, capacity, width), kind),
        pltpu.VMEM((extent, plane, capacity, width), kind),
        pltpu.VMEM((extent, plane, capacity, width), kind),
        pltpu.VMEM((extent, plane, capacity, width), kind),
        pltpu.VMEM((extent, token_count, width), kind),
        pltpu.VMEM((extent + 1, token_count, width), kind),
        pltpu.VMEM((token_count, width), jnp.float32),
        pltpu.VMEM((2, token_count, width), kind),
        dma((7,)),
        dma((2, extent)),
        dma((2, extent, 2)),
        dma((2, extent)),
        dma((2, extent, plane)),
        dma((2, extent, plane)),
        dma((2, extent)),
        dma((2, extent)),
        dma((2, extent)),
        dma((extent, plane)),
        dma((extent, plane)),
        dma((extent, columns)),
        dma((extent + 1, columns)),
        dma((5, extent)),
        dma((2, columns)),
        pltpu.VMEM((row_count, local), kind),
        pltpu.VMEM(out_weight.shape, kind),
        pltpu.VMEM((2, 2, row_count, 128), jnp.float32),
        pltpu.VMEM((row_count, local), jnp.float32),
        pltpu.VMEM((row_count, 128), jnp.float32),
        pltpu.VMEM((plane, row_count, local), kind),
        pltpu.VMEM((extent, 2, plane, token_count, lanes), kind),
        pltpu.VMEM((extent, own_block, local), kind),
        pltpu.VMEM((extent + 1, own_block, local), kind),
        pltpu.VMEM((own_block, local), jnp.float32),
        pltpu.VMEM((row_count + 2 * edge, local), kind),
        pltpu.VMEM((row_count + 2 * edge, local), jnp.float32),
        dma((2, 2)),
        dma((plane, extent)),
        dma((plane, extent)),
        dma((extent, plane)),
        dma((extent, plane)),
        dma((2, extent)),
        dma((extent, 2)),
        dma((extent + 1, 2)),
        dma((2, 2)),
    ]
    held = sum(
        math.prod(s.shape) * jnp.dtype(s.dtype).itemsize
        for s in scratch
        if s.memory_space == pltpu.VMEM
    )
    out = pl.pallas_call(
        functools.partial(routed_kernel, extent, plane, capacity),
        out_shape=[
            jax.ShapeDtypeStruct((own_block, local), jnp.float32),
            jax.ShapeDtypeStruct((row_count, local), kind),
            jax.ShapeDtypeStruct(rows_shape, kind),
            jax.ShapeDtypeStruct(rows_shape, kind),
            jax.ShapeDtypeStruct(small_shape, kind),
            jax.ShapeDtypeStruct(small_shape, kind),
            jax.ShapeDtypeStruct(small_shape, kind),
        ],
        in_specs=[any_space] * 2 + [vmem] + [any_space] * 5 + [vmem] * 2,
        out_specs=[any_space] * 7,
        scratch_shapes=scratch,
        compiler_params=pltpu.CompilerParams(
            collective_id=0, has_side_effects=True, vmem_limit_bytes=min(held + SPARE, 67_043_328)
        ),
    )(
        mid_rows, cotangent, meta, gate_mat, up_mat, down_mat, filtered, out_weight, taps, gain
    )
    proj_grad, input_grad, inputs, routed, hidden, gate_pre, up_pre = out
    every = 2 * slots * extent
    return (
        proj_grad,
        input_grad,
        inputs.reshape(every, width),
        routed.reshape(every, width),
        hidden.reshape(every, half),
        gate_pre.reshape(every, half),
        up_pre.reshape(every, half),
    )


def per_device(
    mid_rows,
    cotangent,
    routes,
    route_weight,
    filtered,
    conv_taps,
    norm_gain,
    out_weight,
    gate_weight,
    up_weight,
    down_weight,
):
    sp_count = lax.axis_size("sp")
    token_count, model_width = mid_rows.shape
    per_token = routes.shape[1]
    local_experts = gate_weight.shape[0]
    experts = local_experts * sp_count
    capacity = 2 * token_count * per_token // sp_count
    target = slot_targets(routes, experts, capacity).astype(jnp.float32)
    meta = jnp.concatenate([target.T, route_weight.T], axis=0)
    meta = jnp.pad(meta, ((0, 8 - meta.shape[0]), (0, 0)))
    proj_grad, input_grad, inputs, routed, hidden, gate_pre, up_pre = routed_backward(
        mid_rows,
        cotangent,
        meta,
        gate_weight[0],
        up_weight[0],
        down_weight[0],
        filtered,
        out_weight,
        conv_taps,
        norm_gain[None],
        capacity,
    )
    gate_grad = transposed_product(inputs, gate_pre)[None]
    up_grad = transposed_product(inputs, up_pre)[None]
    down_grad = transposed_product(hidden, routed)[None]
    return (gate_grad, up_grad, down_grad, proj_grad, input_grad)


def solution(mesh):
    in_specs = (
        P(("sp", "tp"), None),
        P(("sp", "tp"), None),
        P(("sp", "tp"), None),
        P(("sp", "tp"), None),
        P("sp", "tp"),
        P(None, "tp"),
        P("tp"),
        P("tp", None),
        P("sp", None, "tp"),
        P("sp", None, "tp"),
        P("sp", "tp", None),
    )
    out_specs = (
        P("sp", None, "tp"),
        P("sp", None, "tp"),
        P("sp", "tp", None),
        P("sp", "tp"),
        P("sp", "tp"),
    )
    return jax.shard_map(
        per_device, mesh=mesh, in_specs=in_specs, out_specs=out_specs, check_vma=False
    )
```

```python
import functools
import math

import jax
import jax.numpy as jnp
from jax import lax
from jax.experimental import pallas as pl
from jax.experimental.pallas import tpu as pltpu
from jax.sharding import PartitionSpec as P

MESH = pl.DeviceIdType.MESH
NORM_EPS = 1e-05
SPARE = 4 << 20


def line_extent(count):
    bits = count.bit_length() - 1
    return 1 << -(-bits // 3)


def chunk_orders(extent):
    orders = []
    for own in range(extent):
        toward = [i for i in range(own + 1, extent)] if 2 * own < extent - 1 else [i for i in range(own - 1, -1, -1)]
        back = [i for i in range(extent) if i != own and i not in toward]
        back.sort(key=lambda i: abs(i - own))
        if own in (0, extent - 1):
            order = toward[1:] + toward[:1]
        else:
            order = toward[:1] + back + toward[1:]
        orders.append([own] + order)
    return orders


def pick_events(extent):
    table = []
    for own, order in enumerate(chunk_orders(extent)):
        rest = order[1:]
        if own in (0, extent - 1):
            near, far = rest[-1], rest[:-1]
            events = [(0, near)] + [(t, i) for i in far for t in range(2)] + [(1, near)]
        else:
            near = [i for i in rest if abs(i - own) == 1]
            far = [i for i in rest if abs(i - own) > 1]
            events = [(t, i) for t in range(2) for i in near]
            events = events + [(t, i) for i in far for t in range(2)]
        table.append(events)
    return table


def relay_orders(extent):
    return [
        sorted(
            (i for i in range(extent) if i != own),
            key=lambda i: (own if i > own else extent - 1 - own, abs(i - own)),
        )
        for own in range(extent)
    ]


def sum_orders(extent):
    return [
        sorted((i for i in range(extent) if i != own), key=lambda i: -abs(i - own)) + [own]
        for own in range(extent)
    ]


def sum_relays(extent):
    return [
        sorted(
            (i for i in range(extent) if i != own),
            key=lambda i: (own if i > own else extent - 1 - own, -abs(i - own)),
        )
        for own in range(extent)
    ]


def looked_up(table, row, column):
    value = jnp.int32(0)
    for i, entries in enumerate(table):
        for k, entry in enumerate(entries):
            value = value + jnp.where((row == i) & (column == k), entry, 0)
    return value


def routed_kernel(
    extent,
    plane,
    capacity,
    mid_hbm,
    cot_hbm,
    routes,
    route_weight,
    gate_hbm,
    up_hbm,
    down_hbm,
    filtered_hbm,
    out_weight_hbm,
    taps,
    gain,
    proj_out,
    input_out,
    gate_out,
    up_out,
    down_out,
    tok,
    meta,
    metas,
    picks,
    rows,
    gate,
    up,
    down,
    pre_gate,
    pre_up,
    hidden,
    gate_pre,
    up_pre,
    part_sent,
    part_got,
    ret_sent,
    ret_got,
    line_sent,
    line_got,
    total,
    tokens,
    load_sem,
    meta_sems,
    tok_send,
    tok_recv,
    row_send,
    row_recv,
    swap_send,
    swap_recv,
    part_sems,
    ret_send,
    ret_recv,
    line_send,
    line_recv,
    out_sems,
    token_sems,
    values,
    out_weight,
    stats,
    normed,
    inverse,
    active,
    blocks,
    sums_sent,
    sums_got,
    sums_own,
    padded,
    spread,
    stat_sems,
    active_send,
    active_recv,
    block_send,
    block_recv,
    block_swaps,
    sums_send,
    sums_recv,
    halo_sems,
):
    sp, tp = lax.axis_index("sp"), lax.axis_index("tp")
    z, p = sp // plane, sp % plane
    slots = plane * capacity
    token_count, width = tok.shape[2], tok.shape[3]
    other = 1 - tp
    step = width // extent
    columns = extent
    orders, relays = chunk_orders(extent), relay_orders(extent)

    def remote(src, dst, send, recv, to_sp, to_tp):
        return pltpu.make_async_remote_copy(
            src_ref=src,
            dst_ref=dst,
            send_sem=send,
            recv_sem=recv,
            device_id=(to_sp, to_tp),
            device_id_type=MESH,
        )

    loads = [
        pltpu.make_async_copy(mid_hbm, tok.at[0, z], load_sem.at[0]),
        pltpu.make_async_copy(cot_hbm, tok.at[1, z], load_sem.at[1]),
        pltpu.make_async_copy(gate_hbm, gate, load_sem.at[2]),
        pltpu.make_async_copy(up_hbm, up, load_sem.at[3]),
        pltpu.make_async_copy(down_hbm, down, load_sem.at[4]),
        pltpu.make_async_copy(filtered_hbm, values, load_sem.at[5]),
        pltpu.make_async_copy(out_weight_hbm, out_weight, load_sem.at[6]),
    ]
    for load in loads:
        load.start()
    experts = extent * plane
    chosen = [
        lax.broadcasted_iota(jnp.int32, (experts, token_count), 0) == routes[k : k + 1, :]
        for k in range(TOPK_ROWS)
    ]
    taken = jnp.where(chosen[0] | chosen[1], 1.0, 0.0).astype(jnp.bfloat16)
    square = (token_count, token_count)
    before = lax.broadcasted_iota(jnp.int32, square, 0) < lax.broadcasted_iota(jnp.int32, square, 1)
    earlier = jnp.dot(
        taken,
        jnp.where(before, 1.0, 0.0).astype(jnp.bfloat16),
        preferred_element_type=jnp.float32,
    )
    for k in range(TOPK_ROWS):
        place = jnp.sum(jnp.where(chosen[k], earlier, 0.0), axis=0, keepdims=True)
        meta[k : k + 1, :] = place + (routes[k : k + 1, :] * capacity).astype(jnp.float32)
        meta[TOPK_ROWS + k : TOPK_ROWS + k + 1, :] = route_weight[k : k + 1, :]
    meta[2 * TOPK_ROWS :, :] = jnp.zeros((8 - 2 * TOPK_ROWS, token_count), jnp.float32)
    metas[z] = meta[...]

    barrier = pltpu.get_barrier_semaphore()

    def greet(to_sp, to_tp):
        pl.semaphore_signal(barrier, inc=1, device_id=(to_sp, to_tp), device_id_type=MESH)

    def line_peer(i):
        return lax.rem(z + i, extent)

    def plane_peer(i):
        return lax.rem(p + i, plane)

    for i in range(1, extent):
        greet(line_peer(i) * plane + p, tp)

    @pl.loop(1, plane)
    def _(i):
        greet(z * plane + plane_peer(i), tp)

    greet(sp, other)
    last_sp = extent * plane - 1

    @pl.when(sp > 0)
    def _():
        greet(sp - 1, tp)

    @pl.when(sp < last_sp)
    def _():
        greet(sp + 1, tp)

    ends = jnp.where(sp > 0, 1, 0) + jnp.where(sp < last_sp, 1, 0)
    pl.semaphore_wait(barrier, extent - 1 + plane - 1 + 1 + ends)

    def meta_copy(to_z, from_z):
        return remote(
            meta, metas.at[from_z], meta_sems.at[0, to_z], meta_sems.at[1, from_z], to_z * plane + p, tp
        )

    def tok_copy(t, origin, up_way):
        to_z = z + 1 if up_way else z - 1
        return remote(
            tok.at[t, origin],
            tok.at[t, origin],
            tok_send.at[t, origin, int(up_way)],
            tok_recv.at[t, origin],
            to_z * plane + p,
            tp,
        )

    def forwards(origin, up_way):
        if up_way:
            return (origin <= z) & (z < extent - 1)
        return (origin >= z) & (z > 0)

    def row_copy(t, origin, q):
        return remote(
            picks.at[t, origin, q],
            rows.at[t, origin, 0, p],
            row_send.at[t, origin, q],
            row_recv.at[t, origin, p],
            z * plane + q,
            tp,
        )

    def row_arrival(t, origin, q):
        return remote(
            picks.at[t, origin, q],
            rows.at[t, origin, 0, q],
            row_send.at[t, origin, q],
            row_recv.at[t, origin, q],
            z * plane + q,
            tp,
        )

    def swap_copy(t, origin):
        return remote(
            rows.at[t, origin, 0],
            rows.at[t, origin, 1],
            swap_send.at[t, origin],
            swap_recv.at[t, origin],
            sp,
            other,
        )

    def part_copy(origin):
        return remote(
            part_sent.at[origin],
            part_got.at[origin],
            part_sems.at[0, origin],
            part_sems.at[1, origin],
            sp,
            other,
        )

    def ret_copy(origin, q):
        return remote(
            ret_sent.at[origin, q],
            ret_got.at[origin, p],
            ret_send.at[origin, q],
            ret_recv.at[origin, p],
            z * plane + q,
            tp,
        )

    def ret_arrival(origin, q):
        return remote(
            ret_sent.at[origin, q],
            ret_got.at[origin, q],
            ret_send.at[origin, q],
            ret_recv.at[origin, q],
            z * plane + q,
            tp,
        )

    def band(j):
        return pl.ds(pl.multiple_of(j * step, step), step)

    def band_for(home, jj):
        return looked_up(sum_orders(extent), home, jj)

    def line_copy(home, j):
        to_z = jnp.where(home > z, z + 1, z - 1)
        slot = jnp.where((home < z) & (to_z == home), extent, home)
        return remote(
            line_sent.at[home, :, band(j)],
            line_got.at[slot, :, band(j)],
            line_send.at[home, j],
            line_recv.at[slot, j],
            to_z * plane + p,
            tp,
        )

    def line_arrival(slot, j):
        return remote(
            line_sent.at[0, :, band(j)],
            line_got.at[slot, :, band(j)],
            line_send.at[0, j],
            line_recv.at[slot, j],
            z * plane + p,
            other,
        )

    def has_inflow(home):
        return ((home > z) & (z > 0)) | ((home < z) & (z < extent - 1))

    def hits(origin):
        slot = lax.broadcasted_iota(jnp.int32, (slots, token_count), 0) + z * slots
        slot = slot.astype(jnp.float32)
        return [slot == metas[origin, pl.ds(k, 1), :] for k in range(TOPK_ROWS)]

    def chooser(origin):
        first, second = hits(origin)
        return jnp.where(first | second, 1.0, 0.0).astype(jnp.bfloat16)

    def scale_of(origin):
        first, second = hits(origin)
        weighted = jnp.where(first, metas[origin, pl.ds(TOPK_ROWS, 1), :], 0.0) + jnp.where(
            second, metas[origin, pl.ds(TOPK_ROWS + 1, 1), :], 0.0
        )
        return jnp.sum(weighted, axis=1, keepdims=True)

    def late(up_way):
        if extent < 3:
            return False
        return (z == extent - 2) if up_way else (z == 1)

    def send_own(t, held_back):
        for up_way in (False, True):
            now = forwards(z, up_way)
            if t == 1 and extent > 2:
                now = now & (late(up_way) == held_back)
            elif held_back:
                continue

            @pl.when(now)
            def _():
                tok_copy(t, z, up_way).start()

    def forward(t, distance):
        below = lax.rem(z - distance + extent, extent)
        above = lax.rem(z + distance, extent)
        for origin, up_way, there in (
            (above, False, (z + distance < extent) & (z > 0)),
            (below, True, (z >= distance) & (z < extent - 1)),
        ):

            @pl.when(there)
            def _():
                tok_copy(t, origin, up_way).wait_recv()
                tok_copy(t, origin, up_way).start()

        if t == 1 and extent > 2:

            @pl.when(distance == extent - 2)
            def _():
                send_own(1, True)

    def arrive(t, origin):
        @pl.when((origin != z) & jnp.logical_not(has_inflow(origin)))
        def _():
            tok_copy(t, origin, True).wait_recv()

        @pl.when((origin != z) & (t == 0))
        def _():
            meta_copy(origin, origin).wait_recv()

        select = chooser(origin)
        scale = jnp.where(t == 1, scale_of(origin), 1.0)
        for j in range(columns):
            picked = scale * jnp.dot(
                select, tok[t, origin, :, band(j)], preferred_element_type=jnp.float32
            )
            picks[t, origin, :, :, band(j)] = picked.astype(jnp.bfloat16).reshape(
                plane, capacity, step
            )

        @pl.loop(1, plane)
        def _(i):
            row_copy(t, origin, plane_peer(i)).start()

        rows[t, origin, 0, p] = picks[t, origin, p]

    def event(i):
        kinds = [[t for t, _ in row] for row in pick_events(extent)]
        origins = [[origin for _, origin in row] for row in pick_events(extent)]
        arrive(looked_up(kinds, z, i), looked_up(origins, z, i))

    def swap(t, k):
        origin = looked_up(orders, z, k)

        @pl.loop(1, plane)
        def _(i):
            row_arrival(t, origin, plane_peer(i)).wait_recv()

        swap_copy(t, origin).start()

    def expert_rows(t, origin):
        return rows[t, origin].reshape(2 * slots, width)

    half = gate.shape[1]
    tile = min(256, half)

    def first_products(k):
        origin = looked_up(orders, z, k)

        @pl.when(k == 0)
        def _():
            loads[2].wait()
            loads[3].wait()

        swap_copy(0, origin).wait_recv()

        @pl.loop(0, half // tile)
        def _(n):
            cut = pl.ds(pl.multiple_of(n * tile, tile), tile)
            block = expert_rows(0, origin)
            pre_gate[:, cut] = jnp.dot(block, gate[:, cut], preferred_element_type=jnp.float32)
            pre_up[:, cut] = jnp.dot(block, up[:, cut], preferred_element_type=jnp.float32)

    def products(k):
        origin = looked_up(orders, z, k)

        @pl.when(k == 0)
        def _():
            loads[4].wait()

        swap_copy(1, origin).wait_recv()

        @pl.loop(0, half // tile)
        def _(n):
            cut = pl.ds(pl.multiple_of(n * tile, tile), tile)
            hidden_grad = lax.dot_general(
                expert_rows(1, origin),
                down[cut, :],
                (((1,), (1,)), ((), ())),
                preferred_element_type=jnp.float32,
            )
            g, u = pre_gate[:, cut], pre_up[:, cut]
            logistic = jax.nn.sigmoid(g)
            gate_act = g * logistic
            hidden[origin, :, cut] = (gate_act * u).astype(jnp.bfloat16)
            gate_pre[origin, :, cut] = (
                hidden_grad * u * (logistic * (1.0 + g * (1.0 - logistic)))
            ).astype(jnp.bfloat16)
            up_pre[origin, :, cut] = (hidden_grad * gate_act).astype(jnp.bfloat16)

        wide = min(256, width)

        @pl.loop(0, width // wide)
        def _(n):
            cut = pl.ds(pl.multiple_of(n * wide, wide), wide)
            part = lax.dot_general(
                gate_pre[origin],
                gate[cut, :],
                (((1,), (1,)), ((), ())),
                preferred_element_type=jnp.float32,
            ) + lax.dot_general(
                up_pre[origin],
                up[cut, :],
                (((1,), (1,)), ((), ())),
                preferred_element_type=jnp.float32,
            )
            part = part.astype(jnp.bfloat16).reshape(2, plane, capacity, wide)
            ret_sent[origin, :, :, cut] = part[0]
            part_sent[origin, :, :, cut] = part[1]

        part_copy(origin).start()

    def all_rows(t, cut):
        return rows[t, :, :, :, :, cut].reshape(extent * 2 * slots, -1)

    def small_rows(ref, cut):
        return ref[:, :, cut].reshape(extent * 2 * slots, -1)

    def weight_grads(which):
        store = pltpu.make_async_copy(
            (gate, up, down)[which], (gate_out, up_out, down_out)[which], out_sems.at[which]
        )
        size = width if which < 2 else half
        deep = min(256, size)

        @pl.loop(0, size // deep)
        def _(n):
            cut = pl.ds(pl.multiple_of(n * deep, deep), deep)
            if which < 2:
                left = all_rows(0, cut)
                right = small_rows((gate_pre, up_pre)[which], slice(None))
            else:
                left = small_rows(hidden, cut)
                right = all_rows(1, slice(None))
            (gate, up, down)[which][cut, :] = lax.dot_general(
                left, right, (((0,), (0,)), ((), ())), preferred_element_type=jnp.float32
            ).astype(jnp.bfloat16)

        store.start()
        return store

    def send_back(k):
        origin = looked_up(orders, z, k)
        part_copy(origin).wait_recv()
        for j in range(columns):
            both = ret_sent[origin, :, :, band(j)].astype(jnp.float32) + part_got[
                origin, :, :, band(j)
            ].astype(jnp.float32)
            ret_sent[origin, :, :, band(j)] = both.astype(jnp.bfloat16)

        @pl.loop(1, plane)
        def _(i):
            ret_copy(origin, plane_peer(i)).start()

        ret_got[origin, p] = ret_sent[origin, p]

    def combine(k):
        origin = looked_up(orders, z, k)

        @pl.loop(1, plane)
        def _(i):
            ret_arrival(origin, plane_peer(i)).wait_recv()

        select = chooser(origin)
        for jj in range(columns):
            j = band_for(origin, jj)
            back = ret_got[origin, :, :, band(j)].reshape(slots, step)
            added = lax.dot_general(
                select, back, (((0,), (0,)), ((), ())), preferred_element_type=jnp.float32
            )

            @pl.when(origin == z)
            def _():
                total[:, band(j)] = added

            @pl.when(origin != z)
            def _():
                line_sent[origin, :, band(j)] = added.astype(jnp.bfloat16)

            @pl.when((origin != z) & jnp.logical_not(has_inflow(origin)))
            def _():
                line_copy(origin, j).start()

    def line_relay(k):
        home = looked_up(relays, z, k)

        @pl.when(has_inflow(home))
        def _():
            for jj in range(columns):
                j = band_for(home, jj)
                line_arrival(home, j).wait_recv()
                line_sent[home, :, band(j)] = (
                    line_sent[home, :, band(j)].astype(jnp.float32)
                    + line_got[home, :, band(j)].astype(jnp.float32)
                ).astype(jnp.bfloat16)
                line_copy(home, j).start()

    for load in loads[:2]:
        load.wait()
    for i in range(1, extent):
        meta_copy(line_peer(i), z).start()

    local = values.shape[1]
    strip = min(256, local)
    strips = local // strip
    row_count = values.shape[0]

    def strip_at(n):
        return pl.ds(pl.multiple_of(n * strip, strip), strip)

    def stat_copy(i):
        return remote(
            stats.at[i, 0], stats.at[i, 1], stat_sems.at[0, i], stat_sems.at[1, i], sp, other
        )

    def paired(i, first, second):
        lane = lax.broadcasted_iota(jnp.int32, (row_count, stats.shape[3]), 1)
        stats[i, 0] = jnp.where(lane == 0, first, second)
        stat_copy(i).start()

    def both_sums(i):
        stat_copy(i).wait_recv()
        merged = (stats[i, 0] + stats[i, 1]) / width
        return merged[:, 0:1], merged[:, 1:2]

    share = row_count // extent

    def active_copy(q, owner, i):
        part = active.at[owner, pl.ds(i * share, share)]
        return remote(
            part, part, active_send.at[q, i], active_recv.at[owner, i], z * plane + q, tp
        )

    def prepare():
        loads[5].wait()
        sums = jnp.zeros((row_count, 1), jnp.float32)
        squares = jnp.zeros((row_count, 1), jnp.float32)
        for n in range(strips):
            block = values[:, n * strip : (n + 1) * strip].astype(jnp.float32)
            sums = sums + jnp.sum(block, axis=1, keepdims=True)
            squares = squares + jnp.sum(block * block, axis=1, keepdims=True)
        paired(0, sums, squares)
        average, second = both_sums(0)
        scale = lax.rsqrt(second - average * average + NORM_EPS)
        inverse[...] = jnp.broadcast_to(scale, inverse.shape)
        for n in range(strips):
            cut = slice(n * strip, (n + 1) * strip)
            flat = (values[:, cut].astype(jnp.float32) - average) * scale
            normed[:, cut] = flat
            scaled = flat * gain[:, cut]
            active[p, :, cut] = (scaled * jax.nn.sigmoid(scaled)).astype(jnp.bfloat16)

    def share_active(k):
        @pl.loop(1, plane)
        def _(i):
            active_copy(plane_peer(i), p, k).start()

    send_own(0, False)
    send_own(1, False)
    arrive(0, z)
    arrive(1, z)
    prepare()

    @pl.loop(0, extent)
    def _(k):
        @pl.when(k > 0)
        def _():
            forward(1, k)

        swap(0, k)
        first_products(k)

        @pl.when(k == 0)
        def _():
            forward(0, 1)

        @pl.when(k < extent - 1)
        def _():
            event(2 * k)

        @pl.when((k > 0) & (k < extent - 1))
        def _():
            forward(0, k + 1)

        @pl.when((k > 0) & (k < extent - 1))
        def _():
            combine(k - 1)

        swap(1, k)
        share_active(k)
        products(k)

        @pl.when(k < extent - 1)
        def _():
            event(2 * k + 1)

        @pl.when(k == extent - 1)
        def _():
            combine(k - 1)

        send_back(k)

    line_relay(0)
    combine(extent - 1)

    stores = [weight_grads(0)]
    if extent > 2:
        line_relay(1)
    stores.append(weight_grads(1))

    @pl.loop(2, extent - 1)
    def _(k):
        line_relay(k)

    stores.append(weight_grads(2))

    own_block = width // (extent * plane)
    lanes = blocks.shape[4]

    def block_at(j, q):
        start = (j * plane + q) * own_block
        return pl.ds(pl.multiple_of(start // lanes * lanes, lanes), lanes)

    def token_copy(j):
        return remote(
            tokens.at[tp, :, band(j)],
            tokens.at[tp, :, band(j)],
            token_sems.at[0, j],
            token_sems.at[1, j],
            sp,
            other,
        )

    def token_arrival(j):
        return remote(
            tokens.at[other, :, band(j)],
            tokens.at[other, :, band(j)],
            token_sems.at[0, j],
            token_sems.at[1, j],
            sp,
            other,
        )

    def block_copy(j, q):
        return remote(
            tokens.at[tp, :, block_at(j, q)],
            blocks.at[j, tp, p],
            block_send.at[j, q],
            block_recv.at[j, p],
            z * plane + q,
            tp,
        )

    def block_arrival(j, q):
        return remote(
            tokens.at[tp, :, block_at(j, q)],
            blocks.at[j, tp, q],
            block_send.at[j, q],
            block_recv.at[j, q],
            z * plane + q,
            tp,
        )

    def block_swap(j):
        return remote(
            blocks.at[j, tp],
            blocks.at[j, tp],
            block_swaps.at[0, j],
            block_swaps.at[1, j],
            sp,
            other,
        )

    def block_swap_arrival(j):
        return remote(
            blocks.at[j, other],
            blocks.at[j, other],
            block_swaps.at[0, j],
            block_swaps.at[1, j],
            sp,
            other,
        )

    def home_band(jj):
        j = band_for(z, jj)
        for slot, there in ((z, z > 0), (extent, z < extent - 1)):

            @pl.when(there)
            def _():
                line_arrival(slot, j).wait_recv()
                total[:, band(j)] = total[:, band(j)] + line_got[slot, :, band(j)].astype(
                    jnp.float32
                )

        tokens[tp, :, band(j)] = (
            tok[1, z, :, band(j)].astype(jnp.float32) + total[:, band(j)]
        ).astype(jnp.bfloat16)
        token_copy(j).start()

        @pl.loop(1, plane)
        def _(i):
            block_copy(j, plane_peer(i)).start()

        blocks[j, tp, p] = tokens[tp, :, block_at(j, p)]

    def swap_block(jj):
        j = band_for(z, jj)

        @pl.loop(1, plane)
        def _(i):
            block_arrival(j, plane_peer(i)).wait_recv()

        block_swap(j).start()

    pieces = 2
    piece = local // pieces

    def piece_at(h):
        return pl.ds(h * piece, piece)

    def sums_copy(j, h):
        to_z = jnp.where(j > z, z + 1, z - 1)
        slot = jnp.where((j < z) & (to_z == j), extent, j)
        return remote(
            sums_sent.at[j, :, piece_at(h)],
            sums_got.at[slot, :, piece_at(h)],
            sums_send.at[j, h],
            sums_recv.at[slot, h],
            to_z * plane + p,
            tp,
        )

    def sums_arrival(slot, h):
        return remote(
            sums_sent.at[0, :, piece_at(h)],
            sums_got.at[slot, :, piece_at(h)],
            sums_send.at[0, h],
            sums_recv.at[slot, h],
            sp,
            other,
        )

    def act_grads():
        loads[6].wait()
        for j in range(columns):
            token_arrival(j).wait_recv()
        grad_sum = jnp.zeros((row_count, 1), jnp.float32)
        grad_corr = jnp.zeros((row_count, 1), jnp.float32)
        for n in range(strips):
            cut = slice(n * strip, (n + 1) * strip)
            act_grad = lax.dot_general(
                tokens[...].reshape(row_count, width),
                out_weight[cut, :],
                (((1,), (1,)), ((), ())),
                preferred_element_type=jnp.float32,
            )
            flat = normed[:, cut]
            weight = gain[:, cut]
            scaled = flat * weight
            logistic = jax.nn.sigmoid(scaled)
            slope = act_grad * (logistic * (1.0 + scaled * (1.0 - logistic))) * weight
            spread[:row_count, cut] = slope
            grad_sum = grad_sum + jnp.sum(slope, axis=1, keepdims=True)
            grad_corr = grad_corr + jnp.sum(slope * flat, axis=1, keepdims=True)
        paired(1, grad_sum, grad_corr)

    def partial_block(jj):
        j = band_for(z, jj)
        block_swap_arrival(j).wait_recv()
        at = lax.rem((j * plane + p) * own_block, lanes)
        for n in range(strips):
            cut = slice(n * strip, (n + 1) * strip)
            mine = sum(
                lax.dot_general(
                    blocks[j, side].reshape(plane * token_count, lanes),
                    active[:, side * token_count : (side + 1) * token_count, cut].reshape(
                        plane * token_count, strip
                    ),
                    (((0,), (0,)), ((), ())),
                    preferred_element_type=jnp.float32,
                )
                for side in range(2)
            )
            if own_block != lanes:
                mine = sum(
                    jnp.where(at == start, mine[start : start + own_block], 0.0)
                    for start in range(0, lanes, own_block)
                )

            @pl.when(j == z)
            def _():
                sums_own[:, cut] = mine

            @pl.when(j != z)
            def _():
                sums_sent[j, :, cut] = mine.astype(jnp.bfloat16)

        @pl.when((j != z) & jnp.logical_not(has_inflow(j)))
        def _():
            for h in range(pieces):
                sums_copy(j, h).start()

    @pl.loop(1, plane)
    def _(i):
        for k in range(extent):
            active_copy(plane_peer(i), plane_peer(i), k).wait_recv()

    @pl.loop(0, extent + 2)
    def _(jj):
        @pl.when(jj < extent)
        def _():
            home_band(jj)

        @pl.when(jj == extent)
        def _():
            act_grads()

        @pl.when((jj > 0) & (jj <= extent))
        def _():
            swap_block(jj - 1)

        @pl.when(jj > 1)
        def _():
            partial_block(jj - 2)

    mean, corr = both_sums(1)
    edge = (padded.shape[0] - row_count) // 2
    scale = inverse[:, 0:1]
    for n in range(strips):
        cut = slice(n * strip, (n + 1) * strip)
        padded[edge : edge + row_count, cut] = (
            scale * (spread[:row_count, cut] - mean - normed[:, cut] * corr)
        ).astype(jnp.bfloat16)

    def halo_copy(up_way):
        if up_way:
            src, dst, to = row_count, 0, sp + 1
        else:
            src, dst, to = edge, edge + row_count, sp - 1
        return remote(
            padded.at[pl.ds(src, edge), :],
            padded.at[pl.ds(dst, edge), :],
            halo_sems.at[0, int(up_way)],
            halo_sems.at[1, int(up_way)],
            to,
            tp,
        )

    inside = {True: sp < last_sp, False: sp > 0}
    for up_way in (True, False):

        @pl.when(inside[up_way])
        def _():
            halo_copy(up_way).start()

    def relay(k):
        j = looked_up(sum_relays(extent), z, k)

        @pl.when(has_inflow(j))
        def _():
            for h in range(pieces):
                sums_arrival(j, h).wait_recv()
                sums_sent[j, :, piece_at(h)] = (
                    sums_sent[j, :, piece_at(h)].astype(jnp.float32)
                    + sums_got[j, :, piece_at(h)].astype(jnp.float32)
                ).astype(jnp.bfloat16)
                sums_copy(j, h).start()

    relay(0)
    tap_count = taps.shape[0]
    reach = tap_count // 2
    narrow = min(128, local)
    extra = (edge + reach) // 8 * 8

    def convolve(first, count):
        @pl.loop(0, local // narrow)
        def _(n):
            cut = pl.ds(pl.multiple_of(n * narrow, narrow), narrow)
            acc = jnp.zeros((count, narrow), jnp.float32)
            for s in range(8):
                taps_at = [o for o in range(tap_count) if (edge + reach - o) % 8 == s]
                if not taps_at:
                    continue
                shifted = spread[first + s : first + s + extra + count, cut]
                for o in taps_at:
                    m = (edge + reach - o) // 8 * 8
                    acc = acc + taps[o : o + 1, cut] * shifted[m : m + count]
            values[first : first + count, cut] = acc.astype(jnp.bfloat16)

    inner = slice(edge, edge + row_count)
    spread[inner] = padded[inner].astype(jnp.float32)
    if row_count > 2 * edge:
        convolve(edge, row_count - 2 * edge)
    for k in range(1, extent - 1):
        relay(k)
    for up_way in (True, False):
        at = 0 if up_way else edge + row_count

        @pl.when(inside[not up_way])
        def _():
            halo_copy(up_way).wait_recv()
            spread[at : at + edge, :] = padded[at : at + edge, :].astype(jnp.float32)

        @pl.when(jnp.logical_not(inside[not up_way]))
        def _():
            spread[at : at + edge, :] = jnp.zeros((edge, local), jnp.float32)

    convolve(0, edge)
    convolve(row_count - edge, edge)
    finish = pltpu.make_async_copy(values, input_out, load_sem.at[0])
    finish.start()
    for h in range(pieces):
        for slot, there in ((z, z > 0), (extent, z < extent - 1)):

            @pl.when(there)
            def _():
                sums_arrival(slot, h).wait_recv()
                sums_own[:, piece_at(h)] = sums_own[:, piece_at(h)] + sums_got[
                    slot, :, piece_at(h)
                ].astype(jnp.float32)

    store = pltpu.make_async_copy(sums_own, proj_out, load_sem.at[1])
    store.start()
    for i in range(2):
        stat_copy(i).wait_send()
    for up_way in (True, False):

        @pl.when(inside[up_way])
        def _():
            halo_copy(up_way).wait_send()

    @pl.loop(1, plane)
    def _(i):
        for k in range(extent):
            active_copy(plane_peer(i), p, k).wait_send()

    for j in range(columns):
        token_copy(j).wait_send()

        @pl.loop(1, plane)
        def _(i):
            block_copy(j, plane_peer(i)).wait_send()

        block_swap(j).wait_send()

        @pl.when(z != j)
        def _():
            for h in range(pieces):
                sums_copy(j, h).wait_send()

    for i in range(1, extent):
        meta_copy(line_peer(i), z).wait_send()

    @pl.loop(0, extent)
    def _(origin):
        for t in range(2):
            for up_way in (False, True):

                @pl.when(forwards(origin, up_way))
                def _():
                    tok_copy(t, origin, up_way).wait_send()

            @pl.loop(1, plane)
            def _(i):
                row_copy(t, origin, plane_peer(i)).wait_send()

            swap_copy(t, origin).wait_send()
        part_copy(origin).wait_send()

        @pl.loop(1, plane)
        def _(i):
            ret_copy(origin, plane_peer(i)).wait_send()

        @pl.when(origin != z)
        def _():
            for j in range(columns):
                line_copy(origin, j).wait_send()


    finish.wait()
    store.wait()
    for store in stores:
        store.wait()


TOPK_ROWS = 2


def routed_backward(
    mid_rows,
    cotangent,
    routes,
    route_weight,
    gate_mat,
    up_mat,
    down_mat,
    filtered,
    out_weight,
    taps,
    gain,
    capacity,
):
    sp_count = lax.axis_size("sp")
    extent = line_extent(sp_count)
    plane = sp_count // extent
    token_count, width = mid_rows.shape
    half = gate_mat.shape[1]
    slots = plane * capacity
    kind = jnp.bfloat16
    any_space = pl.BlockSpec(memory_space=pl.ANY)
    vmem = pl.BlockSpec(memory_space=pltpu.VMEM)
    dma = pltpu.SemaphoreType.DMA
    columns = extent
    row_count, local = filtered.shape
    own_block = width // sp_count
    lanes = min(max(own_block, 128), width // extent)
    edge = -(-(taps.shape[0] // 2) // 16) * 16
    rows_shape = (extent, 2, plane, capacity, width)
    small_shape = (extent, 2 * slots, half)
    scratch = [
        pltpu.VMEM((2, extent, token_count, width), kind),
        pltpu.VMEM((8, token_count), jnp.float32),
        pltpu.VMEM((extent, 8, token_count), jnp.float32),
        pltpu.VMEM((2, extent, plane, capacity, width), kind),
        pltpu.VMEM((2,) + rows_shape, kind),
        pltpu.VMEM(gate_mat.shape, kind),
        pltpu.VMEM(up_mat.shape, kind),
        pltpu.VMEM(down_mat.shape, kind),
        pltpu.VMEM((2 * slots, half), jnp.float32),
        pltpu.VMEM((2 * slots, half), jnp.float32),
        pltpu.VMEM(small_shape, kind),
        pltpu.VMEM(small_shape, kind),
        pltpu.VMEM(small_shape, kind),
        pltpu.VMEM((extent, plane, capacity, width), kind),
        pltpu.VMEM((extent, plane, capacity, width), kind),
        pltpu.VMEM((extent, plane, capacity, width), kind),
        pltpu.VMEM((extent, plane, capacity, width), kind),
        pltpu.VMEM((extent, token_count, width), kind),
        pltpu.VMEM((extent + 1, token_count, width), kind),
        pltpu.VMEM((token_count, width), jnp.float32),
        pltpu.VMEM((2, token_count, width), kind),
        dma((7,)),
        dma((2, extent)),
        dma((2, extent, 2)),
        dma((2, extent)),
        dma((2, extent, plane)),
        dma((2, extent, plane)),
        dma((2, extent)),
        dma((2, extent)),
        dma((2, extent)),
        dma((extent, plane)),
        dma((extent, plane)),
        dma((extent, columns)),
        dma((extent + 1, columns)),
        dma((3,)),
        dma((2, columns)),
        pltpu.VMEM((row_count, local), kind),
        pltpu.VMEM(out_weight.shape, kind),
        pltpu.VMEM((2, 2, row_count, 128), jnp.float32),
        pltpu.VMEM((row_count, local), jnp.float32),
        pltpu.VMEM((row_count, 128), jnp.float32),
        pltpu.VMEM((plane, row_count, local), kind),
        pltpu.VMEM((extent, 2, plane, token_count, lanes), kind),
        pltpu.VMEM((extent, own_block, local), kind),
        pltpu.VMEM((extent + 1, own_block, local), kind),
        pltpu.VMEM((own_block, local), jnp.float32),
        pltpu.VMEM((row_count + 2 * edge, local), kind),
        pltpu.VMEM((row_count + 2 * edge, local), jnp.float32),
        dma((2, 2)),
        dma((plane, extent)),
        dma((plane, extent)),
        dma((extent, plane)),
        dma((extent, plane)),
        dma((2, extent)),
        dma((extent, 2)),
        dma((extent + 1, 2)),
        dma((2, 2)),
    ]
    held = sum(
        math.prod(s.shape) * jnp.dtype(s.dtype).itemsize
        for s in scratch
        if s.memory_space == pltpu.VMEM
    )
    out = pl.pallas_call(
        functools.partial(routed_kernel, extent, plane, capacity),
        out_shape=[
            jax.ShapeDtypeStruct((own_block, local), jnp.float32),
            jax.ShapeDtypeStruct((row_count, local), kind),
            jax.ShapeDtypeStruct(gate_mat.shape, kind),
            jax.ShapeDtypeStruct(up_mat.shape, kind),
            jax.ShapeDtypeStruct(down_mat.shape, kind),
        ],
        in_specs=[any_space] * 2 + [vmem] * 2 + [any_space] * 5 + [vmem] * 2,
        out_specs=[any_space] * 5,
        scratch_shapes=scratch,
        compiler_params=pltpu.CompilerParams(
            collective_id=0, has_side_effects=True, vmem_limit_bytes=min(held + SPARE, 67_043_328)
        ),
    )(
        mid_rows,
        cotangent,
        routes,
        route_weight,
        gate_mat,
        up_mat,
        down_mat,
        filtered,
        out_weight,
        taps,
        gain,
    )
    return out


def per_device(
    mid_rows,
    cotangent,
    routes,
    route_weight,
    filtered,
    conv_taps,
    norm_gain,
    out_weight,
    gate_weight,
    up_weight,
    down_weight,
):
    sp_count = lax.axis_size("sp")
    token_count, model_width = mid_rows.shape
    per_token = routes.shape[1]
    local_experts = gate_weight.shape[0]
    experts = local_experts * sp_count
    capacity = 2 * token_count * per_token // sp_count
    proj_grad, input_grad, *weight_grads = routed_backward(
        mid_rows,
        cotangent,
        routes.T,
        route_weight.T,
        gate_weight[0],
        up_weight[0],
        down_weight[0],
        filtered,
        out_weight,
        conv_taps,
        norm_gain[None],
        capacity,
    )
    gate_grad, up_grad, down_grad = (grad.astype(jnp.float32)[None] for grad in weight_grads)
    return (gate_grad, up_grad, down_grad, proj_grad, input_grad)


def solution(mesh):
    in_specs = (
        P(("sp", "tp"), None),
        P(("sp", "tp"), None),
        P(("sp", "tp"), None),
        P(("sp", "tp"), None),
        P("sp", "tp"),
        P(None, "tp"),
        P("tp"),
        P("tp", None),
        P("sp", None, "tp"),
        P("sp", None, "tp"),
        P("sp", "tp", None),
    )
    out_specs = (
        P("sp", None, "tp"),
        P("sp", None, "tp"),
        P("sp", "tp", None),
        P("sp", "tp"),
        P("sp", "tp"),
    )
    return jax.shard_map(
        per_device, mesh=mesh, in_specs=in_specs, out_specs=out_specs, check_vma=False
    )
```

```python
import functools
import math

import jax
import jax.numpy as jnp
from jax import lax
from jax.experimental import pallas as pl
from jax.experimental.pallas import tpu as pltpu
from jax.sharding import PartitionSpec as P

MESH = pl.DeviceIdType.MESH
NORM_EPS = 1e-05
SPARE = 4 << 20


def line_extent(count):
    bits = count.bit_length() - 1
    return 1 << -(-bits // 3)


def chunk_orders(extent):
    orders = []
    for own in range(extent):
        toward = [i for i in range(own + 1, extent)] if 2 * own < extent - 1 else [i for i in range(own - 1, -1, -1)]
        back = [i for i in range(extent) if i != own and i not in toward]
        back.sort(key=lambda i: abs(i - own))
        if own in (0, extent - 1):
            order = toward[1:] + toward[:1]
        else:
            order = toward[:1] + back + toward[1:]
        orders.append([own] + order)
    return orders


def pick_events(extent):
    table = []
    for own, order in enumerate(chunk_orders(extent)):
        rest = order[1:]
        if own in (0, extent - 1):
            near, far = rest[-1], rest[:-1]
            events = [(0, near)] + [(t, i) for i in far for t in range(2)] + [(1, near)]
        else:
            near = [i for i in rest if abs(i - own) == 1]
            far = [i for i in rest if abs(i - own) > 1]
            events = [(t, i) for t in range(2) for i in near]
            events = events + [(t, i) for i in far for t in range(2)]
        table.append(events)
    return table


def relay_orders(extent):
    return [
        sorted(
            (i for i in range(extent) if i != own),
            key=lambda i: (own if i > own else extent - 1 - own, abs(i - own)),
        )
        for own in range(extent)
    ]


def sum_orders(extent):
    return [
        sorted((i for i in range(extent) if i != own), key=lambda i: -abs(i - own)) + [own]
        for own in range(extent)
    ]


def sum_relays(extent):
    return [
        sorted(
            (i for i in range(extent) if i != own),
            key=lambda i: (own if i > own else extent - 1 - own, -abs(i - own)),
        )
        for own in range(extent)
    ]


def looked_up(table, row, column):
    value = jnp.int32(0)
    for i, entries in enumerate(table):
        for k, entry in enumerate(entries):
            value = value + jnp.where((row == i) & (column == k), entry, 0)
    return value


def routed_kernel(
    extent,
    plane,
    capacity,
    mid_hbm,
    cot_hbm,
    routes,
    route_weight,
    gate_hbm,
    up_hbm,
    down_hbm,
    filtered_hbm,
    out_weight_hbm,
    taps,
    gain,
    proj_out,
    input_out,
    gate_out,
    up_out,
    down_out,
    tok,
    meta,
    metas,
    picks,
    rows,
    gate,
    up,
    down,
    pre_gate,
    pre_up,
    hidden,
    gate_pre,
    up_pre,
    part_sent,
    part_got,
    ret_sent,
    ret_got,
    line_sent,
    line_got,
    total,
    tokens,
    load_sem,
    meta_sems,
    tok_send,
    tok_recv,
    row_send,
    row_recv,
    swap_send,
    swap_recv,
    part_sems,
    ret_send,
    ret_recv,
    line_send,
    line_recv,
    out_sems,
    token_sems,
    values,
    out_weight,
    stats,
    normed,
    inverse,
    active,
    blocks,
    sums_sent,
    sums_got,
    sums_own,
    padded,
    spread,
    stat_sems,
    active_send,
    active_recv,
    block_send,
    block_recv,
    block_swaps,
    sums_send,
    sums_recv,
    halo_sems,
):
    sp, tp = lax.axis_index("sp"), lax.axis_index("tp")
    z, p = sp // plane, sp % plane
    slots = plane * capacity
    token_count, width = tok.shape[2], tok.shape[3]
    other = 1 - tp
    step = width // extent
    columns = extent
    orders, relays = chunk_orders(extent), relay_orders(extent)

    def remote(src, dst, send, recv, to_sp, to_tp):
        return pltpu.make_async_remote_copy(
            src_ref=src,
            dst_ref=dst,
            send_sem=send,
            recv_sem=recv,
            device_id=(to_sp, to_tp),
            device_id_type=MESH,
        )

    loads = [
        pltpu.make_async_copy(mid_hbm, tok.at[0, z], load_sem.at[0]),
        pltpu.make_async_copy(cot_hbm, tok.at[1, z], load_sem.at[1]),
        pltpu.make_async_copy(gate_hbm, gate, load_sem.at[2]),
        pltpu.make_async_copy(up_hbm, up, load_sem.at[3]),
        pltpu.make_async_copy(down_hbm, down, load_sem.at[4]),
        pltpu.make_async_copy(filtered_hbm, values, load_sem.at[5]),
        pltpu.make_async_copy(out_weight_hbm, out_weight, load_sem.at[6]),
    ]
    for load in loads:
        load.start()
    experts = extent * plane
    chosen = [
        lax.broadcasted_iota(jnp.int32, (experts, token_count), 0) == routes[k : k + 1, :]
        for k in range(TOPK_ROWS)
    ]
    taken = jnp.where(chosen[0] | chosen[1], 1.0, 0.0).astype(jnp.bfloat16)
    square = (token_count, token_count)
    before = lax.broadcasted_iota(jnp.int32, square, 0) < lax.broadcasted_iota(jnp.int32, square, 1)
    earlier = jnp.dot(
        taken,
        jnp.where(before, 1.0, 0.0).astype(jnp.bfloat16),
        preferred_element_type=jnp.float32,
    )
    for k in range(TOPK_ROWS):
        place = jnp.sum(jnp.where(chosen[k], earlier, 0.0), axis=0, keepdims=True)
        meta[k : k + 1, :] = place + (routes[k : k + 1, :] * capacity).astype(jnp.float32)
        meta[TOPK_ROWS + k : TOPK_ROWS + k + 1, :] = route_weight[k : k + 1, :]
    meta[2 * TOPK_ROWS :, :] = jnp.zeros((8 - 2 * TOPK_ROWS, token_count), jnp.float32)
    metas[z] = meta[...]

    barrier = pltpu.get_barrier_semaphore()

    def greet(to_sp, to_tp):
        pl.semaphore_signal(barrier, inc=1, device_id=(to_sp, to_tp), device_id_type=MESH)

    def line_peer(i):
        return lax.rem(z + i, extent)

    def plane_peer(i):
        return lax.rem(p + i, plane)

    for i in range(1, extent):
        greet(line_peer(i) * plane + p, tp)

    @pl.loop(1, plane)
    def _(i):
        greet(z * plane + plane_peer(i), tp)

    greet(sp, other)
    last_sp = extent * plane - 1

    @pl.when(sp > 0)
    def _():
        greet(sp - 1, tp)

    @pl.when(sp < last_sp)
    def _():
        greet(sp + 1, tp)

    ends = jnp.where(sp > 0, 1, 0) + jnp.where(sp < last_sp, 1, 0)
    pl.semaphore_wait(barrier, extent - 1 + plane - 1 + 1 + ends)

    def meta_copy(to_z, from_z):
        return remote(
            meta, metas.at[from_z], meta_sems.at[0, to_z], meta_sems.at[1, from_z], to_z * plane + p, tp
        )

    def tok_copy(t, origin, up_way):
        to_z = z + 1 if up_way else z - 1
        return remote(
            tok.at[t, origin],
            tok.at[t, origin],
            tok_send.at[t, origin, int(up_way)],
            tok_recv.at[t, origin],
            to_z * plane + p,
            tp,
        )

    def forwards(origin, up_way):
        if up_way:
            return (origin <= z) & (z < extent - 1)
        return (origin >= z) & (z > 0)

    def row_copy(t, origin, q):
        return remote(
            picks.at[t, origin, q],
            rows.at[t, origin, 0, p],
            row_send.at[t, origin, q],
            row_recv.at[t, origin, p],
            z * plane + q,
            tp,
        )

    def row_arrival(t, origin, q):
        return remote(
            picks.at[t, origin, q],
            rows.at[t, origin, 0, q],
            row_send.at[t, origin, q],
            row_recv.at[t, origin, q],
            z * plane + q,
            tp,
        )

    def swap_copy(t, origin):
        return remote(
            rows.at[t, origin, 0],
            rows.at[t, origin, 1],
            swap_send.at[t, origin],
            swap_recv.at[t, origin],
            sp,
            other,
        )

    def part_copy(origin):
        return remote(
            part_sent.at[origin],
            part_got.at[origin],
            part_sems.at[0, origin],
            part_sems.at[1, origin],
            sp,
            other,
        )

    def ret_copy(origin, q):
        return remote(
            ret_sent.at[origin, q],
            ret_got.at[origin, p],
            ret_send.at[origin, q],
            ret_recv.at[origin, p],
            z * plane + q,
            tp,
        )

    def ret_arrival(origin, q):
        return remote(
            ret_sent.at[origin, q],
            ret_got.at[origin, q],
            ret_send.at[origin, q],
            ret_recv.at[origin, q],
            z * plane + q,
            tp,
        )

    def band(j):
        return pl.ds(pl.multiple_of(j * step, step), step)

    def band_for(home, jj):
        return looked_up(sum_orders(extent), home, jj)

    def line_copy(home, j):
        to_z = jnp.where(home > z, z + 1, z - 1)
        slot = jnp.where((home < z) & (to_z == home), extent, home)
        return remote(
            line_sent.at[home, :, band(j)],
            line_got.at[slot, :, band(j)],
            line_send.at[home, j],
            line_recv.at[slot, j],
            to_z * plane + p,
            tp,
        )

    def line_arrival(slot, j):
        return remote(
            line_sent.at[0, :, band(j)],
            line_got.at[slot, :, band(j)],
            line_send.at[0, j],
            line_recv.at[slot, j],
            z * plane + p,
            other,
        )

    def has_inflow(home):
        return ((home > z) & (z > 0)) | ((home < z) & (z < extent - 1))

    def hits(origin):
        slot = lax.broadcasted_iota(jnp.int32, (slots, token_count), 0) + z * slots
        slot = slot.astype(jnp.float32)
        return [slot == metas[origin, pl.ds(k, 1), :] for k in range(TOPK_ROWS)]

    def chooser(origin):
        first, second = hits(origin)
        return jnp.where(first | second, 1.0, 0.0).astype(jnp.bfloat16)

    def scale_of(origin):
        first, second = hits(origin)
        weighted = jnp.where(first, metas[origin, pl.ds(TOPK_ROWS, 1), :], 0.0) + jnp.where(
            second, metas[origin, pl.ds(TOPK_ROWS + 1, 1), :], 0.0
        )
        return jnp.sum(weighted, axis=1, keepdims=True)

    def late(up_way):
        return (z == extent - 2) if up_way else (z == 1)

    def send_own(t):
        for up_way in (False, True):
            whole = forwards(z, up_way)
            if t == 1 and extent > 3:
                whole = whole & jnp.logical_not(late(up_way))

            @pl.when(whole)
            def _():
                tok_copy(t, z, up_way).start()

    def forward(t, distance):
        below = lax.rem(z - distance + extent, extent)
        above = lax.rem(z + distance, extent)
        for origin, up_way, there in (
            (above, False, (z + distance < extent) & (z > 0)),
            (below, True, (z >= distance) & (z < extent - 1)),
        ):

            @pl.when(there)
            def _():
                tok_copy(t, origin, up_way).wait_recv()
                tok_copy(t, origin, up_way).start()

        if t == 1 and extent > 3:
            for up_way in (False, True):

                @pl.when((distance == extent - 2) & late(up_way))
                def _():
                    tok_copy(1, z, up_way).start()

    def arrive(t, origin):
        @pl.when((origin != z) & jnp.logical_not(has_inflow(origin)))
        def _():
            tok_copy(t, origin, True).wait_recv()

        @pl.when((origin != z) & (t == 0))
        def _():
            meta_copy(origin, origin).wait_recv()

        select = chooser(origin)
        scale = jnp.where(t == 1, scale_of(origin), 1.0)
        for j in range(columns):
            picked = scale * jnp.dot(
                select, tok[t, origin, :, band(j)], preferred_element_type=jnp.float32
            )
            picks[t, origin, :, :, band(j)] = picked.astype(jnp.bfloat16).reshape(
                plane, capacity, step
            )

        @pl.loop(1, plane)
        def _(i):
            row_copy(t, origin, plane_peer(i)).start()

        rows[t, origin, 0, p] = picks[t, origin, p]

    def event(i):
        kinds = [[t for t, _ in row] for row in pick_events(extent)]
        origins = [[origin for _, origin in row] for row in pick_events(extent)]
        arrive(looked_up(kinds, z, i), looked_up(origins, z, i))

    def swap(t, k):
        origin = looked_up(orders, z, k)

        @pl.loop(1, plane)
        def _(i):
            row_arrival(t, origin, plane_peer(i)).wait_recv()

        swap_copy(t, origin).start()

    def expert_rows(t, origin):
        return rows[t, origin].reshape(2 * slots, width)

    half = gate.shape[1]
    tile = min(256, half)

    def first_products(k):
        origin = looked_up(orders, z, k)

        @pl.when(k == 0)
        def _():
            loads[2].wait()
            loads[3].wait()

        swap_copy(0, origin).wait_recv()

        @pl.loop(0, half // tile)
        def _(n):
            cut = pl.ds(pl.multiple_of(n * tile, tile), tile)
            block = expert_rows(0, origin)
            pre_gate[:, cut] = jnp.dot(block, gate[:, cut], preferred_element_type=jnp.float32)
            pre_up[:, cut] = jnp.dot(block, up[:, cut], preferred_element_type=jnp.float32)

    def products(k):
        origin = looked_up(orders, z, k)

        @pl.when(k == 0)
        def _():
            loads[4].wait()

        swap_copy(1, origin).wait_recv()

        @pl.loop(0, half // tile)
        def _(n):
            cut = pl.ds(pl.multiple_of(n * tile, tile), tile)
            hidden_grad = lax.dot_general(
                expert_rows(1, origin),
                down[cut, :],
                (((1,), (1,)), ((), ())),
                preferred_element_type=jnp.float32,
            )
            g, u = pre_gate[:, cut], pre_up[:, cut]
            logistic = jax.nn.sigmoid(g)
            gate_act = g * logistic
            hidden[origin, :, cut] = (gate_act * u).astype(jnp.bfloat16)
            gate_pre[origin, :, cut] = (
                hidden_grad * u * (logistic * (1.0 + g * (1.0 - logistic)))
            ).astype(jnp.bfloat16)
            up_pre[origin, :, cut] = (hidden_grad * gate_act).astype(jnp.bfloat16)

        wide = min(256, width)

        @pl.loop(0, width // wide)
        def _(n):
            cut = pl.ds(pl.multiple_of(n * wide, wide), wide)
            part = lax.dot_general(
                gate_pre[origin],
                gate[cut, :],
                (((1,), (1,)), ((), ())),
                preferred_element_type=jnp.float32,
            ) + lax.dot_general(
                up_pre[origin],
                up[cut, :],
                (((1,), (1,)), ((), ())),
                preferred_element_type=jnp.float32,
            )
            part = part.astype(jnp.bfloat16).reshape(2, plane, capacity, wide)
            ret_sent[origin, :, :, cut] = part[0]
            part_sent[origin, :, :, cut] = part[1]

        part_copy(origin).start()

    def all_rows(t, cut):
        return rows[t, :, :, :, :, cut].reshape(extent * 2 * slots, -1)

    def small_rows(ref, cut):
        return ref[:, :, cut].reshape(extent * 2 * slots, -1)

    def grad_store(which):
        return pltpu.make_async_copy(
            (gate, up, down)[which], (gate_out, up_out, down_out)[which], out_sems.at[which]
        )

    def grad_tiles(which, first, count, size):
        @pl.loop(first, first + count)
        def _(n):
            cut = pl.ds(pl.multiple_of(n * size, size), size)
            if which < 2:
                left = all_rows(0, cut)
                right = small_rows((gate_pre, up_pre)[which], slice(None))
            else:
                left = small_rows(hidden, cut)
                right = all_rows(1, slice(None))
            (gate, up, down)[which][cut, :] = lax.dot_general(
                left, right, (((0,), (0,)), ((), ())), preferred_element_type=jnp.float32
            ).astype(jnp.bfloat16)

    def gate_up_share(which, jj):
        size = min(256, width // columns)
        each = width // columns // size
        grad_tiles(which, jj * each, each, size)

    def send_back(k):
        origin = looked_up(orders, z, k)
        part_copy(origin).wait_recv()
        for j in range(columns):
            both = ret_sent[origin, :, :, band(j)].astype(jnp.float32) + part_got[
                origin, :, :, band(j)
            ].astype(jnp.float32)
            ret_sent[origin, :, :, band(j)] = both.astype(jnp.bfloat16)

        @pl.loop(1, plane)
        def _(i):
            ret_copy(origin, plane_peer(i)).start()

        ret_got[origin, p] = ret_sent[origin, p]

    def combine(k):
        origin = looked_up(orders, z, k)

        @pl.loop(1, plane)
        def _(i):
            ret_arrival(origin, plane_peer(i)).wait_recv()

        select = chooser(origin)
        for jj in range(columns):
            j = band_for(origin, jj)
            back = ret_got[origin, :, :, band(j)].reshape(slots, step)
            added = lax.dot_general(
                select, back, (((0,), (0,)), ((), ())), preferred_element_type=jnp.float32
            )

            @pl.when(origin == z)
            def _():
                total[:, band(j)] = added

            @pl.when(origin != z)
            def _():
                line_sent[origin, :, band(j)] = added.astype(jnp.bfloat16)

            @pl.when((origin != z) & jnp.logical_not(has_inflow(origin)))
            def _():
                line_copy(origin, j).start()

    def drain(k):
        origin = looked_up(orders, z, k)
        for t in range(2):
            for up_way in (False, True):
                sent = forwards(origin, up_way)
                if t == 1 and extent > 3:
                    sent = sent & jnp.logical_not((origin == z) & late(up_way))

                @pl.when(sent)
                def _():
                    tok_copy(t, origin, up_way).wait_send()

            @pl.loop(1, plane)
            def _(i):
                row_copy(t, origin, plane_peer(i)).wait_send()

            swap_copy(t, origin).wait_send()
        part_copy(origin).wait_send()

    def drain_returns():
        for i in range(1, extent):
            meta_copy(line_peer(i), z).wait_send()
        if extent > 3:
            for up_way in (False, True):

                @pl.when(late(up_way))
                def _():
                    tok_copy(1, z, up_way).wait_send()

        @pl.loop(0, extent)
        def _(origin):
            @pl.loop(1, plane)
            def _(i):
                ret_copy(origin, plane_peer(i)).wait_send()

            @pl.when(origin != z)
            def _():
                for j in range(columns):
                    line_copy(origin, j).wait_send()

        @pl.loop(1, plane)
        def _(i):
            for k in range(extent):
                active_copy(plane_peer(i), p, k).wait_send()

    def relay_band(k, jj):
        home = looked_up(relays, z, k)

        @pl.when(has_inflow(home))
        def _():
            j = band_for(home, jj)
            line_arrival(home, j).wait_recv()
            line_sent[home, :, band(j)] = (
                line_sent[home, :, band(j)].astype(jnp.float32)
                + line_got[home, :, band(j)].astype(jnp.float32)
            ).astype(jnp.bfloat16)
            line_copy(home, j).start()

    for load in loads[:2]:
        load.wait()
    for i in range(1, extent):
        meta_copy(line_peer(i), z).start()

    local = values.shape[1]
    strip = min(256, local)
    strips = local // strip
    row_count = values.shape[0]

    def strip_at(n):
        return pl.ds(pl.multiple_of(n * strip, strip), strip)

    def stat_copy(i):
        return remote(
            stats.at[i, 0], stats.at[i, 1], stat_sems.at[0, i], stat_sems.at[1, i], sp, other
        )

    def paired(i, first, second):
        lane = lax.broadcasted_iota(jnp.int32, (row_count, stats.shape[3]), 1)
        stats[i, 0] = jnp.where(lane == 0, first, second)
        stat_copy(i).start()

    def both_sums(i):
        stat_copy(i).wait_recv()
        merged = (stats[i, 0] + stats[i, 1]) / width
        return merged[:, 0:1], merged[:, 1:2]

    share = row_count // extent

    def active_copy(q, owner, i):
        part = active.at[owner, pl.ds(i * share, share)]
        return remote(
            part, part, active_send.at[q, i], active_recv.at[owner, i], z * plane + q, tp
        )

    def prepare():
        loads[5].wait()
        sums = jnp.zeros((row_count, 1), jnp.float32)
        squares = jnp.zeros((row_count, 1), jnp.float32)
        for n in range(strips):
            block = values[:, n * strip : (n + 1) * strip].astype(jnp.float32)
            sums = sums + jnp.sum(block, axis=1, keepdims=True)
            squares = squares + jnp.sum(block * block, axis=1, keepdims=True)
        paired(0, sums, squares)
        average, second = both_sums(0)
        scale = lax.rsqrt(second - average * average + NORM_EPS)
        inverse[...] = jnp.broadcast_to(scale, inverse.shape)
        for n in range(strips):
            cut = slice(n * strip, (n + 1) * strip)
            flat = (values[:, cut].astype(jnp.float32) - average) * scale
            normed[:, cut] = flat
            scaled = flat * gain[:, cut]
            active[p, :, cut] = (scaled * jax.nn.sigmoid(scaled)).astype(jnp.bfloat16)

    def share_active(k):
        @pl.loop(1, plane)
        def _(i):
            active_copy(plane_peer(i), p, k).start()

    send_own(0)
    send_own(1)
    arrive(0, z)
    arrive(1, z)
    prepare()

    @pl.loop(0, extent)
    def _(k):
        @pl.when(k > 0)
        def _():
            forward(1, k)

        swap(0, k)
        first_products(k)

        @pl.when(k == 0)
        def _():
            forward(0, 1)

        @pl.when(k < extent - 1)
        def _():
            event(2 * k)

        @pl.when((k > 0) & (k < extent - 1))
        def _():
            forward(0, k + 1)

        @pl.when((k > 0) & (k < extent - 1))
        def _():
            combine(k - 1)

        @pl.when(k > 0)
        def _():
            drain(k - 1)

        swap(1, k)
        share_active(k)
        products(k)

        @pl.when(k < extent - 1)
        def _():
            event(2 * k + 1)

        @pl.when(k == extent - 1)
        def _():
            combine(k - 1)

        send_back(k)

    @pl.loop(0, columns)
    def _(jj):
        relay_band(0, jj)

    drain(extent - 1)
    combine(extent - 1)

    @pl.loop(0, columns)
    def _(jj):
        relay_band(1, jj)
        gate_up_share(0, jj)

    grad_store(0).start()

    @pl.loop(0, columns)
    def _(jj):
        for k in range(2, extent - 1):
            relay_band(k, jj)
        gate_up_share(1, jj)

    grad_store(1).start()

    own_block = width // (extent * plane)
    lanes = blocks.shape[4]

    def block_at(j, q):
        start = (j * plane + q) * own_block
        return pl.ds(pl.multiple_of(start // lanes * lanes, lanes), lanes)

    def token_copy(j):
        return remote(
            tokens.at[tp, :, band(j)],
            tokens.at[tp, :, band(j)],
            token_sems.at[0, j],
            token_sems.at[1, j],
            sp,
            other,
        )

    def token_arrival(j):
        return remote(
            tokens.at[other, :, band(j)],
            tokens.at[other, :, band(j)],
            token_sems.at[0, j],
            token_sems.at[1, j],
            sp,
            other,
        )

    def block_copy(j, q):
        return remote(
            tokens.at[tp, :, block_at(j, q)],
            blocks.at[j, tp, p],
            block_send.at[j, q],
            block_recv.at[j, p],
            z * plane + q,
            tp,
        )

    def block_arrival(j, q):
        return remote(
            tokens.at[tp, :, block_at(j, q)],
            blocks.at[j, tp, q],
            block_send.at[j, q],
            block_recv.at[j, q],
            z * plane + q,
            tp,
        )

    def block_swap(j):
        return remote(
            blocks.at[j, tp],
            blocks.at[j, tp],
            block_swaps.at[0, j],
            block_swaps.at[1, j],
            sp,
            other,
        )

    def block_swap_arrival(j):
        return remote(
            blocks.at[j, other],
            blocks.at[j, other],
            block_swaps.at[0, j],
            block_swaps.at[1, j],
            sp,
            other,
        )

    def home_band(jj):
        j = band_for(z, jj)
        for slot, there in ((z, z > 0), (extent, z < extent - 1)):

            @pl.when(there)
            def _():
                line_arrival(slot, j).wait_recv()
                total[:, band(j)] = total[:, band(j)] + line_got[slot, :, band(j)].astype(
                    jnp.float32
                )

        tokens[tp, :, band(j)] = (
            tok[1, z, :, band(j)].astype(jnp.float32) + total[:, band(j)]
        ).astype(jnp.bfloat16)
        token_copy(j).start()

        @pl.loop(1, plane)
        def _(i):
            block_copy(j, plane_peer(i)).start()

        blocks[j, tp, p] = tokens[tp, :, block_at(j, p)]

    def swap_block(jj):
        j = band_for(z, jj)

        @pl.loop(1, plane)
        def _(i):
            block_arrival(j, plane_peer(i)).wait_recv()

        block_swap(j).start()

    pieces = 2
    piece = local // pieces

    def piece_at(h):
        return pl.ds(h * piece, piece)

    def sums_copy(j, h):
        to_z = jnp.where(j > z, z + 1, z - 1)
        slot = jnp.where((j < z) & (to_z == j), extent, j)
        return remote(
            sums_sent.at[j, :, piece_at(h)],
            sums_got.at[slot, :, piece_at(h)],
            sums_send.at[j, h],
            sums_recv.at[slot, h],
            to_z * plane + p,
            tp,
        )

    def sums_arrival(slot, h):
        return remote(
            sums_sent.at[0, :, piece_at(h)],
            sums_got.at[slot, :, piece_at(h)],
            sums_send.at[0, h],
            sums_recv.at[slot, h],
            sp,
            other,
        )

    def act_grads():
        loads[6].wait()
        for j in range(columns):
            token_arrival(j).wait_recv()
        grad_sum = jnp.zeros((row_count, 1), jnp.float32)
        grad_corr = jnp.zeros((row_count, 1), jnp.float32)
        for n in range(strips):
            cut = slice(n * strip, (n + 1) * strip)
            act_grad = lax.dot_general(
                tokens[...].reshape(row_count, width),
                out_weight[cut, :],
                (((1,), (1,)), ((), ())),
                preferred_element_type=jnp.float32,
            )
            flat = normed[:, cut]
            weight = gain[:, cut]
            scaled = flat * weight
            logistic = jax.nn.sigmoid(scaled)
            slope = act_grad * (logistic * (1.0 + scaled * (1.0 - logistic))) * weight
            spread[:row_count, cut] = slope
            grad_sum = grad_sum + jnp.sum(slope, axis=1, keepdims=True)
            grad_corr = grad_corr + jnp.sum(slope * flat, axis=1, keepdims=True)
        paired(1, grad_sum, grad_corr)

    def partial_block(jj):
        j = band_for(z, jj)
        block_swap_arrival(j).wait_recv()
        at = lax.rem((j * plane + p) * own_block, lanes)
        for n in range(strips):
            cut = slice(n * strip, (n + 1) * strip)
            mine = sum(
                lax.dot_general(
                    blocks[j, side].reshape(plane * token_count, lanes),
                    active[:, side * token_count : (side + 1) * token_count, cut].reshape(
                        plane * token_count, strip
                    ),
                    (((0,), (0,)), ((), ())),
                    preferred_element_type=jnp.float32,
                )
                for side in range(2)
            )
            if own_block != lanes:
                mine = sum(
                    jnp.where(at == start, mine[start : start + own_block], 0.0)
                    for start in range(0, lanes, own_block)
                )

            @pl.when(j == z)
            def _():
                sums_own[:, cut] = mine

            @pl.when(j != z)
            def _():
                sums_sent[j, :, cut] = mine.astype(jnp.bfloat16)

        @pl.when((j != z) & jnp.logical_not(has_inflow(j)))
        def _():
            for h in range(pieces):
                sums_copy(j, h).start()

    @pl.loop(1, plane)
    def _(i):
        for k in range(extent):
            active_copy(plane_peer(i), plane_peer(i), k).wait_recv()

    @pl.loop(0, extent)
    def _(jj):
        home_band(jj)

        @pl.when(jj > 0)
        def _():
            swap_block(jj - 1)

        @pl.when(jj > 1)
        def _():
            partial_block(jj - 2)

    act_grads()
    swap_block(extent - 1)
    mean, corr = both_sums(1)
    edge = (padded.shape[0] - row_count) // 2
    scale = inverse[:, 0:1]
    for n in range(strips):
        cut = slice(n * strip, (n + 1) * strip)
        padded[edge : edge + row_count, cut] = (
            scale * (spread[:row_count, cut] - mean - normed[:, cut] * corr)
        ).astype(jnp.bfloat16)

    def halo_copy(up_way):
        if up_way:
            src, dst, to = row_count, 0, sp + 1
        else:
            src, dst, to = edge, edge + row_count, sp - 1
        return remote(
            padded.at[pl.ds(src, edge), :],
            padded.at[pl.ds(dst, edge), :],
            halo_sems.at[0, int(up_way)],
            halo_sems.at[1, int(up_way)],
            to,
            tp,
        )

    inside = {True: sp < last_sp, False: sp > 0}
    for up_way in (True, False):

        @pl.when(inside[up_way])
        def _():
            halo_copy(up_way).start()

    def relay(k):
        j = looked_up(sum_relays(extent), z, k)

        @pl.when(has_inflow(j))
        def _():
            for h in range(pieces):
                sums_arrival(j, h).wait_recv()
                sums_sent[j, :, piece_at(h)] = (
                    sums_sent[j, :, piece_at(h)].astype(jnp.float32)
                    + sums_got[j, :, piece_at(h)].astype(jnp.float32)
                ).astype(jnp.bfloat16)
                sums_copy(j, h).start()

    @pl.loop(max(0, extent - 2), extent)
    def _(jj):
        partial_block(jj)

    relay(0)
    tap_count = taps.shape[0]
    reach = tap_count // 2
    narrow = min(128, local)
    extra = (edge + reach) // 8 * 8

    def convolve(first, count):
        @pl.loop(0, local // narrow)
        def _(n):
            cut = pl.ds(pl.multiple_of(n * narrow, narrow), narrow)
            acc = jnp.zeros((count, narrow), jnp.float32)
            for s in range(8):
                taps_at = [o for o in range(tap_count) if (edge + reach - o) % 8 == s]
                if not taps_at:
                    continue
                shifted = spread[first + s : first + s + extra + count, cut]
                for o in taps_at:
                    m = (edge + reach - o) // 8 * 8
                    acc = acc + taps[o : o + 1, cut] * shifted[m : m + count]
            values[first : first + count, cut] = acc.astype(jnp.bfloat16)

    inner = slice(edge, edge + row_count)
    spread[inner] = padded[inner].astype(jnp.float32)
    if row_count > 2 * edge:
        convolve(edge, row_count - 2 * edge)
    for k in range(1, extent - 1):
        relay(k)
    grad_tiles(2, 0, half // min(256, half), min(256, half))
    grad_store(2).start()
    for up_way in (True, False):
        at = 0 if up_way else edge + row_count

        @pl.when(inside[not up_way])
        def _():
            halo_copy(up_way).wait_recv()
            spread[at : at + edge, :] = padded[at : at + edge, :].astype(jnp.float32)

        @pl.when(jnp.logical_not(inside[not up_way]))
        def _():
            spread[at : at + edge, :] = jnp.zeros((edge, local), jnp.float32)

    convolve(0, edge)
    convolve(row_count - edge, edge)
    finish = pltpu.make_async_copy(values, input_out, load_sem.at[0])
    finish.start()
    drain_returns()
    for h in range(pieces):
        for slot, there in ((z, z > 0), (extent, z < extent - 1)):

            @pl.when(there)
            def _():
                sums_arrival(slot, h).wait_recv()
                sums_own[:, piece_at(h)] = sums_own[:, piece_at(h)] + sums_got[
                    slot, :, piece_at(h)
                ].astype(jnp.float32)

    store = pltpu.make_async_copy(sums_own, proj_out, load_sem.at[1])
    store.start()
    for i in range(2):
        stat_copy(i).wait_send()
    for up_way in (True, False):

        @pl.when(inside[up_way])
        def _():
            halo_copy(up_way).wait_send()

    for j in range(columns):
        token_copy(j).wait_send()

        @pl.loop(1, plane)
        def _(i):
            block_copy(j, plane_peer(i)).wait_send()

        block_swap(j).wait_send()

        @pl.when(z != j)
        def _():
            for h in range(pieces):
                sums_copy(j, h).wait_send()

    finish.wait()
    store.wait()
    for which in range(3):
        grad_store(which).wait()


TOPK_ROWS = 2


def routed_backward(
    mid_rows,
    cotangent,
    routes,
    route_weight,
    gate_mat,
    up_mat,
    down_mat,
    filtered,
    out_weight,
    taps,
    gain,
    capacity,
):
    sp_count = lax.axis_size("sp")
    extent = line_extent(sp_count)
    plane = sp_count // extent
    token_count, width = mid_rows.shape
    half = gate_mat.shape[1]
    slots = plane * capacity
    kind = jnp.bfloat16
    any_space = pl.BlockSpec(memory_space=pl.ANY)
    vmem = pl.BlockSpec(memory_space=pltpu.VMEM)
    dma = pltpu.SemaphoreType.DMA
    columns = extent
    row_count, local = filtered.shape
    own_block = width // sp_count
    lanes = min(max(own_block, 128), width // extent)
    edge = -(-(taps.shape[0] // 2) // 16) * 16
    rows_shape = (extent, 2, plane, capacity, width)
    small_shape = (extent, 2 * slots, half)
    scratch = [
        pltpu.VMEM((2, extent, token_count, width), kind),
        pltpu.VMEM((8, token_count), jnp.float32),
        pltpu.VMEM((extent, 8, token_count), jnp.float32),
        pltpu.VMEM((2, extent, plane, capacity, width), kind),
        pltpu.VMEM((2,) + rows_shape, kind),
        pltpu.VMEM(gate_mat.shape, kind),
        pltpu.VMEM(up_mat.shape, kind),
        pltpu.VMEM(down_mat.shape, kind),
        pltpu.VMEM((2 * slots, half), jnp.float32),
        pltpu.VMEM((2 * slots, half), jnp.float32),
        pltpu.VMEM(small_shape, kind),
        pltpu.VMEM(small_shape, kind),
        pltpu.VMEM(small_shape, kind),
        pltpu.VMEM((extent, plane, capacity, width), kind),
        pltpu.VMEM((extent, plane, capacity, width), kind),
        pltpu.VMEM((extent, plane, capacity, width), kind),
        pltpu.VMEM((extent, plane, capacity, width), kind),
        pltpu.VMEM((extent, token_count, width), kind),
        pltpu.VMEM((extent + 1, token_count, width), kind),
        pltpu.VMEM((token_count, width), jnp.float32),
        pltpu.VMEM((2, token_count, width), kind),
        dma((7,)),
        dma((2, extent)),
        dma((2, extent, 2)),
        dma((2, extent)),
        dma((2, extent, plane)),
        dma((2, extent, plane)),
        dma((2, extent)),
        dma((2, extent)),
        dma((2, extent)),
        dma((extent, plane)),
        dma((extent, plane)),
        dma((extent, columns)),
        dma((extent + 1, columns)),
        dma((3,)),
        dma((2, columns)),
        pltpu.VMEM((row_count, local), kind),
        pltpu.VMEM(out_weight.shape, kind),
        pltpu.VMEM((2, 2, row_count, 128), jnp.float32),
        pltpu.VMEM((row_count, local), jnp.float32),
        pltpu.VMEM((row_count, 128), jnp.float32),
        pltpu.VMEM((plane, row_count, local), kind),
        pltpu.VMEM((extent, 2, plane, token_count, lanes), kind),
        pltpu.VMEM((extent, own_block, local), kind),
        pltpu.VMEM((extent + 1, own_block, local), kind),
        pltpu.VMEM((own_block, local), jnp.float32),
        pltpu.VMEM((row_count + 2 * edge, local), kind),
        pltpu.VMEM((row_count + 2 * edge, local), jnp.float32),
        dma((2, 2)),
        dma((plane, extent)),
        dma((plane, extent)),
        dma((extent, plane)),
        dma((extent, plane)),
        dma((2, extent)),
        dma((extent, 2)),
        dma((extent + 1, 2)),
        dma((2, 2)),
    ]
    held = sum(
        math.prod(s.shape) * jnp.dtype(s.dtype).itemsize
        for s in scratch
        if s.memory_space == pltpu.VMEM
    )
    out = pl.pallas_call(
        functools.partial(routed_kernel, extent, plane, capacity),
        out_shape=[
            jax.ShapeDtypeStruct((own_block, local), jnp.float32),
            jax.ShapeDtypeStruct((row_count, local), kind),
            jax.ShapeDtypeStruct(gate_mat.shape, kind),
            jax.ShapeDtypeStruct(up_mat.shape, kind),
            jax.ShapeDtypeStruct(down_mat.shape, kind),
        ],
        in_specs=[any_space] * 2 + [vmem] * 2 + [any_space] * 5 + [vmem] * 2,
        out_specs=[any_space] * 5,
        scratch_shapes=scratch,
        compiler_params=pltpu.CompilerParams(
            collective_id=0, has_side_effects=True, vmem_limit_bytes=min(held + SPARE, 67_043_328)
        ),
    )(
        mid_rows,
        cotangent,
        routes,
        route_weight,
        gate_mat,
        up_mat,
        down_mat,
        filtered,
        out_weight,
        taps,
        gain,
    )
    return out


def per_device(
    mid_rows,
    cotangent,
    routes,
    route_weight,
    filtered,
    conv_taps,
    norm_gain,
    out_weight,
    gate_weight,
    up_weight,
    down_weight,
):
    sp_count = lax.axis_size("sp")
    token_count, model_width = mid_rows.shape
    per_token = routes.shape[1]
    local_experts = gate_weight.shape[0]
    experts = local_experts * sp_count
    capacity = 2 * token_count * per_token // sp_count
    proj_grad, input_grad, *weight_grads = routed_backward(
        mid_rows,
        cotangent,
        routes.T,
        route_weight.T,
        gate_weight[0],
        up_weight[0],
        down_weight[0],
        filtered,
        out_weight,
        conv_taps,
        norm_gain[None],
        capacity,
    )
    gate_grad, up_grad, down_grad = (grad.astype(jnp.float32)[None] for grad in weight_grads)
    return (gate_grad, up_grad, down_grad, proj_grad, input_grad)


def solution(mesh):
    in_specs = (
        P(("sp", "tp"), None),
        P(("sp", "tp"), None),
        P(("sp", "tp"), None),
        P(("sp", "tp"), None),
        P("sp", "tp"),
        P(None, "tp"),
        P("tp"),
        P("tp", None),
        P("sp", None, "tp"),
        P("sp", None, "tp"),
        P("sp", "tp", None),
    )
    out_specs = (
        P("sp", None, "tp"),
        P("sp", None, "tp"),
        P("sp", "tp", None),
        P("sp", "tp"),
        P("sp", "tp"),
    )
    return jax.shard_map(
        per_device, mesh=mesh, in_specs=in_specs, out_specs=out_specs, check_vma=False
    )
```

```python
import functools
import math

import jax
import jax.numpy as jnp
from jax import lax
from jax.experimental import pallas as pl
from jax.experimental.pallas import tpu as pltpu
from jax.sharding import PartitionSpec as P

MESH = pl.DeviceIdType.MESH
NORM_EPS = 1e-05
SPARE = 4 << 20


def line_extent(count):
    bits = count.bit_length() - 1
    return 1 << -(-bits // 3)


def chunk_orders(extent):
    orders = []
    for own in range(extent):
        toward = [i for i in range(own + 1, extent)] if 2 * own < extent - 1 else [i for i in range(own - 1, -1, -1)]
        back = [i for i in range(extent) if i != own and i not in toward]
        back.sort(key=lambda i: abs(i - own))
        if own in (0, extent - 1):
            order = toward[1:] + toward[:1]
        else:
            order = toward[:1] + back + toward[1:]
        orders.append([own] + order)
    return orders


def pick_events(extent):
    table = []
    for own, order in enumerate(chunk_orders(extent)):
        rest = order[1:]
        if own in (0, extent - 1):
            near, far = rest[-1], rest[:-1]
            events = [(0, near)] + [(t, i) for i in far for t in range(2)] + [(1, near)]
        else:
            near = [i for i in rest if abs(i - own) == 1]
            far = [i for i in rest if abs(i - own) > 1]
            events = [(t, i) for t in range(2) for i in near]
            events = events + [(t, i) for i in far for t in range(2)]
        table.append(events)
    return table


def relay_orders(extent):
    return [
        sorted(
            (i for i in range(extent) if i != own),
            key=lambda i: (own if i > own else extent - 1 - own, abs(i - own)),
        )
        for own in range(extent)
    ]


def sum_orders(extent):
    return [
        sorted((i for i in range(extent) if i != own), key=lambda i: -abs(i - own)) + [own]
        for own in range(extent)
    ]


def sum_relays(extent):
    return [
        sorted(
            (i for i in range(extent) if i != own),
            key=lambda i: (own if i > own else extent - 1 - own, -abs(i - own)),
        )
        for own in range(extent)
    ]


def looked_up(table, row, column):
    value = jnp.int32(0)
    for i, entries in enumerate(table):
        for k, entry in enumerate(entries):
            value = value + jnp.where((row == i) & (column == k), entry, 0)
    return value


def routed_kernel(
    extent,
    plane,
    capacity,
    mid_hbm,
    cot_hbm,
    routes,
    route_weight,
    gate_hbm,
    up_hbm,
    down_hbm,
    filtered_hbm,
    out_weight_hbm,
    taps,
    gain,
    proj_out,
    input_out,
    gate_out,
    up_out,
    down_out,
    tok,
    meta,
    metas,
    picks,
    rows,
    gate,
    up,
    down,
    pre_gate,
    pre_up,
    hidden,
    gate_pre,
    up_pre,
    part_sent,
    part_got,
    ret_sent,
    ret_got,
    line_sent,
    line_got,
    total,
    tokens,
    load_sem,
    meta_sems,
    tok_send,
    tok_recv,
    row_send,
    row_recv,
    swap_send,
    swap_recv,
    part_sems,
    ret_send,
    ret_recv,
    line_send,
    line_recv,
    out_sems,
    token_sems,
    values,
    out_weight,
    stats,
    normed,
    inverse,
    active,
    blocks,
    sums_sent,
    sums_got,
    sums_own,
    padded,
    spread,
    stat_sems,
    active_send,
    active_recv,
    block_send,
    block_recv,
    block_swaps,
    sums_send,
    sums_recv,
    halo_sems,
):
    sp, tp = lax.axis_index("sp"), lax.axis_index("tp")
    z, p = sp // plane, sp % plane
    slots = plane * capacity
    token_count, width = tok.shape[2], tok.shape[3]
    other = 1 - tp
    step = width // extent
    columns = extent
    orders, relays = chunk_orders(extent), relay_orders(extent)

    def remote(src, dst, send, recv, to_sp, to_tp):
        return pltpu.make_async_remote_copy(
            src_ref=src,
            dst_ref=dst,
            send_sem=send,
            recv_sem=recv,
            device_id=(to_sp, to_tp),
            device_id_type=MESH,
        )

    loads = [
        pltpu.make_async_copy(mid_hbm, tok.at[0, z], load_sem.at[0]),
        pltpu.make_async_copy(cot_hbm, tok.at[1, z], load_sem.at[1]),
        pltpu.make_async_copy(gate_hbm, gate, load_sem.at[2]),
        pltpu.make_async_copy(up_hbm, up, load_sem.at[3]),
        pltpu.make_async_copy(down_hbm, down, load_sem.at[4]),
        pltpu.make_async_copy(filtered_hbm, values, load_sem.at[5]),
        pltpu.make_async_copy(out_weight_hbm, out_weight, load_sem.at[6]),
    ]
    for load in loads:
        load.start()
    experts = extent * plane
    chosen = [
        lax.broadcasted_iota(jnp.int32, (experts, token_count), 0) == routes[k : k + 1, :]
        for k in range(TOPK_ROWS)
    ]
    taken = jnp.where(chosen[0] | chosen[1], 1.0, 0.0).astype(jnp.bfloat16)
    square = (token_count, token_count)
    before = lax.broadcasted_iota(jnp.int32, square, 0) < lax.broadcasted_iota(jnp.int32, square, 1)
    earlier = jnp.dot(
        taken,
        jnp.where(before, 1.0, 0.0).astype(jnp.bfloat16),
        preferred_element_type=jnp.float32,
    )
    for k in range(TOPK_ROWS):
        place = jnp.sum(jnp.where(chosen[k], earlier, 0.0), axis=0, keepdims=True)
        meta[k : k + 1, :] = place + (routes[k : k + 1, :] * capacity).astype(jnp.float32)
        meta[TOPK_ROWS + k : TOPK_ROWS + k + 1, :] = route_weight[k : k + 1, :]
    meta[2 * TOPK_ROWS :, :] = jnp.zeros((8 - 2 * TOPK_ROWS, token_count), jnp.float32)
    metas[z] = meta[...]

    barrier = pltpu.get_barrier_semaphore()

    def greet(to_sp, to_tp):
        pl.semaphore_signal(barrier, inc=1, device_id=(to_sp, to_tp), device_id_type=MESH)

    def line_peer(i):
        return lax.rem(z + i, extent)

    def plane_peer(i):
        return lax.rem(p + i, plane)

    for i in range(1, extent):
        greet(line_peer(i) * plane + p, tp)

    @pl.loop(1, plane)
    def _(i):
        greet(z * plane + plane_peer(i), tp)

    greet(sp, other)
    last_sp = extent * plane - 1

    @pl.when(sp > 0)
    def _():
        greet(sp - 1, tp)

    @pl.when(sp < last_sp)
    def _():
        greet(sp + 1, tp)

    ends = jnp.where(sp > 0, 1, 0) + jnp.where(sp < last_sp, 1, 0)
    pl.semaphore_wait(barrier, extent - 1 + plane - 1 + 1 + ends)

    def meta_copy(to_z, from_z):
        return remote(
            meta, metas.at[from_z], meta_sems.at[0, to_z], meta_sems.at[1, from_z], to_z * plane + p, tp
        )

    def tok_copy(t, origin, up_way):
        to_z = z + 1 if up_way else z - 1
        return remote(
            tok.at[t, origin],
            tok.at[t, origin],
            tok_send.at[t, origin, int(up_way)],
            tok_recv.at[t, origin],
            to_z * plane + p,
            tp,
        )

    def forwards(origin, up_way):
        if up_way:
            return (origin <= z) & (z < extent - 1)
        return (origin >= z) & (z > 0)

    def row_copy(t, origin, q):
        return remote(
            picks.at[t, origin, q],
            rows.at[t, origin, 0, p],
            row_send.at[t, origin, q],
            row_recv.at[t, origin, p],
            z * plane + q,
            tp,
        )

    def row_arrival(t, origin, q):
        return remote(
            picks.at[t, origin, q],
            rows.at[t, origin, 0, q],
            row_send.at[t, origin, q],
            row_recv.at[t, origin, q],
            z * plane + q,
            tp,
        )

    def swap_copy(t, origin):
        return remote(
            rows.at[t, origin, 0],
            rows.at[t, origin, 1],
            swap_send.at[t, origin],
            swap_recv.at[t, origin],
            sp,
            other,
        )

    def part_copy(origin):
        return remote(
            part_sent.at[origin],
            part_got.at[origin],
            part_sems.at[0, origin],
            part_sems.at[1, origin],
            sp,
            other,
        )

    def ret_copy(origin, q):
        return remote(
            ret_sent.at[origin, q],
            ret_got.at[origin, p],
            ret_send.at[origin, q],
            ret_recv.at[origin, p],
            z * plane + q,
            tp,
        )

    def ret_arrival(origin, q):
        return remote(
            ret_sent.at[origin, q],
            ret_got.at[origin, q],
            ret_send.at[origin, q],
            ret_recv.at[origin, q],
            z * plane + q,
            tp,
        )

    def band(j):
        return pl.ds(pl.multiple_of(j * step, step), step)

    def band_for(home, jj):
        return looked_up(sum_orders(extent), home, jj)

    def line_copy(home, j):
        to_z = jnp.where(home > z, z + 1, z - 1)
        slot = jnp.where((home < z) & (to_z == home), extent, home)
        return remote(
            line_sent.at[home, :, band(j)],
            line_got.at[slot, :, band(j)],
            line_send.at[home, j],
            line_recv.at[slot, j],
            to_z * plane + p,
            tp,
        )

    def line_arrival(slot, j):
        return remote(
            line_sent.at[0, :, band(j)],
            line_got.at[slot, :, band(j)],
            line_send.at[0, j],
            line_recv.at[slot, j],
            z * plane + p,
            other,
        )

    def has_inflow(home):
        return ((home > z) & (z > 0)) | ((home < z) & (z < extent - 1))

    def hits(origin):
        slot = lax.broadcasted_iota(jnp.int32, (slots, token_count), 0) + z * slots
        slot = slot.astype(jnp.float32)
        return [slot == metas[origin, pl.ds(k, 1), :] for k in range(TOPK_ROWS)]

    def chooser(origin):
        first, second = hits(origin)
        return jnp.where(first | second, 1.0, 0.0).astype(jnp.bfloat16)

    def scale_of(origin):
        first, second = hits(origin)
        weighted = jnp.where(first, metas[origin, pl.ds(TOPK_ROWS, 1), :], 0.0) + jnp.where(
            second, metas[origin, pl.ds(TOPK_ROWS + 1, 1), :], 0.0
        )
        return jnp.sum(weighted, axis=1, keepdims=True)

    def late(up_way):
        return (z == extent - 2) if up_way else (z == 1)

    def send_own(t):
        for up_way in (False, True):
            whole = forwards(z, up_way)
            if t == 1 and extent > 3:
                whole = whole & jnp.logical_not(late(up_way))

            @pl.when(whole)
            def _():
                tok_copy(t, z, up_way).start()

    def forward(t, distance):
        below = lax.rem(z - distance + extent, extent)
        above = lax.rem(z + distance, extent)
        for origin, up_way, there in (
            (above, False, (z + distance < extent) & (z > 0)),
            (below, True, (z >= distance) & (z < extent - 1)),
        ):

            @pl.when(there)
            def _():
                tok_copy(t, origin, up_way).wait_recv()
                tok_copy(t, origin, up_way).start()

        if t == 1 and extent > 3:
            for up_way in (False, True):

                @pl.when((distance == extent - 2) & late(up_way))
                def _():
                    tok_copy(1, z, up_way).start()

    def arrive(t, origin):
        @pl.when((origin != z) & jnp.logical_not(has_inflow(origin)))
        def _():
            tok_copy(t, origin, True).wait_recv()

        @pl.when((origin != z) & (t == 0))
        def _():
            meta_copy(origin, origin).wait_recv()

        select = chooser(origin)
        scale = jnp.where(t == 1, scale_of(origin), 1.0)
        for j in range(columns):
            picked = scale * jnp.dot(
                select, tok[t, origin, :, band(j)], preferred_element_type=jnp.float32
            )
            picks[t, origin, :, :, band(j)] = picked.astype(jnp.bfloat16).reshape(
                plane, capacity, step
            )

        @pl.loop(1, plane)
        def _(i):
            row_copy(t, origin, plane_peer(i)).start()

        rows[t, origin, 0, p] = picks[t, origin, p]

    def event(i):
        kinds = [[t for t, _ in row] for row in pick_events(extent)]
        origins = [[origin for _, origin in row] for row in pick_events(extent)]
        arrive(looked_up(kinds, z, i), looked_up(origins, z, i))

    def swap(t, k):
        origin = looked_up(orders, z, k)

        @pl.loop(1, plane)
        def _(i):
            row_arrival(t, origin, plane_peer(i)).wait_recv()

        swap_copy(t, origin).start()

    def expert_rows(t, origin):
        return rows[t, origin].reshape(2 * slots, width)

    half = gate.shape[1]
    tile = min(256, half)

    def first_products(k):
        origin = looked_up(orders, z, k)

        @pl.when(k == 0)
        def _():
            loads[2].wait()
            loads[3].wait()

        swap_copy(0, origin).wait_recv()

        @pl.loop(0, half // tile)
        def _(n):
            cut = pl.ds(pl.multiple_of(n * tile, tile), tile)
            block = expert_rows(0, origin)
            pre_gate[:, cut] = jnp.dot(block, gate[:, cut], preferred_element_type=jnp.float32)
            pre_up[:, cut] = jnp.dot(block, up[:, cut], preferred_element_type=jnp.float32)

    def products(k):
        origin = looked_up(orders, z, k)

        @pl.when(k == 0)
        def _():
            loads[4].wait()

        swap_copy(1, origin).wait_recv()

        @pl.loop(0, half // tile)
        def _(n):
            cut = pl.ds(pl.multiple_of(n * tile, tile), tile)
            hidden_grad = lax.dot_general(
                expert_rows(1, origin),
                down[cut, :],
                (((1,), (1,)), ((), ())),
                preferred_element_type=jnp.float32,
            )
            g, u = pre_gate[:, cut], pre_up[:, cut]
            logistic = jax.nn.sigmoid(g)
            gate_act = g * logistic
            hidden[origin, :, cut] = (gate_act * u).astype(jnp.bfloat16)
            gate_pre[origin, :, cut] = (
                hidden_grad * u * (logistic * (1.0 + g * (1.0 - logistic)))
            ).astype(jnp.bfloat16)
            up_pre[origin, :, cut] = (hidden_grad * gate_act).astype(jnp.bfloat16)

        wide = min(256, width)

        @pl.loop(0, width // wide)
        def _(n):
            cut = pl.ds(pl.multiple_of(n * wide, wide), wide)
            part = lax.dot_general(
                gate_pre[origin],
                gate[cut, :],
                (((1,), (1,)), ((), ())),
                preferred_element_type=jnp.float32,
            ) + lax.dot_general(
                up_pre[origin],
                up[cut, :],
                (((1,), (1,)), ((), ())),
                preferred_element_type=jnp.float32,
            )
            part = part.astype(jnp.bfloat16).reshape(2, plane, capacity, wide)
            ret_sent[origin, :, :, cut] = part[0]
            part_sent[origin, :, :, cut] = part[1]

        part_copy(origin).start()

    def all_rows(t, cut):
        return rows[t, :, :, :, :, cut].reshape(extent * 2 * slots, -1)

    def small_rows(ref, cut):
        return ref[:, :, cut].reshape(extent * 2 * slots, -1)

    def grad_store(which):
        return pltpu.make_async_copy(
            (gate, up, down)[which], (gate_out, up_out, down_out)[which], out_sems.at[which]
        )

    def grad_tiles(which, first, count, size):
        @pl.loop(first, first + count)
        def _(n):
            cut = pl.ds(pl.multiple_of(n * size, size), size)
            if which < 2:
                left = all_rows(0, cut)
                right = small_rows((gate_pre, up_pre)[which], slice(None))
            else:
                left = small_rows(hidden, cut)
                right = all_rows(1, slice(None))
            (gate, up, down)[which][cut, :] = lax.dot_general(
                left, right, (((0,), (0,)), ((), ())), preferred_element_type=jnp.float32
            ).astype(jnp.bfloat16)

    def gate_up_share(which, jj):
        size = min(256, width // columns)
        each = width // columns // size
        grad_tiles(which, jj * each, each, size)

    def send_back(k):
        origin = looked_up(orders, z, k)
        part_copy(origin).wait_recv()
        for j in range(columns):
            both = ret_sent[origin, :, :, band(j)].astype(jnp.float32) + part_got[
                origin, :, :, band(j)
            ].astype(jnp.float32)
            ret_sent[origin, :, :, band(j)] = both.astype(jnp.bfloat16)

        @pl.loop(1, plane)
        def _(i):
            ret_copy(origin, plane_peer(i)).start()

        ret_got[origin, p] = ret_sent[origin, p]

    def combine(k):
        origin = looked_up(orders, z, k)

        @pl.loop(1, plane)
        def _(i):
            ret_arrival(origin, plane_peer(i)).wait_recv()

        select = chooser(origin)
        for jj in range(columns):
            j = band_for(origin, jj)
            back = ret_got[origin, :, :, band(j)].reshape(slots, step)
            added = lax.dot_general(
                select, back, (((0,), (0,)), ((), ())), preferred_element_type=jnp.float32
            )

            @pl.when(origin == z)
            def _():
                total[:, band(j)] = added

            @pl.when(origin != z)
            def _():
                line_sent[origin, :, band(j)] = added.astype(jnp.bfloat16)

            @pl.when((origin != z) & jnp.logical_not(has_inflow(origin)))
            def _():
                line_copy(origin, j).start()

    def drain(k):
        origin = looked_up(orders, z, k)
        for t in range(2):
            for up_way in (False, True):
                sent = forwards(origin, up_way)
                if t == 1 and extent > 3:
                    sent = sent & jnp.logical_not((origin == z) & late(up_way))

                @pl.when(sent)
                def _():
                    tok_copy(t, origin, up_way).wait_send()

            @pl.loop(1, plane)
            def _(i):
                row_copy(t, origin, plane_peer(i)).wait_send()

            swap_copy(t, origin).wait_send()
        part_copy(origin).wait_send()

    def drain_returns():
        for i in range(1, extent):
            meta_copy(line_peer(i), z).wait_send()
        if extent > 3:
            for up_way in (False, True):

                @pl.when(late(up_way))
                def _():
                    tok_copy(1, z, up_way).wait_send()

        @pl.loop(0, extent)
        def _(origin):
            @pl.loop(1, plane)
            def _(i):
                ret_copy(origin, plane_peer(i)).wait_send()

            @pl.when(origin != z)
            def _():
                for j in range(columns):
                    line_copy(origin, j).wait_send()

        @pl.loop(1, plane)
        def _(i):
            for k in range(extent):
                active_copy(plane_peer(i), p, k).wait_send()

    def relay_band(k, jj):
        home = looked_up(relays, z, k)

        @pl.when(has_inflow(home))
        def _():
            j = band_for(home, jj)
            line_arrival(home, j).wait_recv()
            line_sent[home, :, band(j)] = (
                line_sent[home, :, band(j)].astype(jnp.float32)
                + line_got[home, :, band(j)].astype(jnp.float32)
            ).astype(jnp.bfloat16)
            line_copy(home, j).start()

    for load in loads[:2]:
        load.wait()
    for i in range(1, extent):
        meta_copy(line_peer(i), z).start()

    local = values.shape[1]
    strip = min(256, local)
    strips = local // strip
    row_count = values.shape[0]

    def strip_at(n):
        return pl.ds(pl.multiple_of(n * strip, strip), strip)

    def stat_copy(i):
        return remote(
            stats.at[i, 0], stats.at[i, 1], stat_sems.at[0, i], stat_sems.at[1, i], sp, other
        )

    def paired(i, first, second):
        lane = lax.broadcasted_iota(jnp.int32, (row_count, stats.shape[3]), 1)
        stats[i, 0] = jnp.where(lane == 0, first, second)
        stat_copy(i).start()

    def both_sums(i):
        stat_copy(i).wait_recv()
        merged = (stats[i, 0] + stats[i, 1]) / width
        return merged[:, 0:1], merged[:, 1:2]

    share = row_count // extent

    def active_copy(q, owner, i):
        part = active.at[owner, pl.ds(i * share, share)]
        return remote(
            part, part, active_send.at[q, i], active_recv.at[owner, i], z * plane + q, tp
        )

    def prepare():
        loads[5].wait()
        sums = jnp.zeros((row_count, 1), jnp.float32)
        squares = jnp.zeros((row_count, 1), jnp.float32)
        for n in range(strips):
            block = values[:, n * strip : (n + 1) * strip].astype(jnp.float32)
            sums = sums + jnp.sum(block, axis=1, keepdims=True)
            squares = squares + jnp.sum(block * block, axis=1, keepdims=True)
        paired(0, sums, squares)
        average, second = both_sums(0)
        scale = lax.rsqrt(second - average * average + NORM_EPS)
        inverse[...] = jnp.broadcast_to(scale, inverse.shape)
        for n in range(strips):
            cut = slice(n * strip, (n + 1) * strip)
            flat = (values[:, cut].astype(jnp.float32) - average) * scale
            normed[:, cut] = flat
            scaled = flat * gain[:, cut]
            active[p, :, cut] = (scaled * jax.nn.sigmoid(scaled)).astype(jnp.bfloat16)

    def share_active(k):
        @pl.loop(1, plane)
        def _(i):
            active_copy(plane_peer(i), p, k).start()

    send_own(0)
    send_own(1)
    arrive(0, z)
    arrive(1, z)
    prepare()

    @pl.loop(0, extent)
    def _(k):
        @pl.when(k > 0)
        def _():
            forward(1, k)

        swap(0, k)
        first_products(k)

        @pl.when(k == 0)
        def _():
            forward(0, 1)

        @pl.when(k < extent - 1)
        def _():
            event(2 * k)

        @pl.when((k > 0) & (k < extent - 1))
        def _():
            forward(0, k + 1)

        @pl.when((k > 0) & (k < extent - 1))
        def _():
            combine(k - 1)

        @pl.when(k > 0)
        def _():
            drain(k - 1)

        @pl.when(k == extent - 1)
        def _():
            @pl.loop(0, columns)
            def _(jj):
                relay_band(0, jj)

        swap(1, k)
        share_active(k)
        products(k)

        @pl.when(k < extent - 1)
        def _():
            event(2 * k + 1)

        @pl.when(k == extent - 1)
        def _():
            combine(k - 1)

        send_back(k)

    drain(extent - 1)
    combine(extent - 1)

    @pl.loop(0, columns)
    def _(jj):
        relay_band(1, jj)
        gate_up_share(0, jj)

    grad_store(0).start()

    @pl.loop(0, columns)
    def _(jj):
        for k in range(2, extent - 1):
            relay_band(k, jj)
        gate_up_share(1, jj)

    grad_store(1).start()

    own_block = width // (extent * plane)
    lanes = blocks.shape[4]

    def block_at(j, q):
        start = (j * plane + q) * own_block
        return pl.ds(pl.multiple_of(start // lanes * lanes, lanes), lanes)

    def token_copy(j):
        return remote(
            tokens.at[tp, :, band(j)],
            tokens.at[tp, :, band(j)],
            token_sems.at[0, j],
            token_sems.at[1, j],
            sp,
            other,
        )

    def token_arrival(j):
        return remote(
            tokens.at[other, :, band(j)],
            tokens.at[other, :, band(j)],
            token_sems.at[0, j],
            token_sems.at[1, j],
            sp,
            other,
        )

    def block_copy(j, q):
        return remote(
            tokens.at[tp, :, block_at(j, q)],
            blocks.at[j, tp, p],
            block_send.at[j, q],
            block_recv.at[j, p],
            z * plane + q,
            tp,
        )

    def block_arrival(j, q):
        return remote(
            tokens.at[tp, :, block_at(j, q)],
            blocks.at[j, tp, q],
            block_send.at[j, q],
            block_recv.at[j, q],
            z * plane + q,
            tp,
        )

    def block_swap(j):
        return remote(
            blocks.at[j, tp],
            blocks.at[j, tp],
            block_swaps.at[0, j],
            block_swaps.at[1, j],
            sp,
            other,
        )

    def block_swap_arrival(j):
        return remote(
            blocks.at[j, other],
            blocks.at[j, other],
            block_swaps.at[0, j],
            block_swaps.at[1, j],
            sp,
            other,
        )

    def home_band(jj):
        j = band_for(z, jj)
        for slot, there in ((z, z > 0), (extent, z < extent - 1)):

            @pl.when(there)
            def _():
                line_arrival(slot, j).wait_recv()
                total[:, band(j)] = total[:, band(j)] + line_got[slot, :, band(j)].astype(
                    jnp.float32
                )

        tokens[tp, :, band(j)] = (
            tok[1, z, :, band(j)].astype(jnp.float32) + total[:, band(j)]
        ).astype(jnp.bfloat16)
        token_copy(j).start()

        @pl.loop(1, plane)
        def _(i):
            block_copy(j, plane_peer(i)).start()

        blocks[j, tp, p] = tokens[tp, :, block_at(j, p)]

    def swap_block(jj):
        j = band_for(z, jj)

        @pl.loop(1, plane)
        def _(i):
            block_arrival(j, plane_peer(i)).wait_recv()

        block_swap(j).start()

    pieces = 2
    piece = local // pieces

    def piece_at(h):
        return pl.ds(h * piece, piece)

    def sums_copy(j, h):
        to_z = jnp.where(j > z, z + 1, z - 1)
        slot = jnp.where((j < z) & (to_z == j), extent, j)
        return remote(
            sums_sent.at[j, :, piece_at(h)],
            sums_got.at[slot, :, piece_at(h)],
            sums_send.at[j, h],
            sums_recv.at[slot, h],
            to_z * plane + p,
            tp,
        )

    def sums_arrival(slot, h):
        return remote(
            sums_sent.at[0, :, piece_at(h)],
            sums_got.at[slot, :, piece_at(h)],
            sums_send.at[0, h],
            sums_recv.at[slot, h],
            sp,
            other,
        )

    def act_grads():
        loads[6].wait()
        for j in range(columns):
            token_arrival(j).wait_recv()
        grad_sum = jnp.zeros((row_count, 1), jnp.float32)
        grad_corr = jnp.zeros((row_count, 1), jnp.float32)
        for n in range(strips):
            cut = slice(n * strip, (n + 1) * strip)
            act_grad = lax.dot_general(
                tokens[...].reshape(row_count, width),
                out_weight[cut, :],
                (((1,), (1,)), ((), ())),
                preferred_element_type=jnp.float32,
            )
            flat = normed[:, cut]
            weight = gain[:, cut]
            scaled = flat * weight
            logistic = jax.nn.sigmoid(scaled)
            slope = act_grad * (logistic * (1.0 + scaled * (1.0 - logistic))) * weight
            spread[:row_count, cut] = slope
            grad_sum = grad_sum + jnp.sum(slope, axis=1, keepdims=True)
            grad_corr = grad_corr + jnp.sum(slope * flat, axis=1, keepdims=True)
        paired(1, grad_sum, grad_corr)

    def partial_block(jj):
        j = band_for(z, jj)
        block_swap_arrival(j).wait_recv()
        at = lax.rem((j * plane + p) * own_block, lanes)
        for n in range(strips):
            cut = slice(n * strip, (n + 1) * strip)
            mine = sum(
                lax.dot_general(
                    blocks[j, side].reshape(plane * token_count, lanes),
                    active[:, side * token_count : (side + 1) * token_count, cut].reshape(
                        plane * token_count, strip
                    ),
                    (((0,), (0,)), ((), ())),
                    preferred_element_type=jnp.float32,
                )
                for side in range(2)
            )
            if own_block != lanes:
                mine = sum(
                    jnp.where(at == start, mine[start : start + own_block], 0.0)
                    for start in range(0, lanes, own_block)
                )

            @pl.when(j == z)
            def _():
                sums_own[:, cut] = mine

            @pl.when(j != z)
            def _():
                sums_sent[j, :, cut] = mine.astype(jnp.bfloat16)

        @pl.when((j != z) & jnp.logical_not(has_inflow(j)))
        def _():
            for h in range(pieces):
                sums_copy(j, h).start()

    @pl.loop(1, plane)
    def _(i):
        for k in range(extent):
            active_copy(plane_peer(i), plane_peer(i), k).wait_recv()

    @pl.loop(0, extent)
    def _(jj):
        home_band(jj)

        @pl.when(jj > 0)
        def _():
            swap_block(jj - 1)

        @pl.when((jj > 0) & (jj < extent - 1))
        def _():
            partial_block(jj - 1)

    act_grads()
    swap_block(extent - 1)
    mean, corr = both_sums(1)
    edge = (padded.shape[0] - row_count) // 2
    scale = inverse[:, 0:1]
    for n in range(strips):
        cut = slice(n * strip, (n + 1) * strip)
        padded[edge : edge + row_count, cut] = (
            scale * (spread[:row_count, cut] - mean - normed[:, cut] * corr)
        ).astype(jnp.bfloat16)

    def halo_copy(up_way):
        if up_way:
            src, dst, to = row_count, 0, sp + 1
        else:
            src, dst, to = edge, edge + row_count, sp - 1
        return remote(
            padded.at[pl.ds(src, edge), :],
            padded.at[pl.ds(dst, edge), :],
            halo_sems.at[0, int(up_way)],
            halo_sems.at[1, int(up_way)],
            to,
            tp,
        )

    inside = {True: sp < last_sp, False: sp > 0}
    for up_way in (True, False):

        @pl.when(inside[up_way])
        def _():
            halo_copy(up_way).start()

    def relay(k):
        j = looked_up(sum_relays(extent), z, k)

        @pl.when(has_inflow(j))
        def _():
            for h in range(pieces):
                sums_arrival(j, h).wait_recv()
                sums_sent[j, :, piece_at(h)] = (
                    sums_sent[j, :, piece_at(h)].astype(jnp.float32)
                    + sums_got[j, :, piece_at(h)].astype(jnp.float32)
                ).astype(jnp.bfloat16)
                sums_copy(j, h).start()

    @pl.loop(max(0, extent - 2), extent)
    def _(jj):
        partial_block(jj)

    relay(0)
    tap_count = taps.shape[0]
    reach = tap_count // 2
    narrow = min(128, local)
    extra = (edge + reach) // 8 * 8

    def convolve(first, count):
        @pl.loop(0, local // narrow)
        def _(n):
            cut = pl.ds(pl.multiple_of(n * narrow, narrow), narrow)
            acc = jnp.zeros((count, narrow), jnp.float32)
            for s in range(8):
                taps_at = [o for o in range(tap_count) if (edge + reach - o) % 8 == s]
                if not taps_at:
                    continue
                shifted = spread[first + s : first + s + extra + count, cut]
                for o in taps_at:
                    m = (edge + reach - o) // 8 * 8
                    acc = acc + taps[o : o + 1, cut] * shifted[m : m + count]
            values[first : first + count, cut] = acc.astype(jnp.bfloat16)

    inner = slice(edge, edge + row_count)
    spread[inner] = padded[inner].astype(jnp.float32)
    if row_count > 2 * edge:
        convolve(edge, row_count - 2 * edge)
    for k in range(1, extent - 1):
        relay(k)
    grad_tiles(2, 0, half // min(256, half), min(256, half))
    grad_store(2).start()
    for up_way in (True, False):
        at = 0 if up_way else edge + row_count

        @pl.when(inside[not up_way])
        def _():
            halo_copy(up_way).wait_recv()
            spread[at : at + edge, :] = padded[at : at + edge, :].astype(jnp.float32)

        @pl.when(jnp.logical_not(inside[not up_way]))
        def _():
            spread[at : at + edge, :] = jnp.zeros((edge, local), jnp.float32)

    convolve(0, edge)
    convolve(row_count - edge, edge)
    finish = pltpu.make_async_copy(values, input_out, load_sem.at[0])
    finish.start()
    drain_returns()
    for h in range(pieces):
        for slot, there in ((z, z > 0), (extent, z < extent - 1)):

            @pl.when(there)
            def _():
                sums_arrival(slot, h).wait_recv()
                sums_own[:, piece_at(h)] = sums_own[:, piece_at(h)] + sums_got[
                    slot, :, piece_at(h)
                ].astype(jnp.float32)

    store = pltpu.make_async_copy(sums_own, proj_out, load_sem.at[1])
    store.start()
    for i in range(2):
        stat_copy(i).wait_send()
    for up_way in (True, False):

        @pl.when(inside[up_way])
        def _():
            halo_copy(up_way).wait_send()

    for j in range(columns):
        token_copy(j).wait_send()

        @pl.loop(1, plane)
        def _(i):
            block_copy(j, plane_peer(i)).wait_send()

        block_swap(j).wait_send()

        @pl.when(z != j)
        def _():
            for h in range(pieces):
                sums_copy(j, h).wait_send()

    finish.wait()
    store.wait()
    for which in range(3):
        grad_store(which).wait()


TOPK_ROWS = 2


def routed_backward(
    mid_rows,
    cotangent,
    routes,
    route_weight,
    gate_mat,
    up_mat,
    down_mat,
    filtered,
    out_weight,
    taps,
    gain,
    capacity,
):
    sp_count = lax.axis_size("sp")
    extent = line_extent(sp_count)
    plane = sp_count // extent
    token_count, width = mid_rows.shape
    half = gate_mat.shape[1]
    slots = plane * capacity
    kind = jnp.bfloat16
    any_space = pl.BlockSpec(memory_space=pl.ANY)
    vmem = pl.BlockSpec(memory_space=pltpu.VMEM)
    dma = pltpu.SemaphoreType.DMA
    columns = extent
    row_count, local = filtered.shape
    own_block = width // sp_count
    lanes = min(max(own_block, 128), width // extent)
    edge = -(-(taps.shape[0] // 2) // 16) * 16
    rows_shape = (extent, 2, plane, capacity, width)
    small_shape = (extent, 2 * slots, half)
    scratch = [
        pltpu.VMEM((2, extent, token_count, width), kind),
        pltpu.VMEM((8, token_count), jnp.float32),
        pltpu.VMEM((extent, 8, token_count), jnp.float32),
        pltpu.VMEM((2, extent, plane, capacity, width), kind),
        pltpu.VMEM((2,) + rows_shape, kind),
        pltpu.VMEM(gate_mat.shape, kind),
        pltpu.VMEM(up_mat.shape, kind),
        pltpu.VMEM(down_mat.shape, kind),
        pltpu.VMEM((2 * slots, half), jnp.float32),
        pltpu.VMEM((2 * slots, half), jnp.float32),
        pltpu.VMEM(small_shape, kind),
        pltpu.VMEM(small_shape, kind),
        pltpu.VMEM(small_shape, kind),
        pltpu.VMEM((extent, plane, capacity, width), kind),
        pltpu.VMEM((extent, plane, capacity, width), kind),
        pltpu.VMEM((extent, plane, capacity, width), kind),
        pltpu.VMEM((extent, plane, capacity, width), kind),
        pltpu.VMEM((extent, token_count, width), kind),
        pltpu.VMEM((extent + 1, token_count, width), kind),
        pltpu.VMEM((token_count, width), jnp.float32),
        pltpu.VMEM((2, token_count, width), kind),
        dma((7,)),
        dma((2, extent)),
        dma((2, extent, 2)),
        dma((2, extent)),
        dma((2, extent, plane)),
        dma((2, extent, plane)),
        dma((2, extent)),
        dma((2, extent)),
        dma((2, extent)),
        dma((extent, plane)),
        dma((extent, plane)),
        dma((extent, columns)),
        dma((extent + 1, columns)),
        dma((3,)),
        dma((2, columns)),
        pltpu.VMEM((row_count, local), kind),
        pltpu.VMEM(out_weight.shape, kind),
        pltpu.VMEM((2, 2, row_count, 128), jnp.float32),
        pltpu.VMEM((row_count, local), jnp.float32),
        pltpu.VMEM((row_count, 128), jnp.float32),
        pltpu.VMEM((plane, row_count, local), kind),
        pltpu.VMEM((extent, 2, plane, token_count, lanes), kind),
        pltpu.VMEM((extent, own_block, local), kind),
        pltpu.VMEM((extent + 1, own_block, local), kind),
        pltpu.VMEM((own_block, local), jnp.float32),
        pltpu.VMEM((row_count + 2 * edge, local), kind),
        pltpu.VMEM((row_count + 2 * edge, local), jnp.float32),
        dma((2, 2)),
        dma((plane, extent)),
        dma((plane, extent)),
        dma((extent, plane)),
        dma((extent, plane)),
        dma((2, extent)),
        dma((extent, 2)),
        dma((extent + 1, 2)),
        dma((2, 2)),
    ]
    held = sum(
        math.prod(s.shape) * jnp.dtype(s.dtype).itemsize
        for s in scratch
        if s.memory_space == pltpu.VMEM
    )
    out = pl.pallas_call(
        functools.partial(routed_kernel, extent, plane, capacity),
        out_shape=[
            jax.ShapeDtypeStruct((own_block, local), jnp.float32),
            jax.ShapeDtypeStruct((row_count, local), kind),
            jax.ShapeDtypeStruct(gate_mat.shape, kind),
            jax.ShapeDtypeStruct(up_mat.shape, kind),
            jax.ShapeDtypeStruct(down_mat.shape, kind),
        ],
        in_specs=[any_space] * 2 + [vmem] * 2 + [any_space] * 5 + [vmem] * 2,
        out_specs=[any_space] * 5,
        scratch_shapes=scratch,
        compiler_params=pltpu.CompilerParams(
            collective_id=0, has_side_effects=True, vmem_limit_bytes=min(held + SPARE, 67_043_328)
        ),
    )(
        mid_rows,
        cotangent,
        routes,
        route_weight,
        gate_mat,
        up_mat,
        down_mat,
        filtered,
        out_weight,
        taps,
        gain,
    )
    return out


def per_device(
    mid_rows,
    cotangent,
    routes,
    route_weight,
    filtered,
    conv_taps,
    norm_gain,
    out_weight,
    gate_weight,
    up_weight,
    down_weight,
):
    sp_count = lax.axis_size("sp")
    token_count, model_width = mid_rows.shape
    per_token = routes.shape[1]
    local_experts = gate_weight.shape[0]
    experts = local_experts * sp_count
    capacity = 2 * token_count * per_token // sp_count
    proj_grad, input_grad, *weight_grads = routed_backward(
        mid_rows,
        cotangent,
        routes.T,
        route_weight.T,
        gate_weight[0],
        up_weight[0],
        down_weight[0],
        filtered,
        out_weight,
        conv_taps,
        norm_gain[None],
        capacity,
    )
    gate_grad, up_grad, down_grad = (grad.astype(jnp.float32)[None] for grad in weight_grads)
    return (gate_grad, up_grad, down_grad, proj_grad, input_grad)


def solution(mesh):
    in_specs = (
        P(("sp", "tp"), None),
        P(("sp", "tp"), None),
        P(("sp", "tp"), None),
        P(("sp", "tp"), None),
        P("sp", "tp"),
        P(None, "tp"),
        P("tp"),
        P("tp", None),
        P("sp", None, "tp"),
        P("sp", None, "tp"),
        P("sp", "tp", None),
    )
    out_specs = (
        P("sp", None, "tp"),
        P("sp", None, "tp"),
        P("sp", "tp", None),
        P("sp", "tp"),
        P("sp", "tp"),
    )
    return jax.shard_map(
        per_device, mesh=mesh, in_specs=in_specs, out_specs=out_specs, check_vma=False
    )
```
